128 devices in a mesh: sp: 16 (over z, y), fs: 4 (over x), tp: 2 (over core).
Axes of the slice: x: 4, y: 4, z: 4, core: 2. Of those that a mesh axis runs over, the one named last changes fastest.
Arguments:
- tokens: bfloat16 [4, 6144, 2048], P('fs', 'sp', 'tp'), may hold values from -6 to 6
- in_gain: float32 [2048], replicated, may hold values from 0.1 to 1.9
- w_query: bfloat16 [2048, 1024], P('fs', 'tp'), may hold values from -0.125 to 0.125
- w_key: bfloat16 [2048, 1024], P('fs', 'tp'), may hold values from -0.125 to 0.125
- w_value: bfloat16 [2048, 1024], P('fs', 'tp'), may hold values from -0.125 to 0.125
- w_outgate: bfloat16 [2048, 1024], P('fs', 'tp'), may hold values from -0.125 to 0.125
- w_ingate: bfloat16 [2048, 1024], P('fs', 'tp'), may hold values from -0.125 to 0.125
- w_conv_in: bfloat16 [2048, 1024], P('fs', 'tp'), may hold values from -0.125 to 0.125
- score_offset: float32 [16], P('tp'), may hold values from 3.5 to 12
- conv_taps: float32 [3, 1024], P(None, 'tp'), may hold values from -3.5 to 3.5
- att_gain: float32 [1024], P('tp'), may hold values from 0.1 to 1.9
- conv_gain: float32 [1024], P('tp'), may hold values from 0.1 to 1.9
- out_att: bfloat16 [1024, 2048], P('tp'), may hold values from -0.125 to 0.125
- out_conv: bfloat16 [1024, 2048], P('tp'), may hold values from -0.125 to 0.125
Outputs:
- mixed: bfloat16 [4, 6144, 2048], P('fs', ('sp', 'tp'))
- log_mass: float32 [4, 6144, 16], P('fs', 'sp', 'tp')
The draws below stay inside these ranges and needn't reach their ends.
All inputs are finite; a program needn't handle non-finite values.
Results may differ from the reference program's by a relative error of at most 0.012.
Values may be sent and summed in bfloat16 or wider, within the bound.
A program may use at most 128 MiB of HBM per device.

```python
import jax
import jax.numpy as jnp
from jax import lax

D = 2048
HEADS = 16
HEAD_DIM = 64
CONV_CH = 1024
KTAP = 3
TOK_DEV = 384
ATT_WIDTH = 1024
LENGTH = 6144
SEQS = 4


def draw_score_offset(key, part):
    spread = jax.random.uniform(key, (HEADS,), jnp.float32)
    upper = jnp.maximum(jnp.log(jnp.float32(LENGTH)) + 0.5, 4.5)
    return 3.5 + spread * (upper - 3.5)


def levels(rng, extent, pieces, least, high):
    def one(dim, blocks):
        heights = jax.random.uniform(jax.random.fold_in(jax.random.fold_in(rng, 6), dim), (blocks,), jnp.float32, least / len(pieces), high / len(pieces))
        return jnp.repeat(jnp.exp(heights), extent[dim] // blocks).reshape((-1,) + (1,) * (len(extent) - dim - 1))

    level = one(*pieces[0])
    for cut in pieces[1:]:
        level = level * one(*cut)
    return level


def centred(key, extent, scale, bound, cuts=(), kind=jnp.bfloat16):
    level = levels(key, extent, cuts, -0.22, 0.18) if cuts else 1.0
    result = jax.random.normal(key, extent, jnp.float32) * scale * level
    return jnp.minimum(jnp.maximum(result, -bound), bound).astype(kind)


def setup_inputs(seed: int = 0) -> dict:
    key_of = jax.random.split(jax.random.key(seed), 15)
    tokens = centred(key_of[0], (SEQS, LENGTH, D), 1.0, 6.0, ((0, 4), (1, 16), (2, 2)))
    in_gain = jnp.clip(1.0 + 0.18 * jax.random.normal(key_of[1], (D,), jnp.float32), 0.1, 1.9)
    w_query = centred(key_of[2], (D, ATT_WIDTH), D ** -0.5, 0.125, ((0, 4), (1, 2)))
    w_key = centred(key_of[3], (D, ATT_WIDTH), D ** -0.5, 0.125, ((0, 4), (1, 2)))
    w_value = centred(key_of[4], (D, ATT_WIDTH), D ** -0.5, 0.125, ((0, 4), (1, 2)))
    w_outgate = centred(key_of[5], (D, CONV_CH), D ** -0.5, 0.125, ((0, 4), (1, 2)))
    w_ingate = centred(key_of[6], (D, CONV_CH), D ** -0.5, 0.125, ((0, 4), (1, 2)))
    w_conv_in = centred(key_of[7], (D, CONV_CH), D ** -0.5, 0.125, ((0, 4), (1, 2)))
    score_offset = draw_score_offset(jax.random.fold_in(key_of[14], 71), 0)
    conv_taps = centred(key_of[9], (KTAP, CONV_CH), KTAP ** -0.5, 3.5, ((1, 2),), jnp.float32)
    att_gain = jnp.clip(1.0 + 0.18 * jax.random.normal(key_of[10], (ATT_WIDTH,), jnp.float32), 0.1, 1.9)
    conv_gain = jnp.clip(1.0 + 0.18 * jax.random.normal(key_of[11], (CONV_CH,), jnp.float32), 0.1, 1.9)
    out_att = centred(key_of[12], (ATT_WIDTH, D), (ATT_WIDTH + CONV_CH) ** -0.5, 0.125, ((0, 2),))
    out_conv = centred(key_of[13], (CONV_CH, D), (ATT_WIDTH + CONV_CH) ** -0.5, 0.125, ((0, 2),))
    return dict(tokens=tokens, in_gain=in_gain, w_query=w_query, w_key=w_key, w_value=w_value, w_outgate=w_outgate, w_ingate=w_ingate, w_conv_in=w_conv_in, score_offset=score_offset, conv_taps=conv_taps, att_gain=att_gain, conv_gain=conv_gain, out_att=out_att, out_conv=out_conv)


epsilon = 1e-06

def attention_block(block_index, query_heads, key_heads, value_heads, offsets):
    start = block_index * TOK_DEV
    queries = lax.dynamic_slice_in_dim(query_heads, start, TOK_DEV, 0)
    scores = jnp.einsum('qhd,khd->hqk', queries, key_heads) * HEAD_DIM ** (-0.5) - offsets[:, None, None]
    query_pos = start + lax.iota(jnp.int32, TOK_DEV)
    key_pos = lax.iota(jnp.int32, LENGTH)
    valid = key_pos[None, None, :] < query_pos[None, :, None]
    log_keep = jnp.where(valid, -jax.nn.softplus(scores), 0.0)
    later = lax.cumsum(log_keep, axis=2, reverse=True) - log_keep
    weights = jnp.where(valid, jnp.exp(-jax.nn.softplus(-scores) + later), 0.0)
    rounded = lax.optimization_barrier(weights.astype(jnp.bfloat16)).astype(jnp.float32)
    attended = jnp.einsum('hqk,khd->qhd', rounded, value_heads)
    masses = jnp.log(1.0 + lax.optimization_barrier(jnp.sum(weights, axis=2))).T
    return (attended.reshape(TOK_DEV, ATT_WIDTH), masses)

def reference(tokens, in_gain, w_query, w_key, w_value, w_outgate, w_ingate, w_conv_in, score_offset, conv_taps, att_gain, conv_gain, out_att, out_conv):

    def one_sequence(sequence):
        widened = sequence.astype(jnp.float32)
        in_scale = lax.rsqrt(lax.optimization_barrier(jnp.mean(widened * widened, axis=1)) + epsilon)
        scaled = (widened * in_gain).astype(jnp.bfloat16)

        def project(matrix):
            product = jnp.dot(scaled, matrix, preferred_element_type=jnp.float32)
            return (product * in_scale[:, None]).astype(jnp.bfloat16)
        query = project(w_query)
        key_rows = project(w_key)
        value_rows = project(w_value)
        outgate = project(w_outgate)
        ingate = project(w_ingate)
        conv_input = project(w_conv_in)
        query_heads = query.astype(jnp.float32).reshape(LENGTH, HEADS, HEAD_DIM)
        key_heads = key_rows.astype(jnp.float32).reshape(LENGTH, HEADS, HEAD_DIM)
        value_heads = value_rows.astype(jnp.float32).reshape(LENGTH, HEADS, HEAD_DIM)

        def run_block(block_index):
            return attention_block(block_index, query_heads, key_heads, value_heads, score_offset)
        attended, masses = lax.map(run_block, jnp.arange(LENGTH // TOK_DEV, dtype=jnp.int32))
        attended = attended.reshape(LENGTH, ATT_WIDTH)
        masses = masses.reshape(LENGTH, HEADS)
        gated_input = ingate.astype(jnp.float32) * conv_input.astype(jnp.float32)
        padded = jnp.pad(gated_input, ((KTAP - 1, 0), (0, 0)))
        convolved = sum((conv_taps[tap_index] * padded[tap_index:tap_index + LENGTH] for tap_index in range(KTAP)))
        conv_out = outgate.astype(jnp.float32) * convolved
        att_scale = lax.rsqrt(lax.optimization_barrier(jnp.mean(attended * attended, axis=1)) + epsilon)
        conv_scale = lax.rsqrt(lax.optimization_barrier(jnp.mean(conv_out * conv_out, axis=1)) + epsilon)
        att_scaled = (attended * att_gain).astype(jnp.bfloat16)
        conv_scaled = (conv_out * conv_gain).astype(jnp.bfloat16)
        total = att_scale[:, None] * jnp.dot(att_scaled, out_att, preferred_element_type=jnp.float32)
        total = total + conv_scale[:, None] * jnp.dot(conv_scaled, out_conv, preferred_element_type=jnp.float32)
        return (total.astype(jnp.bfloat16), masses)
    mixed, log_mass = lax.map(one_sequence, tokens)
    return (mixed, log_mass)
```

```python
import functools

import jax
import jax.numpy as jnp
from jax import lax
from jax.experimental import pallas as pl
from jax.experimental.pallas import tpu as pltpu
from jax.sharding import PartitionSpec as P

D = 2048
CONV_CH = 1024
ATT_WIDTH = 1024
SEQS = 4
ROWS = 384
HALF = 192
BLOCKS = 16
HD = 64
MESSAGE = ROWS + HALF // 2
epsilon = 1e-06
LOG2E = 1.4426950408889634
F32 = jnp.float32
BF16 = jnp.bfloat16


def dot(a, b):
    return jnp.dot(a, b, preferred_element_type=F32)


def dot_nt(a, b):
    return lax.dot_general(a, b, (((1,), (1,)), ((), ())), preferred_element_type=F32)


def three_parts(x):
    a = x.astype(BF16)
    rest = x - a.astype(F32)
    b = rest.astype(BF16)
    return a, b, (rest - b.astype(F32)).astype(BF16)


def project_kernel(tok_ref, gain_ref, w_ref, msg_ref, gated_ref, outgate_ref):
    flip = lax.rem(lax.axis_index("sp"), 2)
    low = tok_ref[0, 0].astype(F32)
    high = tok_ref[0, 1].astype(F32)
    squares = jnp.sum(low * low, axis=1, keepdims=True) + jnp.sum(high * high, axis=1, keepdims=True)
    scale = lax.rsqrt(squares / D + epsilon)
    total = dot((low * gain_ref[0:1, :]).astype(BF16), w_ref[0:1024, :]) + dot(
        (high * gain_ref[1:2, :]).astype(BF16), w_ref[1024:2048, :]
    )
    out = (total * scale).astype(BF16)
    query, key, value = out[:, 0:128], out[:, 128:256], out[:, 256:384]
    for head in range(2):
        mine = slice(head * HD, (head + 1) * HD)
        pair = jnp.concatenate((key[:, mine], value[:, mine]), axis=1)
        for half in range(2):
            msg_ref[2 * head + half, 0:ROWS, :] = pair
        halves = [
            jnp.concatenate(
                (query[i * HALF : i * HALF + 96, mine], query[i * HALF + 96 : (i + 1) * HALF, mine]),
                axis=1,
            )
            for i in range(2)
        ]

        @pl.when(flip == 0)
        def _():
            msg_ref[2 * head, ROWS:MESSAGE, :] = halves[0]
            msg_ref[2 * head + 1, ROWS:MESSAGE, :] = halves[1]

        @pl.when(flip == 1)
        def _():
            msg_ref[2 * head, ROWS:MESSAGE, :] = halves[1]
            msg_ref[2 * head + 1, ROWS:MESSAGE, :] = halves[0]

    outgate_ref[0] = out[:, 384:512]
    gated_ref[0] = out[:, 512:640].astype(F32) * out[:, 640:768].astype(F32)


def project(tok, gains, weights):
    return pl.pallas_call(
        project_kernel,
        grid=(SEQS,),
        in_specs=[
            pl.BlockSpec((1, 2, ROWS, 1024), lambda s: (s, 0, 0, 0)),
            pl.BlockSpec((2, 1024), lambda s: (0, 0)),
            pl.BlockSpec((D, 768), lambda s: (0, 0)),
        ],
        out_specs=[
            pl.BlockSpec((4, MESSAGE, 128), lambda s: (s, 0, 0)),
            pl.BlockSpec((1, ROWS, 128), lambda s: (s, 0, 0)),
            pl.BlockSpec((1, ROWS, 128), lambda s: (s, 0, 0)),
        ],
        out_shape=[
            jax.ShapeDtypeStruct((16, MESSAGE, 128), BF16),
            jax.ShapeDtypeStruct((SEQS, ROWS, 128), F32),
            jax.ShapeDtypeStruct((SEQS, ROWS, 128), BF16),
        ],
        compiler_params=pltpu.CompilerParams(vmem_limit_bytes=48 << 20),
        cost_estimate=pl.CostEstimate(flops=4_800_000_000, bytes_accessed=13_000_000, transcendentals=0),
        name="project",
    )(tok, gains, weights)


def attend_kernel(
    offset_ref, gain_ref, recv_ref, out_ref, keys, values, queries, scores, decays, weights, total
):
    place = lax.axis_index("sp")
    half = lax.rem(place, 2)
    head = 2 * lax.axis_index("fs") + lax.rem(place // 2, 2)
    lanes = lambda shape: lax.broadcasted_iota(jnp.int32, shape, 1)
    rows = lambda shape: lax.broadcasted_iota(jnp.int32, shape, 0)
    offset = jnp.full((HALF, 128), offset_ref[head] * LOG2E, F32)
    o1, o2, o3 = (part.astype(F32) for part in three_parts(offset))
    lane_q = lanes((HALF, 128))
    offset_row = jnp.where(
        lane_q == 0, -o1, jnp.where(lane_q == 1, -o2, jnp.where(lane_q == 2, -o3, 0.0))
    ).astype(BF16)
    square = (ROWS, ROWS)
    permute = (
        (lanes(square) == lax.rem(rows(square), 8) * 48 + rows(square) // 8).astype(F32).astype(BF16)
    )
    shape = (128, 128)
    twice_low = (rows(shape) == lax.rem(lanes(shape), HD)).astype(F32).astype(BF16)
    twice_high = (rows(shape) == lax.rem(lanes(shape), HD) + HD).astype(F32).astype(BF16)
    take_high = (lanes((HD, 128)) == rows((HD, 128)) + HD).astype(F32).astype(BF16)
    ones = (lanes((ROWS, 128)) < 3).astype(F32).astype(BF16)
    for block in range(BLOCKS):
        pair = dot(permute, recv_ref[block, 0:ROWS, :]).astype(BF16)
        keys[block * ROWS : (block + 1) * ROWS, 0:128] = dot(pair, twice_low).astype(BF16)
        keys[block * ROWS : (block + 1) * ROWS, 128:256] = ones
        values[block] = dot_nt(take_high, pair).astype(BF16)
        packed = recv_ref[block, ROWS:MESSAGE, :]
        q = jnp.concatenate((dot(packed, twice_low), dot(packed, twice_high)), axis=0) * (LOG2E / 8)
        q_high = q.astype(BF16).astype(F32)
        at = slice((block % 2) * HALF, (block % 2 + 1) * HALF)
        queries[block // 2, at, 0:128] = jnp.where(lane_q < HD, q_high, q - q_high).astype(BF16)
        queries[block // 2, at, 128:256] = offset_row

    sub = rows((8, ROWS))
    lane = lanes((8, ROWS))
    where_q = lane + jnp.where(half == 1, HALF, jnp.where(lane < HALF, 0, ROWS))

    def tile(tile_index, block, carry, ahead, slot):
        begin = pl.multiple_of(block * ROWS, ROWS)
        z_ref, d_ref, w_ref = scores.at[slot], decays.at[slot], weights.at[slot]
        z_ref[...] = dot_nt(keys[pl.ds(begin, ROWS), :], queries[tile_index])
        run = jnp.zeros((8, ROWS), F32)
        for r in reversed(range(48)):
            z = z_ref[8 * r : 8 * r + 8, :]
            soft = jnp.maximum(z, jnp.log2(1.0 + jnp.exp2(jnp.minimum(z, 126.0))))
            if ahead is not None:
                valid = ahead > r
                soft = jnp.where(valid, soft, 0.0)
            run = run + soft
            decay = jnp.exp2(z - run)
            if ahead is not None:
                decay = jnp.where(valid, decay, 0.0)
            d_ref[8 * r : 8 * r + 8, :] = decay
        suffix = run
        for step in (1, 2, 4):
            moved = pltpu.roll(suffix, 8 - step, 0)
            suffix = suffix + jnp.where(sub < 8 - step, moved, 0.0)
        after = jnp.where(sub < 7, pltpu.roll(suffix, 7, 0), 0.0)
        kept = jnp.exp2(-(carry + after))
        for i in range(24):
            both = jnp.concatenate(
                (d_ref[16 * i : 16 * i + 8, :] * kept, d_ref[16 * i + 8 : 16 * i + 16, :] * kept), axis=0
            )
            w_ref[16 * i : 16 * i + 16, :] = both.astype(BF16)
        total[...] += dot(values[block], w_ref[...])
        return carry + jnp.broadcast_to(suffix[0:1], (8, ROWS))

    gain = gain_ref[...]
    gain_lane = lanes((8, 512))
    out_lane = lanes((ROWS, 128))

    def one_tile(m, _):
        total[...] = jnp.zeros_like(total)
        carry = jnp.zeros((8, ROWS), F32)
        carry = tile(m, 2 * m + 1, carry, where_q - ROWS - 48 * sub, 0)
        carry = tile(m, 2 * m, carry, where_q - 48 * sub, 1)

        def before(i, carry):
            at = 2 * (m - 1 - i)
            carry = tile(m, at + 1, carry, None, 0)
            return tile(m, at, carry, None, 1)

        carry = lax.fori_loop(0, m, before, carry)
        attended = total[...]
        squares = jnp.sum(attended * attended, axis=0, keepdims=True)
        parts = [p.astype(F32) for p in three_parts(carry[0:1]) + three_parts(squares)]
        side = jnp.concatenate(parts + [jnp.zeros((HD - 6, ROWS), F32)], axis=0)
        message = jnp.concatenate((attended, side), axis=0).T
        message = message * jnp.where(out_lane < HD, gain, 1.0)
        message = message.astype(BF16)
        out_ref[2 * m] = message[0:HALF]
        out_ref[2 * m + 1] = message[HALF:ROWS]
        return 0

    lax.fori_loop(0, BLOCKS // 2, one_tile, 0)


def attend(recv, offsets, gain):
    whole = pl.BlockSpec(memory_space=pltpu.VMEM)
    return pl.pallas_call(
        attend_kernel,
        in_specs=[pl.BlockSpec(memory_space=pltpu.SMEM), whole, whole],
        out_specs=whole,
        out_shape=jax.ShapeDtypeStruct((BLOCKS, HALF, 128), BF16),
        scratch_shapes=[
            pltpu.VMEM((BLOCKS * ROWS, 256), BF16),
            pltpu.VMEM((BLOCKS, HD, ROWS), BF16),
            pltpu.VMEM((BLOCKS // 2, ROWS, 256), BF16),
            pltpu.VMEM((2, ROWS, ROWS), F32),
            pltpu.VMEM((2, ROWS, ROWS), F32),
            pltpu.VMEM((2, ROWS, ROWS), BF16),
            pltpu.VMEM((HD, ROWS), F32),
        ],
        compiler_params=pltpu.CompilerParams(vmem_limit_bytes=48 << 20),
        cost_estimate=pl.CostEstimate(
            flops=10_000_000_000, bytes_accessed=3_000_000, transcendentals=30_000_000
        ),
        name="attend",
    )(offsets, gain, recv)


def per_device(
    tokens,
    in_gain,
    w_query,
    w_key,
    w_value,
    w_outgate,
    w_ingate,
    w_conv_in,
    score_offset,
    conv_taps,
    att_gain,
    conv_gain,
    out_att,
    out_conv,
):
    place = lax.axis_index("sp")
    column = lax.axis_index("fs")
    core = lax.axis_index("tp")
    tok = lax.all_gather(tokens[0], ("fs", "tp")).reshape(SEQS, 2, ROWS, 1024)
    mats = [
        w.reshape(512, 4, 128) for w in (w_query, w_key, w_value, w_outgate, w_ingate, w_conv_in)
    ]
    spread = jnp.moveaxis(jnp.stack(mats, axis=2), 1, 0).reshape(4, 512, 768)
    mine = lax.all_to_all(spread, "fs", 0, 0, tiled=True).reshape(D, 768)
    messages, gated, outgate = project(tok, in_gain.reshape(2, 1024), mine)

    recv = lax.all_to_all(messages, "sp", 0, 0, tiled=True)
    head = 2 * column + lax.rem(place // 2, 2)
    gain = lax.dynamic_slice_in_dim(att_gain, head * HD, HD, 0)
    gain = jnp.concatenate((gain, jnp.ones((HD,), F32)))[None]
    sent = attend(recv, score_offset, gain)
    back = lax.all_to_all(sent, "sp", 0, 0, tiled=True)

    pairs = [(i, i + 1) for i in range(BLOCKS - 1)]
    before = lax.ppermute(gated[:, ROWS - 2 :], "sp", pairs)
    extended = jnp.concatenate((before, gated), axis=1)
    taps = lax.dynamic_slice_in_dim(conv_taps, column * 128, 128, 1)
    convolved = sum(taps[j] * extended[:, j : j + ROWS] for j in range(3))
    conv_out = outgate.astype(F32) * convolved
    conv_squares = jnp.sum(conv_out * conv_out, axis=2)
    conv_mine = lax.dynamic_slice_in_dim(conv_gain, column * 128, 128, 0)
    conv_scaled = (conv_out * conv_mine).astype(BF16)

    att = back.reshape(SEQS, 2, 2, HALF, 128)
    att = jnp.where(lax.rem(place, 2) == 0, att, att[:, :, ::-1])
    pieces = jnp.stack(three_parts(conv_squares), axis=-1).reshape(SEQS, 2, HALF, 3)
    other = att[:, :, ::-1, :, HD : HD + 3]
    both = jnp.concatenate((att[:, 0, :, :, :HD], att[:, 1, :, :, :HD]), axis=-1)
    side = jnp.concatenate(
        [att[:, 0, :, :, HD : HD + 6], att[:, 1, :, :, HD : HD + 6]]
        + [other[:, 0], other[:, 1], pieces, jnp.zeros((SEQS, 2, HALF, 128 - 21), BF16)],
        axis=-1,
    )
    outbound = jnp.stack((both, conv_scaled.reshape(SEQS, 2, HALF, 128), side), axis=2)
    home = lax.all_to_all(outbound.reshape(8, 3, HALF, 128), ("fs", "tp"), 0, 0, tiled=True)
    home = home.reshape(4, 2, 3, HALF, 128)

    wide = lambda a: a.transpose(2, 1, 0, 3).reshape(HALF, 1024)
    att_mat, conv_mat = wide(home[:, :, 0]), wide(home[:, :, 1])
    extra = home[:, :, 2].astype(F32)
    joined = lambda at: extra[..., at] + extra[..., at + 1] + extra[..., at + 2]
    att_sum = jnp.sum(joined(3) + joined(9), axis=(0, 1))
    conv_sum = jnp.sum(joined(18), axis=(0, 1))
    att_scale = lax.rsqrt(att_sum / ATT_WIDTH + epsilon)
    conv_scale = lax.rsqrt(conv_sum / CONV_CH + epsilon)
    out_weights = lax.all_gather(jnp.stack((out_att, out_conv)), "tp", axis=1, tiled=True)
    mixed = att_scale[:, None] * dot(att_mat, out_weights[0]) + conv_scale[:, None] * dot(
        conv_mat, out_weights[1]
    )

    here = lax.dynamic_index_in_dim(extra, core, 1, keepdims=False)
    pick = lambda at: here[..., at] + here[..., at + 1] + here[..., at + 2]
    own = jnp.stack((pick(0), pick(6)), axis=1).reshape(8, HALF)
    far = jnp.stack((pick(12), pick(15)), axis=1).reshape(8, HALF)
    decayed = jnp.where(
        core == 0, jnp.concatenate((own, far), axis=1), jnp.concatenate((far, own), axis=1)
    )
    log_mass = jnp.log(2.0 - jnp.exp2(-decayed)).T
    return (mixed.astype(BF16)[None], log_mass[None])


def solution(mesh):
    return jax.shard_map(
        per_device,
        mesh=mesh,
        in_specs=(
            P("fs", "sp", "tp"),
            P(),
            P("fs", "tp"),
            P("fs", "tp"),
            P("fs", "tp"),
            P("fs", "tp"),
            P("fs", "tp"),
            P("fs", "tp"),
            P("tp"),
            P(None, "tp"),
            P("tp"),
            P("tp"),
            P("tp", None),
            P("tp", None),
        ),
        out_specs=(P("fs", ("sp", "tp"), None), P("fs", "sp", "tp")),
        check_vma=False,
    )
```

```python
import functools

import jax
import jax.numpy as jnp
from jax import lax
from jax.experimental import pallas as pl
from jax.experimental.pallas import tpu as pltpu
from jax.sharding import PartitionSpec as P

D = 2048
CONV_CH = 1024
ATT_WIDTH = 1024
SEQS = 4
ROWS = 384
HALF = 192
BLOCKS = 16
HD = 64
MESSAGE = HALF + HALF // 2
epsilon = 1e-06
LOG2E = 1.4426950408889634
F32 = jnp.float32
BF16 = jnp.bfloat16


def dot(a, b):
    return jnp.dot(a, b, preferred_element_type=F32)


def dot_nt(a, b):
    return lax.dot_general(a, b, (((1,), (1,)), ((), ())), preferred_element_type=F32)


def three_parts(x):
    a = x.astype(BF16)
    rest = x - a.astype(F32)
    b = rest.astype(BF16)
    return a, b, (rest - b.astype(F32)).astype(BF16)


MESH = pl.DeviceIdType.MESH
LEFT, RIGHT = slice(0, 384), slice(384, 768)


def mod4(value):
    return lax.rem(value + 8, 4)


def front_kernel(
    tokens_ref,
    gain_ref,
    wq_ref,
    wk_ref,
    wv_ref,
    wo_ref,
    wi_ref,
    wc_ref,
    att_ref,
    conv_ref,
    own_ref,
    mate_ref,
    gated_ref,
    outgate_ref,
    att_other_ref,
    conv_other_ref,
    tok,
    wts,
    msg,
    recv,
    mate,
    local_sem,
    spread_send,
    spread_recv,
    near_send,
    near_recv,
    far_send,
    far_recv,
    pass_send,
    pass_recv,
    tok_send,
    tok_recv,
    pair_send,
    pair_recv,
    msg_send,
    msg_recv,
    mate_send,
    mate_recv,
    other_send,
    other_recv,
):
    place, x, core = lax.axis_index("sp"), lax.axis_index("fs"), lax.axis_index("tp")
    y, z = lax.rem(place, 4), lax.div(place, 4)
    sibling = (place, x, 1 - core)
    mats = (wq_ref, wk_ref, wv_ref, wo_ref, wi_ref, wc_ref)

    def remote(src, dst, send, recv_sem, device):
        return pltpu.make_async_remote_copy(
            src_ref=src, dst_ref=dst, send_sem=send, recv_sem=recv_sem, device_id=device, device_id_type=MESH
        )

    own_tokens = pltpu.make_async_copy(tokens_ref, tok.at[x, core], local_sem.at[6])
    own_tokens.start()
    own_weights = []
    for m in range(6):
        for part in range(4):
            own_weights.append(
                pltpu.make_async_copy(
                    mats[m].at[pl.ds(part * 128, 128), pl.ds(pl.multiple_of(x * 128, 128), 128)],
                    wts.at[x, part, :, m * 128 : (m + 1) * 128],
                    local_sem.at[7 + 4 * m + part],
                )
            )
    for copy in own_weights:
        copy.start()

    barrier = pltpu.get_barrier_semaphore()
    for k in range(1, 4):
        pl.semaphore_signal(barrier, inc=1, device_id=(place, mod4(x + k), core), device_id_type=MESH)
    pl.semaphore_signal(barrier, inc=1, device_id=sibling, device_id_type=MESH)

    def greet(k, _):
        there = lax.rem(place + k, BLOCKS)
        pl.semaphore_signal(barrier, inc=1, device_id=(there, x, core), device_id_type=MESH)
        pl.semaphore_signal(barrier, inc=1, device_id=(there, x, 1 - core), device_id_type=MESH)
        return 0

    lax.fori_loop(1, BLOCKS, greet, 0)
    pl.semaphore_wait(barrier, 34)

    rows_at = pl.multiple_of(place * 32, 32)

    def spread(k, m):
        there = mod4(x + k)
        return remote(
            mats[m].at[pl.ds(rows_at, 32), pl.ds(pl.multiple_of(there * 128, 128), 128)],
            wts.at[x, z, pl.ds(pl.multiple_of(y * 32, 32), 32), m * 128 : (m + 1) * 128],
            spread_send.at[k - 1, m],
            spread_recv.at[k - 1, m],
            (place, there, core),
        )

    for k in range(1, 4):
        for m in range(6):
            spread(k, m).start()

    own_tokens.wait()
    top, bottom = pl.ds(0, HALF), pl.ds(HALF, HALF)

    def hop(slot, f, rows, by):
        piece = tok.at[f, core, rows]
        return remote(piece, piece, tok_send.at[slot], tok_recv.at[slot], (place, mod4(x + by), core))

    def pair(slot, f, rows):
        piece = tok.at[f, core, rows]
        return remote(piece, piece, pair_send.at[slot], pair_recv.at[slot], sibling)

    right_a, right_b = hop(0, x, top, 1), hop(1, x, bottom, 1)
    left_b, left_a = hop(2, x, bottom, -1), hop(3, x, top, -1)
    before, after, across = mod4(x - 1), mod4(x + 1), mod4(x + 2)
    on_right, on_left = hop(4, before, top, 1), hop(5, after, bottom, -1)
    for copy in (right_a, left_b, right_b, left_a):
        copy.start()
    pairs = [
        pair(0, x, top),
        pair(1, x, bottom),
        pair(2, before, top),
        pair(3, after, bottom),
        pair(4, before, bottom),
        pair(5, after, top),
        pair(6, across, top),
        pair(7, across, bottom),
    ]
    pairs[0].start()
    pairs[1].start()

    for k in range(1, 4):
        for m in range(6):
            spread(k, m).wait_recv()

    my_rows = pl.ds(pl.multiple_of(y * 32, 32), 32)

    def near(k, i, way):
        f = mod4(x + i)
        piece = wts.at[f, z, my_rows, (LEFT, RIGHT)[way]]
        there = (z * 4 + mod4(y + k), x, core) if way == 0 else (mod4(z + k) * 4 + y, x, core)
        at = (3 * way + k - 1) * 3 + i - 1
        return remote(piece, piece, near_send.at[at], near_recv.at[at], there)

    for k in range(1, 4):
        for i in range(1, 4):
            for way in range(2):
                near(k, i, way).start()
    for k in range(1, 4):
        for i in range(1, 4):
            for way in range(2):
                near(k, i, way).wait_recv()

    def far(by, i, way):
        f = mod4(x + i)
        if way == 0:
            piece, there = wts.at[f, z, :, LEFT], (mod4(z + by) * 4 + y, x, core)
        else:
            piece, there = wts.at[f, :, my_rows, RIGHT], (z * 4 + mod4(y + by), x, core)
        at = (2 * way + (by + 1) // 2) * 3 + i - 1
        return remote(piece, piece, far_send.at[at], far_recv.at[at], there)

    def onward(by, i, way):
        f = mod4(x + i)
        start = 0 if by == 1 else 1
        if way == 0:
            piece = wts.at[f, mod4(z - by), 64 * start : 64 * start + 64, LEFT]
            there = (mod4(z + by) * 4 + y, x, core)
        else:
            rows = pl.ds(pl.multiple_of(mod4(y - by) * 32, 32), 32)
            piece = wts.at[f, 2 * start : 2 * start + 2, rows, RIGHT]
            there = (z * 4 + mod4(y + by), x, core)
        at = (2 * way + (by + 1) // 2) * 3 + i - 1
        return remote(piece, piece, pass_send.at[at], pass_recv.at[at], there)

    kinds = [(by, i, way) for i in range(1, 4) for by in (1, -1) for way in range(2)]
    for kind in kinds:
        far(*kind).start()
    right_a.wait_recv()
    on_right.start()
    pairs[2].start()
    left_b.wait_recv()
    on_left.start()
    pairs[3].start()
    for kind in kinds:
        far(*kind).wait_recv()
        onward(*kind).start()
    others = [
        remote(att_ref, att_other_ref, other_send.at[0], other_recv.at[0], sibling),
        remote(conv_ref, conv_other_ref, other_send.at[1], other_recv.at[1], sibling),
    ]
    for copy in own_weights:
        copy.wait()
    for kind in kinds:
        onward(*kind).wait_recv()

    def message(s, j, half):
        number = 2 * core + j
        there = mod4(s + number) * 4 + number
        at = 4 * s + 2 * j + half
        return remote(
            msg.at[at], recv.at[place], msg_send.at[at], msg_recv.at[place], (there, x, half)
        ), lax.abs(there - place) + lax.abs(half - core)

    def step(i, _):
        s = mod4(x + i + lax.div(i, 2) - 2 * lax.div(i, 3))

        @pl.when(i == 0)
        def _():
            pairs[0].wait_recv()
            pairs[1].wait_recv()

        @pl.when(i == 1)
        def _():
            right_b.wait_recv()
            pairs[4].start()
            left_a.wait_recv()
            pairs[5].start()
            pairs[3].wait_recv()
            pairs[5].wait_recv()

        @pl.when(i == 2)
        def _():
            pairs[2].wait_recv()
            pairs[4].wait_recv()

        @pl.when(i == 3)
        def _():
            on_right.wait_recv()
            pairs[6].start()
            on_left.wait_recv()
            pairs[7].start()
            for copy in others:
                copy.start()
            pairs[6].wait_recv()
            pairs[7].wait_recv()

        low = tok[s, 0].astype(F32)
        high = tok[s, 1].astype(F32)
        squares = jnp.sum(low * low, axis=1, keepdims=True) + jnp.sum(high * high, axis=1, keepdims=True)
        scale = lax.rsqrt(squares / D + epsilon)
        total = dot((low * gain_ref[0:1, :]).astype(BF16), wts[0:2].reshape(1024, 768)) + dot(
            (high * gain_ref[1:2, :]).astype(BF16), wts[2:4].reshape(1024, 768)
        )
        out = (total * scale).astype(BF16)
        query, key, value = out[:, 0:128], out[:, 128:256], out[:, 256:384]
        for j in range(2):
            mine = slice(j * HD, (j + 1) * HD)
            both = jnp.concatenate((key[:, mine], value[:, mine]), axis=1)
            for half in range(2):
                r = half * HALF
                folded = jnp.concatenate((query[r : r + 96, mine], query[r + 96 : r + HALF, mine]), axis=1)
                msg[4 * s + 2 * j + half, 0:HALF, :] = both[r : r + HALF]
                msg[4 * s + 2 * j + half, HALF : HALF + 96, :] = folded
        outgate_ref[s] = out[:, 384:512]
        gated_ref[s] = out[:, 512:640].astype(F32) * out[:, 640:768].astype(F32)
        for j in range(2):
            for half in range(2):
                copy, apart = message(s, j, half)

                @pl.when(apart > 0)
                def _():
                    copy.start()

                @pl.when(apart == 0)
                def _():
                    recv[place] = msg[4 * s + 2 * j + half]

        return 0

    lax.fori_loop(0, 4, step, 0)

    def to_mate(block):
        return remote(
            recv.at[block, 0:HALF], mate.at[block], mate_send.at[block], mate_recv.at[block], sibling
        )

    source_core = lax.div(y, 2)

    def arrive(k, _):
        block = lax.rem(place + k, BLOCKS)

        @pl.when(k + lax.abs(source_core - core) > 0)
        def _():
            remote(
                msg.at[0], recv.at[block], msg_send.at[0], msg_recv.at[block], (block, x, source_core)
            ).wait_recv()

        to_mate(block).start()
        return 0

    lax.fori_loop(0, BLOCKS, arrive, 0)
    own_out = pltpu.make_async_copy(recv, own_ref, local_sem.at[0])
    own_out.start()

    def arrived(block, _):
        to_mate(block).wait_recv()
        return 0

    lax.fori_loop(0, BLOCKS, arrived, 0)
    mate_out = pltpu.make_async_copy(mate, mate_ref, local_sem.at[1])
    mate_out.start()

    for k in range(1, 4):
        for m in range(6):
            spread(k, m).wait_send()
        for i in range(1, 4):
            for way in range(2):
                near(k, i, way).wait_send()
    for kind in kinds:
        far(*kind).wait_send()
        onward(*kind).wait_send()
    for copy in [right_a, right_b, left_a, left_b, on_right, on_left] + pairs:
        copy.wait_send()

    def left_here(at, _):
        s = lax.div(at, 4)
        j = lax.div(lax.rem(at, 4), 2)
        copy, apart = message(s, j, lax.rem(at, 2))

        @pl.when(apart > 0)
        def _():
            copy.wait_send()

        to_mate(at).wait_send()
        return 0

    lax.fori_loop(0, BLOCKS, left_here, 0)
    own_out.wait()
    mate_out.wait()
    for copy in others:
        copy.wait()


def front(tokens, gains, mats, out_att, out_conv):
    hbm = pl.BlockSpec(memory_space=pl.ANY)
    vmem = pl.BlockSpec(memory_space=pltpu.VMEM)
    dma = lambda *shape: pltpu.SemaphoreType.DMA(shape)
    return pl.pallas_call(
        front_kernel,
        in_specs=[hbm, vmem] + [hbm] * 8,
        out_specs=[hbm, hbm, vmem, vmem, hbm, hbm],
        out_shape=[
            jax.ShapeDtypeStruct((BLOCKS, MESSAGE, 128), BF16),
            jax.ShapeDtypeStruct((BLOCKS, HALF, 128), BF16),
            jax.ShapeDtypeStruct((SEQS, ROWS, 128), F32),
            jax.ShapeDtypeStruct((SEQS, ROWS, 128), BF16),
            jax.ShapeDtypeStruct(out_att.shape, BF16),
            jax.ShapeDtypeStruct(out_conv.shape, BF16),
        ],
        scratch_shapes=[
            pltpu.VMEM((SEQS, 2, ROWS, 1024), BF16),
            pltpu.VMEM((4, 4, 128, 768), BF16),
            pltpu.VMEM((BLOCKS, MESSAGE, 128), BF16),
            pltpu.VMEM((BLOCKS, MESSAGE, 128), BF16),
            pltpu.VMEM((BLOCKS, HALF, 128), BF16),
            dma(31),
            dma(3, 6), dma(3, 6),
            dma(18), dma(18),
            dma(12), dma(12),
            dma(12), dma(12),
            dma(6), dma(6),
            dma(8), dma(8),
            dma(16), dma(16),
            dma(16), dma(16),
            dma(2), dma(2),
        ],
        compiler_params=pltpu.CompilerParams(
            collective_id=0, has_side_effects=True, vmem_limit_bytes=56 << 20
        ),
        name="front",
    )(tokens, gains, *mats, out_att, out_conv)


def attend_kernel(
    offset_ref, gain_ref, own_ref, mate_ref, out_ref, keys, values, queries, scores, decays, weights, total
):
    half = lax.axis_index("tp")
    lanes = lambda shape: lax.broadcasted_iota(jnp.int32, shape, 1)
    rows = lambda shape: lax.broadcasted_iota(jnp.int32, shape, 0)
    offset = jnp.full((HALF, 128), offset_ref[0] * LOG2E, F32)
    o1, o2, o3 = (part.astype(F32) for part in three_parts(offset))
    lane_q = lanes((HALF, 128))
    offset_row = jnp.where(
        lane_q == 0, -o1, jnp.where(lane_q == 1, -o2, jnp.where(lane_q == 2, -o3, 0.0))
    ).astype(BF16)
    square = (ROWS, HALF)
    source = lax.rem(rows(square), 8) * 48 + rows(square) // 8 - lanes(square)
    permute_own = (source == half * HALF).astype(F32).astype(BF16)
    permute_mate = (source == HALF - half * HALF).astype(F32).astype(BF16)
    shape = (128, 128)
    twice_low = (rows(shape) == lax.rem(lanes(shape), HD)).astype(F32).astype(BF16)
    twice_high = (rows(shape) == lax.rem(lanes(shape), HD) + HD).astype(F32).astype(BF16)
    take_high = (lanes((HD, 128)) == rows((HD, 128)) + HD).astype(F32).astype(BF16)
    ones = (lanes((ROWS, 128)) < 3).astype(F32).astype(BF16)
    for block in range(BLOCKS):
        pair = dot(permute_own, own_ref[block, 0:HALF, :]) + dot(permute_mate, mate_ref[block])
        pair = pair.astype(BF16)
        keys[block * ROWS : (block + 1) * ROWS, 0:128] = dot(pair, twice_low).astype(BF16)
        keys[block * ROWS : (block + 1) * ROWS, 128:256] = ones
        values[block] = dot_nt(take_high, pair).astype(BF16)
        packed = own_ref[block, HALF:MESSAGE, :]
        q = jnp.concatenate((dot(packed, twice_low), dot(packed, twice_high)), axis=0) * (LOG2E / 8)
        q_high = q.astype(BF16).astype(F32)
        at = slice((block % 2) * HALF, (block % 2 + 1) * HALF)
        queries[block // 2, at, 0:128] = jnp.where(lane_q < HD, q_high, q - q_high).astype(BF16)
        queries[block // 2, at, 128:256] = offset_row

    sub = rows((8, ROWS))
    lane = lanes((8, ROWS))
    where_q = lane + half * HALF + jnp.where(lane < HALF, 0, HALF)

    def tile(tile_index, block, carry, ahead, slot):
        begin = pl.multiple_of(block * ROWS, ROWS)
        z_ref, d_ref, w_ref = scores.at[slot], decays.at[slot], weights.at[slot]
        z_ref[...] = dot_nt(keys[pl.ds(begin, ROWS), :], queries[tile_index])
        run = jnp.zeros((8, ROWS), F32)
        for r in reversed(range(48)):
            z = z_ref[8 * r : 8 * r + 8, :]
            soft = jnp.maximum(z, jnp.log2(1.0 + jnp.exp2(jnp.minimum(z, 126.0))))
            if ahead is not None:
                valid = ahead > r
                soft = jnp.where(valid, soft, 0.0)
            run = run + soft
            decay = jnp.exp2(z - run)
            if ahead is not None:
                decay = jnp.where(valid, decay, 0.0)
            d_ref[8 * r : 8 * r + 8, :] = decay
        suffix = run
        for step in (1, 2, 4):
            moved = pltpu.roll(suffix, 8 - step, 0)
            suffix = suffix + jnp.where(sub < 8 - step, moved, 0.0)
        after = jnp.where(sub < 7, pltpu.roll(suffix, 7, 0), 0.0)
        kept = jnp.exp2(-(carry + after))
        for i in range(24):
            both = jnp.concatenate(
                (d_ref[16 * i : 16 * i + 8, :] * kept, d_ref[16 * i + 8 : 16 * i + 16, :] * kept), axis=0
            )
            w_ref[16 * i : 16 * i + 16, :] = both.astype(BF16)
        total[...] += dot(values[block], w_ref[...])
        return carry + jnp.broadcast_to(suffix[0:1], (8, ROWS))

    gain = gain_ref[...]
    gain_lane = lanes((8, 512))
    out_lane = lanes((ROWS, 128))

    def one_tile(m, _):
        total[...] = jnp.zeros_like(total)
        carry = jnp.zeros((8, ROWS), F32)
        carry = tile(m, 2 * m + 1, carry, where_q - ROWS - 48 * sub, 0)
        carry = tile(m, 2 * m, carry, where_q - 48 * sub, 1)

        def before(i, carry):
            at = 2 * (m - 1 - i)
            carry = tile(m, at + 1, carry, None, 0)
            return tile(m, at, carry, None, 1)

        carry = lax.fori_loop(0, m, before, carry)
        attended = total[...]
        squares = jnp.sum(attended * attended, axis=0, keepdims=True)
        parts = [p.astype(F32) for p in three_parts(carry[0:1]) + three_parts(squares)]
        side = jnp.concatenate(parts + [jnp.zeros((HD - 6, ROWS), F32)], axis=0)
        message = jnp.concatenate((attended, side), axis=0).T
        message = message * jnp.where(out_lane < HD, gain, 1.0)
        message = message.astype(BF16)
        out_ref[2 * m] = message[0:HALF]
        out_ref[2 * m + 1] = message[HALF:ROWS]
        return 0

    lax.fori_loop(0, BLOCKS // 2, one_tile, 0)


def attend(own, mate, offset, gain):
    whole = pl.BlockSpec(memory_space=pltpu.VMEM)
    return pl.pallas_call(
        attend_kernel,
        in_specs=[pl.BlockSpec(memory_space=pltpu.SMEM), whole, whole, whole],
        out_specs=whole,
        out_shape=jax.ShapeDtypeStruct((BLOCKS, HALF, 128), BF16),
        scratch_shapes=[
            pltpu.VMEM((BLOCKS * ROWS, 256), BF16),
            pltpu.VMEM((BLOCKS, HD, ROWS), BF16),
            pltpu.VMEM((BLOCKS // 2, ROWS, 256), BF16),
            pltpu.VMEM((2, ROWS, ROWS), F32),
            pltpu.VMEM((2, ROWS, ROWS), F32),
            pltpu.VMEM((2, ROWS, ROWS), BF16),
            pltpu.VMEM((HD, ROWS), F32),
        ],
        compiler_params=pltpu.CompilerParams(vmem_limit_bytes=48 << 20),
        cost_estimate=pl.CostEstimate(
            flops=10_000_000_000, bytes_accessed=3_000_000, transcendentals=30_000_000
        ),
        name="attend",
    )(offset, gain, own, mate)


def per_device(
    tokens,
    in_gain,
    w_query,
    w_key,
    w_value,
    w_outgate,
    w_ingate,
    w_conv_in,
    score_offset,
    conv_taps,
    att_gain,
    conv_gain,
    out_att,
    out_conv,
):
    place = lax.axis_index("sp")
    column = lax.axis_index("fs")
    core = lax.axis_index("tp")
    own, mate, gated, outgate, att_other, conv_other = front(
        tokens[0],
        in_gain.reshape(2, 1024),
        (w_query, w_key, w_value, w_outgate, w_ingate, w_conv_in),
        out_att,
        out_conv,
    )

    number = lax.rem(place, 4)
    both_cores = lax.ppermute(jnp.concatenate((score_offset, att_gain)), "tp", [(0, 1), (1, 0)])
    mine = jnp.where(number // 2 == core, jnp.concatenate((score_offset, att_gain)), both_cores)
    local_head = 2 * column + lax.rem(number, 2)
    offset = lax.dynamic_slice_in_dim(mine, local_head, 1, 0)
    gain = lax.dynamic_slice_in_dim(mine, 8 + local_head * HD, HD, 0)
    gain = jnp.concatenate((gain, jnp.ones((HD,), F32)))[None]
    sent = attend(own, mate, offset, gain)
    back = lax.all_to_all(sent, "sp", 0, 0, tiled=True)

    pairs = [(i, i + 1) for i in range(BLOCKS - 1)]
    before = lax.ppermute(gated[:, ROWS - 2 :], "sp", pairs)
    extended = jnp.concatenate((before, gated), axis=1)
    taps = lax.dynamic_slice_in_dim(conv_taps, column * 128, 128, 1)
    convolved = sum(taps[j] * extended[:, j : j + ROWS] for j in range(3))
    conv_out = outgate.astype(F32) * convolved
    conv_squares = jnp.sum(conv_out * conv_out, axis=2, keepdims=True)
    conv_mine = lax.dynamic_slice_in_dim(conv_gain, column * 128, 128, 0)
    conv_scaled = (conv_out * conv_mine).astype(BF16).reshape(8, HALF, 128)
    pieces = jnp.concatenate(three_parts(conv_squares), axis=2).reshape(8, HALF, 3)
    pieces = jnp.concatenate((pieces, jnp.zeros((8, HALF, 125), BF16)), axis=2)
    conv_home = lax.all_to_all(
        jnp.stack((conv_scaled, pieces), axis=1), ("fs", "tp"), 0, 0, tiled=True
    ).reshape(4, 2, 2, HALF, 128)

    by_head = back.reshape(4, 4, HALF, 128)
    ordered = jnp.stack(
        [jnp.stack([by_head[(s + n) % 4, n] for n in range(4)]) for s in range(SEQS)]
    )
    home = lax.all_to_all(ordered, "fs", 0, 0, tiled=True)
    home = home.reshape(4, 2, 2, HALF, 128)
    extra = home[..., HD : HD + 6].astype(F32)
    kept = extra[..., 0] + extra[..., 1] + extra[..., 2]
    att_sum = jnp.sum(extra[..., 3] + extra[..., 4] + extra[..., 5], axis=(0, 1, 2))
    conv_extra = conv_home[:, :, 1, :, 0:3].astype(F32)
    conv_sum = jnp.sum(conv_extra[..., 0] + conv_extra[..., 1] + conv_extra[..., 2], axis=(0, 1))
    att_scale = lax.rsqrt(att_sum / ATT_WIDTH + epsilon)
    conv_scale = lax.rsqrt(conv_sum / CONV_CH + epsilon)
    att_mat = home[..., :HD].transpose(1, 3, 0, 2, 4).reshape(2, HALF, 512)
    conv_mat = conv_home[:, :, 0].transpose(1, 2, 0, 3).reshape(2, HALF, 512)
    first = core == 0
    near = lambda a: jnp.where(first, a[0], a[1])
    far = lambda a: jnp.where(first, a[1], a[0])
    att_product = dot(near(att_mat), out_att) + dot(far(att_mat), att_other)
    conv_product = dot(near(conv_mat), out_conv) + dot(far(conv_mat), conv_other)
    mixed = att_scale[:, None] * att_product + conv_scale[:, None] * conv_product

    log_mass = jnp.log(2.0 - jnp.exp2(-kept))
    by_core = log_mass.transpose(1, 3, 0, 2).reshape(2, HALF, 8)
    far_rows = lax.ppermute(far(by_core), "tp", [(0, 1), (1, 0)])
    near_rows = near(by_core)
    log_mass = jnp.where(
        first,
        jnp.concatenate((near_rows, far_rows), axis=0),
        jnp.concatenate((far_rows, near_rows), axis=0),
    )
    return (mixed.astype(BF16)[None], log_mass[None])


def solution(mesh):
    return jax.shard_map(
        per_device,
        mesh=mesh,
        in_specs=(
            P("fs", "sp", "tp"),
            P(),
            P("fs", "tp"),
            P("fs", "tp"),
            P("fs", "tp"),
            P("fs", "tp"),
            P("fs", "tp"),
            P("fs", "tp"),
            P("tp"),
            P(None, "tp"),
            P("tp"),
            P("tp"),
            P("tp", None),
            P("tp", None),
        ),
        out_specs=(P("fs", ("sp", "tp"), None), P("fs", "sp", "tp")),
        check_vma=False,
    )
```

```python
import functools

import jax
import jax.numpy as jnp
from jax import lax
from jax.experimental import pallas as pl
from jax.experimental.pallas import tpu as pltpu
from jax.sharding import PartitionSpec as P

D = 2048
CONV_CH = 1024
ATT_WIDTH = 1024
SEQS = 4
ROWS = 384
HALF = 192
BLOCKS = 16
HD = 64
MESSAGE = HALF + HALF // 2
epsilon = 1e-06
LOG2E = 1.4426950408889634
F32 = jnp.float32
BF16 = jnp.bfloat16


def dot(a, b):
    return jnp.dot(a, b, preferred_element_type=F32)


def dot_nt(a, b):
    return lax.dot_general(a, b, (((1,), (1,)), ((), ())), preferred_element_type=F32)


def three_parts(x):
    a = x.astype(BF16)
    rest = x - a.astype(F32)
    b = rest.astype(BF16)
    return a, b, (rest - b.astype(F32)).astype(BF16)


MESH = pl.DeviceIdType.MESH
LEFT, RIGHT = slice(0, 384), slice(384, 768)


def mod4(value):
    return lax.rem(value + 8, 4)


def front_kernel(
    tokens_ref,
    params_hbm,
    params_ref,
    wq_ref,
    wk_ref,
    wv_ref,
    wo_ref,
    wi_ref,
    wc_ref,
    att_ref,
    conv_ref,
    own_ref,
    mate_ref,
    branch_ref,
    params_other_ref,
    att_other_ref,
    conv_other_ref,
    tok,
    wts,
    msg,
    recv,
    mate,
    gated,
    outgate,
    branch_out,
    branch_in,
    local_sem,
    spread_send,
    spread_recv,
    near_send,
    near_recv,
    far_send,
    far_recv,
    pass_send,
    pass_recv,
    tok_send,
    tok_recv,
    pair_send,
    pair_recv,
    msg_send,
    msg_recv,
    mate_send,
    mate_recv,
    other_send,
    other_recv,
    halo_send,
    halo_recv,
    branch_send,
    branch_recv,
):
    place, x, core = lax.axis_index("sp"), lax.axis_index("fs"), lax.axis_index("tp")
    y, z = lax.rem(place, 4), lax.div(place, 4)
    sibling = (place, x, 1 - core)
    mats = (wq_ref, wk_ref, wv_ref, wo_ref, wi_ref, wc_ref)

    def remote(src, dst, send, recv_sem, device):
        return pltpu.make_async_remote_copy(
            src_ref=src, dst_ref=dst, send_sem=send, recv_sem=recv_sem, device_id=device, device_id_type=MESH
        )

    own_tokens = pltpu.make_async_copy(tokens_ref, tok.at[x, core], local_sem.at[6])
    own_tokens.start()
    own_weights = []
    for m in range(6):
        for part in range(4):
            own_weights.append(
                pltpu.make_async_copy(
                    mats[m].at[pl.ds(part * 128, 128), pl.ds(pl.multiple_of(x * 128, 128), 128)],
                    wts.at[x, part, :, m * 128 : (m + 1) * 128],
                    local_sem.at[7 + 4 * m + part],
                )
            )
    for copy in own_weights:
        copy.start()

    barrier = pltpu.get_barrier_semaphore()
    for k in range(1, 4):
        pl.semaphore_signal(barrier, inc=1, device_id=(place, mod4(x + k), core), device_id_type=MESH)
    pl.semaphore_signal(barrier, inc=1, device_id=sibling, device_id_type=MESH)

    def greet(k, _):
        there = lax.rem(place + k, BLOCKS)
        pl.semaphore_signal(barrier, inc=1, device_id=(there, x, core), device_id_type=MESH)
        pl.semaphore_signal(barrier, inc=1, device_id=(there, x, 1 - core), device_id_type=MESH)
        return 0

    lax.fori_loop(1, BLOCKS, greet, 0)
    pl.semaphore_wait(barrier, 34)

    rows_at = pl.multiple_of(place * 32, 32)

    def spread(k, m):
        there = mod4(x + k)
        return remote(
            mats[m].at[pl.ds(rows_at, 32), pl.ds(pl.multiple_of(there * 128, 128), 128)],
            wts.at[x, z, pl.ds(pl.multiple_of(y * 32, 32), 32), m * 128 : (m + 1) * 128],
            spread_send.at[k - 1, m],
            spread_recv.at[k - 1, m],
            (place, there, core),
        )

    for k in range(1, 4):
        for m in range(6):
            spread(k, m).start()

    own_tokens.wait()
    top, bottom = pl.ds(0, HALF), pl.ds(HALF, HALF)

    def hop(slot, f, rows, by):
        piece = tok.at[f, core, rows]
        return remote(piece, piece, tok_send.at[slot], tok_recv.at[slot], (place, mod4(x + by), core))

    def pair(slot, f, rows):
        piece = tok.at[f, core, rows]
        return remote(piece, piece, pair_send.at[slot], pair_recv.at[slot], sibling)

    right_a, right_b = hop(0, x, top, 1), hop(1, x, bottom, 1)
    left_b, left_a = hop(2, x, bottom, -1), hop(3, x, top, -1)
    before, after, across = mod4(x - 1), mod4(x + 1), mod4(x + 2)
    on_right, on_left = hop(4, before, top, 1), hop(5, after, bottom, -1)
    for copy in (right_a, left_b, right_b, left_a):
        copy.start()
    pairs = [
        pair(0, x, top),
        pair(1, x, bottom),
        pair(2, before, top),
        pair(3, after, bottom),
        pair(4, before, bottom),
        pair(5, after, top),
        pair(6, across, top),
        pair(7, across, bottom),
    ]
    pairs[0].start()
    pairs[1].start()

    for k in range(1, 4):
        for m in range(6):
            spread(k, m).wait_recv()

    my_rows = pl.ds(pl.multiple_of(y * 32, 32), 32)

    def near(k, i, way):
        f = mod4(x + i)
        piece = wts.at[f, z, my_rows, (LEFT, RIGHT)[way]]
        there = (z * 4 + mod4(y + k), x, core) if way == 0 else (mod4(z + k) * 4 + y, x, core)
        at = (3 * way + k - 1) * 3 + i - 1
        return remote(piece, piece, near_send.at[at], near_recv.at[at], there)

    for k in range(1, 4):
        for i in range(1, 4):
            for way in range(2):
                near(k, i, way).start()
    for k in range(1, 4):
        for i in range(1, 4):
            for way in range(2):
                near(k, i, way).wait_recv()

    def far(by, i, way):
        f = mod4(x + i)
        if way == 0:
            piece, there = wts.at[f, z, :, LEFT], (mod4(z + by) * 4 + y, x, core)
        else:
            piece, there = wts.at[f, :, my_rows, RIGHT], (z * 4 + mod4(y + by), x, core)
        at = (2 * way + (by + 1) // 2) * 3 + i - 1
        return remote(piece, piece, far_send.at[at], far_recv.at[at], there)

    def onward(by, i, way):
        f = mod4(x + i)
        start = 0 if by == 1 else 1
        if way == 0:
            piece = wts.at[f, mod4(z - by), 64 * start : 64 * start + 64, LEFT]
            there = (mod4(z + by) * 4 + y, x, core)
        else:
            rows = pl.ds(pl.multiple_of(mod4(y - by) * 32, 32), 32)
            piece = wts.at[f, 2 * start : 2 * start + 2, rows, RIGHT]
            there = (z * 4 + mod4(y + by), x, core)
        at = (2 * way + (by + 1) // 2) * 3 + i - 1
        return remote(piece, piece, pass_send.at[at], pass_recv.at[at], there)

    kinds = [(by, i, way) for i in range(1, 4) for by in (1, -1) for way in range(2)]
    for kind in kinds:
        far(*kind).start()
    right_a.wait_recv()
    on_right.start()
    pairs[2].start()
    left_b.wait_recv()
    on_left.start()
    pairs[3].start()
    for kind in kinds:
        far(*kind).wait_recv()
        onward(*kind).start()
    others = [
        remote(att_ref, att_other_ref, other_send.at[0], other_recv.at[0], sibling),
        remote(conv_ref, conv_other_ref, other_send.at[1], other_recv.at[1], sibling),
        remote(params_hbm, params_other_ref, other_send.at[2], other_recv.at[2], sibling),
    ]
    for copy in own_weights:
        copy.wait()
    for kind in kinds:
        onward(*kind).wait_recv()

    def message(s, j, half):
        number = 2 * core + j
        there = mod4(s + number) * 4 + number
        at = 4 * s + 2 * j + half
        return remote(
            msg.at[at], recv.at[place], msg_send.at[at], msg_recv.at[place], (there, x, half)
        ), lax.abs(there - place) + lax.abs(half - core)

    def halo(s):
        return remote(
            gated.at[s, ROWS : ROWS + 8],
            gated.at[s, 0:8],
            halo_send.at[s],
            halo_recv.at[s],
            (lax.rem(place + 1, BLOCKS), x, core),
        )

    def to_home(at):
        s, half = lax.div(at, 2), lax.rem(at, 2)
        mine = 2 * x + core
        return remote(
            branch_out.at[at], branch_in.at[mine], branch_send.at[at], branch_recv.at[mine], (place, s, half)
        ), lax.abs(s - x) + lax.abs(half - core)

    def step(i, _):
        s = mod4(x + i + lax.div(i, 2) - 2 * lax.div(i, 3))

        @pl.when(i == 0)
        def _():
            pairs[0].wait_recv()
            pairs[1].wait_recv()

        @pl.when(i == 1)
        def _():
            right_b.wait_recv()
            pairs[4].start()
            left_a.wait_recv()
            pairs[5].start()
            pairs[3].wait_recv()
            pairs[5].wait_recv()

        @pl.when(i == 2)
        def _():
            pairs[2].wait_recv()
            pairs[4].wait_recv()

        @pl.when(i == 3)
        def _():
            on_right.wait_recv()
            pairs[6].start()
            on_left.wait_recv()
            pairs[7].start()
            for copy in others:
                copy.start()
            pairs[6].wait_recv()
            pairs[7].wait_recv()

        low = tok[s, 0].astype(F32)
        high = tok[s, 1].astype(F32)
        squares = jnp.sum(low * low, axis=1, keepdims=True) + jnp.sum(high * high, axis=1, keepdims=True)
        scale = lax.rsqrt(squares / D + epsilon)
        total = dot((low * params_ref[0:1, :]).astype(BF16), wts[0:2].reshape(1024, 768)) + dot(
            (high * params_ref[1:2, :]).astype(BF16), wts[2:4].reshape(1024, 768)
        )
        out = (total * scale).astype(BF16)
        query, key, value = out[:, 0:128], out[:, 128:256], out[:, 256:384]
        for j in range(2):
            mine = slice(j * HD, (j + 1) * HD)
            both = jnp.concatenate((key[:, mine], value[:, mine]), axis=1)
            for half in range(2):
                r = half * HALF
                folded = jnp.concatenate((query[r : r + 96, mine], query[r + 96 : r + HALF, mine]), axis=1)
                msg[4 * s + 2 * j + half, 0:HALF, :] = both[r : r + HALF]
                msg[4 * s + 2 * j + half, HALF : HALF + 96, :] = folded
        outgate[s] = out[:, 384:512]
        gated[s, 8 : ROWS + 8, :] = out[:, 512:640].astype(F32) * out[:, 640:768].astype(F32)

        @pl.when(place < BLOCKS - 1)
        def _():
            halo(s).start()

        @pl.when(place == 0)
        def _():
            gated[s, 0:8, :] = jnp.zeros((8, 128), F32)

        for j in range(2):
            for half in range(2):
                copy, apart = message(s, j, half)

                @pl.when(apart > 0)
                def _():
                    copy.start()

                @pl.when(apart == 0)
                def _():
                    recv[place] = msg[4 * s + 2 * j + half]

        return 0

    lax.fori_loop(0, 4, step, 0)

    columns = pl.ds(pl.multiple_of(x * 128, 128), 128)

    def convolve(s, _):
        @pl.when(place > 0)
        def _():
            halo(s).wait_recv()

        convolved = sum(
            params_ref[4 + t : 5 + t, columns] * gated[s, 6 + t : 6 + t + ROWS, :] for t in range(3)
        )
        branch = (outgate[s].astype(F32) * convolved).astype(BF16)
        branch_out[2 * s] = branch[0:HALF]
        branch_out[2 * s + 1] = branch[HALF:ROWS]
        for half in range(2):
            copy, apart = to_home(2 * s + half)

            @pl.when(apart > 0)
            def _():
                copy.start()

            @pl.when(apart == 0)
            def _():
                branch_in[2 * x + core] = branch[half * HALF : (half + 1) * HALF]

        return 0

    lax.fori_loop(0, SEQS, convolve, 0)

    def to_mate(block):
        return remote(
            recv.at[block, 0:HALF], mate.at[block], mate_send.at[block], mate_recv.at[block], sibling
        )

    source_core = lax.div(y, 2)

    def arrive(k, _):
        block = lax.rem(place + k, BLOCKS)

        @pl.when(k + lax.abs(source_core - core) > 0)
        def _():
            remote(
                msg.at[0], recv.at[block], msg_send.at[0], msg_recv.at[block], (block, x, source_core)
            ).wait_recv()

        to_mate(block).start()
        return 0

    lax.fori_loop(0, BLOCKS, arrive, 0)
    own_out = pltpu.make_async_copy(recv, own_ref, local_sem.at[0])
    own_out.start()

    def arrived(block, _):
        to_mate(block).wait_recv()
        return 0

    lax.fori_loop(0, BLOCKS, arrived, 0)

    def branch_arrived(k, _):
        there = lax.rem(2 * x + core + k, 8)
        remote(
            branch_out.at[0],
            branch_in.at[there],
            branch_send.at[0],
            branch_recv.at[there],
            (place, lax.div(there, 2), lax.rem(there, 2)),
        ).wait_recv()
        return 0

    lax.fori_loop(1, 8, branch_arrived, 0)
    home_out = pltpu.make_async_copy(branch_in, branch_ref, local_sem.at[2])
    home_out.start()
    mate_out = pltpu.make_async_copy(mate, mate_ref, local_sem.at[1])
    mate_out.start()

    for k in range(1, 4):
        for m in range(6):
            spread(k, m).wait_send()
        for i in range(1, 4):
            for way in range(2):
                near(k, i, way).wait_send()
    for kind in kinds:
        far(*kind).wait_send()
        onward(*kind).wait_send()
    for copy in [right_a, right_b, left_a, left_b, on_right, on_left] + pairs:
        copy.wait_send()

    def left_here(at, _):
        s = lax.div(at, 4)
        j = lax.div(lax.rem(at, 4), 2)
        copy, apart = message(s, j, lax.rem(at, 2))

        @pl.when(apart > 0)
        def _():
            copy.wait_send()

        to_mate(at).wait_send()
        return 0

    lax.fori_loop(0, BLOCKS, left_here, 0)

    def branch_left(at, _):
        copy, apart = to_home(at)

        @pl.when(apart > 0)
        def _():
            copy.wait_send()

        return 0

    lax.fori_loop(0, 8, branch_left, 0)

    @pl.when(place < BLOCKS - 1)
    def _():
        for s in range(SEQS):
            halo(s).wait_send()

    home_out.wait()
    own_out.wait()
    mate_out.wait()
    for copy in others:
        copy.wait()


def front(tokens, params, mats, out_att, out_conv):
    hbm = pl.BlockSpec(memory_space=pl.ANY)
    vmem = pl.BlockSpec(memory_space=pltpu.VMEM)
    dma = lambda *shape: pltpu.SemaphoreType.DMA(shape)
    return pl.pallas_call(
        front_kernel,
        in_specs=[hbm, hbm, vmem] + [hbm] * 8,
        out_specs=[hbm] * 6,
        out_shape=[
            jax.ShapeDtypeStruct((BLOCKS, MESSAGE, 128), BF16),
            jax.ShapeDtypeStruct((BLOCKS, HALF, 128), BF16),
            jax.ShapeDtypeStruct((8, HALF, 128), BF16),
            jax.ShapeDtypeStruct(params.shape, F32),
            jax.ShapeDtypeStruct(out_att.shape, BF16),
            jax.ShapeDtypeStruct(out_conv.shape, BF16),
        ],
        scratch_shapes=[
            pltpu.VMEM((SEQS, 2, ROWS, 1024), BF16),
            pltpu.VMEM((4, 4, 128, 768), BF16),
            pltpu.VMEM((BLOCKS, MESSAGE, 128), BF16),
            pltpu.VMEM((BLOCKS, MESSAGE, 128), BF16),
            pltpu.VMEM((BLOCKS, HALF, 128), BF16),
            pltpu.VMEM((SEQS, ROWS + 8, 128), F32),
            pltpu.VMEM((SEQS, ROWS, 128), BF16),
            pltpu.VMEM((8, HALF, 128), BF16),
            pltpu.VMEM((8, HALF, 128), BF16),
            dma(31),
            dma(3, 6), dma(3, 6),
            dma(18), dma(18),
            dma(12), dma(12),
            dma(12), dma(12),
            dma(6), dma(6),
            dma(8), dma(8),
            dma(16), dma(16),
            dma(16), dma(16),
            dma(3), dma(3),
            dma(4), dma(4),
            dma(8), dma(8),
        ],
        compiler_params=pltpu.CompilerParams(
            collective_id=0, has_side_effects=True, vmem_limit_bytes=56 << 20
        ),
        name="front",
    )(tokens, params, params, *mats, out_att, out_conv)


def attend_kernel(
    offset_ref,
    own_ref,
    mate_ref,
    branch_ref,
    gain_ref,
    gain_other_ref,
    att_ref,
    att_other_ref,
    conv_ref,
    conv_other_ref,
    mixed_ref,
    mass_ref,
    keys,
    values,
    queries,
    scores,
    decays,
    weights,
    total,
    att_out,
    att_in,
    mass_out,
    mass_in,
    att_weights,
    conv_weights,
    matrix,
    gains,
    att_send,
    att_recv,
    mass_send,
    mass_recv,
    local_sem,
):
    place, x, half = lax.axis_index("sp"), lax.axis_index("fs"), lax.axis_index("tp")
    number, row = lax.rem(place, 4), lax.div(place, 4)
    seq = mod4(row - number)

    barrier = pltpu.get_barrier_semaphore()

    def greet(k, _):
        n = lax.rem(k, 4)
        there, column = mod4(x + n) * 4 + n, lax.div(k, 4)
        for core in range(2):
            @pl.when(lax.abs(there - place) + lax.abs(column - x) + lax.abs(core - half) > 0)
            def _():
                pl.semaphore_signal(barrier, inc=1, device_id=(there, column, core), device_id_type=MESH)

        return 0

    lax.fori_loop(0, 16, greet, 0)
    fetches = [
        pltpu.make_async_copy(src, dst, local_sem.at[i])
        for i, (src, dst) in enumerate(
            [
                (att_ref, att_weights.at[half]),
                (att_other_ref, att_weights.at[1 - half]),
                (conv_ref, conv_weights.at[half]),
                (conv_other_ref, conv_weights.at[1 - half]),
                (gain_ref, gains.at[half]),
                (gain_other_ref, gains.at[1 - half]),
            ]
        )
    ]
    for copy in fetches:
        copy.start()

    def remote(src, dst, send, recv, device):
        return pltpu.make_async_remote_copy(
            src_ref=src, dst_ref=dst, send_sem=send, recv_sem=recv, device_id=device, device_id_type=MESH
        )

    def att_home(block):
        at = 4 * x + number
        apart = lax.abs(block - place) + lax.abs(seq - x)
        return remote(
            att_out.at[block], att_in.at[at], att_send.at[block], att_recv.at[at], (block, seq, half)
        ), apart

    def mass_home(block):
        at = 4 * x + 2 * lax.rem(number, 2) + half
        core = lax.div(number, 2)
        apart = lax.abs(block - place) + lax.abs(seq - x) + lax.abs(core - half)
        return remote(
            mass_out.at[block], mass_in.at[at], mass_send.at[block], mass_recv.at[at], (block, seq, core)
        ), apart

    lanes = lambda shape: lax.broadcasted_iota(jnp.int32, shape, 1)
    rows = lambda shape: lax.broadcasted_iota(jnp.int32, shape, 0)
    offset = jnp.full((HALF, 128), offset_ref[0] * LOG2E, F32)
    o1, o2, o3 = (part.astype(F32) for part in three_parts(offset))
    lane_q = lanes((HALF, 128))
    offset_row = jnp.where(
        lane_q == 0, -o1, jnp.where(lane_q == 1, -o2, jnp.where(lane_q == 2, -o3, 0.0))
    ).astype(BF16)
    square = (ROWS, HALF)
    source = lax.rem(rows(square), 8) * 48 + rows(square) // 8 - lanes(square)
    permute_own = (source == half * HALF).astype(F32).astype(BF16)
    permute_mate = (source == HALF - half * HALF).astype(F32).astype(BF16)
    shape = (128, 128)
    twice_low = (rows(shape) == lax.rem(lanes(shape), HD)).astype(F32).astype(BF16)
    twice_high = (rows(shape) == lax.rem(lanes(shape), HD) + HD).astype(F32).astype(BF16)
    take_high = (lanes((HD, 128)) == rows((HD, 128)) + HD).astype(F32).astype(BF16)
    ones = (lanes((ROWS, 128)) < 3).astype(F32).astype(BF16)
    for block in range(BLOCKS):
        pair = dot(permute_own, own_ref[block, 0:HALF, :]) + dot(permute_mate, mate_ref[block])
        pair = pair.astype(BF16)
        keys[block * ROWS : (block + 1) * ROWS, 0:128] = dot(pair, twice_low).astype(BF16)
        keys[block * ROWS : (block + 1) * ROWS, 128:256] = ones
        values[block] = dot_nt(take_high, pair).astype(BF16)
        packed = own_ref[block, HALF:MESSAGE, :]
        q = jnp.concatenate((dot(packed, twice_low), dot(packed, twice_high)), axis=0) * (LOG2E / 8)
        q_high = q.astype(BF16).astype(F32)
        at = slice((block % 2) * HALF, (block % 2 + 1) * HALF)
        queries[block // 2, at, 0:128] = jnp.where(lane_q < HD, q_high, q - q_high).astype(BF16)
        queries[block // 2, at, 128:256] = offset_row

    pl.semaphore_wait(barrier, 31 + lax.min(lax.abs(seq - x), 1))

    sub = rows((8, ROWS))
    lane = lanes((8, ROWS))
    where_q = lane + half * HALF + jnp.where(lane < HALF, 0, HALF)

    def tile(tile_index, block, carry, ahead, slot):
        begin = pl.multiple_of(block * ROWS, ROWS)
        z_ref, d_ref, w_ref = scores.at[slot], decays.at[slot], weights.at[slot]
        z_ref[...] = dot_nt(keys[pl.ds(begin, ROWS), :], queries[tile_index])
        run = jnp.zeros((8, ROWS), F32)
        for r in reversed(range(48)):
            z = z_ref[8 * r : 8 * r + 8, :]
            soft = jnp.maximum(z, jnp.log2(1.0 + jnp.exp2(jnp.minimum(z, 126.0))))
            if ahead is not None:
                valid = ahead > r
                soft = jnp.where(valid, soft, 0.0)
            run = run + soft
            decay = jnp.exp2(z - run)
            if ahead is not None:
                decay = jnp.where(valid, decay, 0.0)
            d_ref[8 * r : 8 * r + 8, :] = decay
        suffix = run
        for step in (1, 2, 4):
            moved = pltpu.roll(suffix, 8 - step, 0)
            suffix = suffix + jnp.where(sub < 8 - step, moved, 0.0)
        after = jnp.where(sub < 7, pltpu.roll(suffix, 7, 0), 0.0)
        kept = jnp.exp2(-(carry + after))
        for i in range(24):
            both = jnp.concatenate(
                (d_ref[16 * i : 16 * i + 8, :] * kept, d_ref[16 * i + 8 : 16 * i + 16, :] * kept), axis=0
            )
            w_ref[16 * i : 16 * i + 16, :] = both.astype(BF16)
        total[...] += dot(values[block], w_ref[...])
        return carry + jnp.broadcast_to(suffix[0:1], (8, ROWS))

    def one_tile(step, _):
        m = BLOCKS // 2 - 1 - step
        total[...] = jnp.zeros_like(total)
        carry = jnp.zeros((8, ROWS), F32)
        carry = tile(m, 2 * m + 1, carry, where_q - ROWS - 48 * sub, 0)
        carry = tile(m, 2 * m, carry, where_q - 48 * sub, 1)

        def before(i, carry):
            at = 2 * (m - 1 - i)
            carry = tile(m, at + 1, carry, None, 0)
            return tile(m, at, carry, None, 1)

        carry = lax.fori_loop(0, m, before, carry)
        attended = total[...]
        attended = jnp.concatenate((attended, attended), axis=0).T
        for part in range(2):
            block = 2 * m + part
            r = part * HALF
            folded = jnp.where(lanes((96, 128)) < HD, attended[r : r + 96], attended[r + 96 : r + HALF])
            folded = folded.astype(BF16)
            mass = carry[:, r : r + HALF]
            att_out[block] = folded
            mass_out[block, :, 0:HALF] = mass
            copy, apart = att_home(block)

            @pl.when(apart > 0)
            def _():
                copy.start()

            @pl.when(apart == 0)
            def _():
                att_in[4 * x + number] = folded

            mass_copy, mass_apart = mass_home(block)

            @pl.when(mass_apart > 0)
            def _():
                mass_copy.start()

            @pl.when(mass_apart == 0)
            def _():
                mass_in[4 * x + 2 * lax.rem(number, 2) + half, :, 0:HALF] = mass

        return 0

    lax.fori_loop(0, BLOCKS // 2, one_tile, 0)

    for copy in fetches:
        copy.wait()

    def branch_product(store, row_gain, projection, load):
        squares = jnp.zeros((HALF, 128), F32)
        for core in range(2):
            for part in range(4):
                piece = load(core, part)
                squares = squares + piece * piece
                gain = gains[core, 2:3, row_gain + 128 * part : row_gain + 128 * part + 128]
                at = 512 * core + 128 * part
                store[:, at : at + 128] = (piece * gain).astype(BF16)
        scale = lax.rsqrt(jnp.sum(squares, axis=1, keepdims=True) / ATT_WIDTH + epsilon)
        return scale * dot(store[...], projection[...].reshape(1024, D))

    mixed = branch_product(
        matrix.at[0], 512, conv_weights, lambda core, part: branch_ref[2 * part + core].astype(F32)
    )

    def landed(at, _):
        column, n = lax.div(at, 4), lax.rem(at, 4)
        there = mod4(x + n) * 4 + n
        apart = lax.abs(there - place) + lax.abs(column - x)

        @pl.when(apart > 0)
        def _():
            remote(
                att_out.at[0], att_in.at[at], att_send.at[0], att_recv.at[at], (there, column, half)
            ).wait_recv()

        n = 2 * half + lax.div(n, 2)
        core = lax.rem(at, 2)
        there = mod4(x + n) * 4 + n
        apart = lax.abs(there - place) + lax.abs(column - x) + lax.abs(core - half)

        @pl.when(apart > 0)
        def _():
            remote(
                mass_out.at[0], mass_in.at[at], mass_send.at[0], mass_recv.at[at], (there, column, core)
            ).wait_recv()

        return 0

    lax.fori_loop(0, 16, landed, 0)

    def heads(core, part):
        a = att_in[4 * part + 2 * core].astype(F32)
        b = att_in[4 * part + 2 * core + 1].astype(F32)
        low = lanes((96, 128)) < HD
        upper = jnp.where(low, a, pltpu.roll(b, HD, 1))
        lower = jnp.where(low, pltpu.roll(a, HD, 1), b)
        return jnp.concatenate((upper, lower), axis=0)

    mixed = mixed + branch_product(matrix.at[1], 0, att_weights, heads)
    mixed_ref[0] = mixed.astype(BF16)
    for part in range(2):
        kept = jnp.concatenate([mass_in[2 * n + part, 0:1, :] for n in range(8)], axis=0)
        mass = jnp.log(2.0 - jnp.exp2(-kept)).T
        mass_ref[0, part * HALF : (part + 1) * HALF, :] = mass[0:HALF]

    def left(block, _):
        copy, apart = att_home(block)

        @pl.when(apart > 0)
        def _():
            copy.wait_send()

        mass_copy, mass_apart = mass_home(block)

        @pl.when(mass_apart > 0)
        def _():
            mass_copy.wait_send()

        return 0

    lax.fori_loop(0, BLOCKS, left, 0)


def attend(offset, own, mate, branch, params, params_other, att, att_other, conv, conv_other):
    whole = pl.BlockSpec(memory_space=pltpu.VMEM)
    hbm = pl.BlockSpec(memory_space=pl.ANY)
    dma = lambda *shape: pltpu.SemaphoreType.DMA(shape)
    return pl.pallas_call(
        attend_kernel,
        in_specs=[pl.BlockSpec(memory_space=pltpu.SMEM), whole, whole, whole] + [hbm] * 6,
        out_specs=[whole, whole],
        out_shape=[
            jax.ShapeDtypeStruct((1, HALF, D), BF16),
            jax.ShapeDtypeStruct((1, ROWS, 8), F32),
        ],
        scratch_shapes=[
            pltpu.VMEM((BLOCKS * ROWS, 256), BF16),
            pltpu.VMEM((BLOCKS, HD, ROWS), BF16),
            pltpu.VMEM((BLOCKS // 2, ROWS, 256), BF16),
            pltpu.VMEM((2, ROWS, ROWS), F32),
            pltpu.VMEM((2, ROWS, ROWS), F32),
            pltpu.VMEM((2, ROWS, ROWS), BF16),
            pltpu.VMEM((HD, ROWS), F32),
            pltpu.VMEM((BLOCKS, 96, 128), BF16),
            pltpu.VMEM((BLOCKS, 96, 128), BF16),
            pltpu.VMEM((BLOCKS, 8, 256), F32),
            pltpu.VMEM((BLOCKS, 8, 256), F32),
            pltpu.VMEM((2, 512, D), BF16),
            pltpu.VMEM((2, 512, D), BF16),
            pltpu.VMEM((2, HALF, 1024), BF16),
            pltpu.VMEM((2, 8, 1024), F32),
            dma(16), dma(16), dma(16), dma(16), dma(6),
        ],
        compiler_params=pltpu.CompilerParams(
            collective_id=1, has_side_effects=True, vmem_limit_bytes=56 << 20
        ),
        name="attend",
    )(offset, own, mate, branch, params, params_other, att, att_other, conv, conv_other)


def per_device(
    tokens,
    in_gain,
    w_query,
    w_key,
    w_value,
    w_outgate,
    w_ingate,
    w_conv_in,
    score_offset,
    conv_taps,
    att_gain,
    conv_gain,
    out_att,
    out_conv,
):
    wide = lambda a: jnp.pad(a, ((0, 0), (0, 1024 - a.shape[1])))
    params = jnp.concatenate(
        (
            in_gain.reshape(2, 1024),
            jnp.concatenate((att_gain, conv_gain))[None],
            wide(score_offset[None]),
            wide(conv_taps),
            jnp.zeros((1, 1024), F32),
        ),
        axis=0,
    )
    own, mate, branch, params_other, att_other, conv_other = front(
        tokens[0], params, (w_query, w_key, w_value, w_outgate, w_ingate, w_conv_in), out_att, out_conv
    )
    number = lax.rem(lax.axis_index("sp"), 4)
    offsets = jnp.where(number // 2 == lax.axis_index("tp"), score_offset, params_other[3, :8])
    offset = lax.dynamic_slice_in_dim(offsets, 2 * lax.axis_index("fs") + lax.rem(number, 2), 1, 0)
    return tuple(
        attend(
            offset, own, mate, branch, params, params_other, out_att, att_other, out_conv, conv_other
        )
    )


def solution(mesh):
    return jax.shard_map(
        per_device,
        mesh=mesh,
        in_specs=(
            P("fs", "sp", "tp"),
            P(),
            P("fs", "tp"),
            P("fs", "tp"),
            P("fs", "tp"),
            P("fs", "tp"),
            P("fs", "tp"),
            P("fs", "tp"),
            P("tp"),
            P(None, "tp"),
            P("tp"),
            P("tp"),
            P("tp", None),
            P("tp", None),
        ),
        out_specs=(P("fs", ("sp", "tp"), None), P("fs", "sp", "tp")),
        check_vma=False,
    )
```

```python
import functools

import jax
import jax.numpy as jnp
from jax import lax
from jax.experimental import pallas as pl
from jax.experimental.pallas import tpu as pltpu
from jax.sharding import PartitionSpec as P

D = 2048
CONV_CH = 1024
ATT_WIDTH = 1024
SEQS = 4
ROWS = 384
HALF = 192
BLOCKS = 16
HD = 64
MESSAGE = HALF + HALF // 2
epsilon = 1e-06
LOG2E = 1.4426950408889634
F32 = jnp.float32
BF16 = jnp.bfloat16


def dot(a, b):
    return jnp.dot(a, b, preferred_element_type=F32)


def dot_nt(a, b):
    return lax.dot_general(a, b, (((1,), (1,)), ((), ())), preferred_element_type=F32)


def three_parts(x):
    a = x.astype(BF16)
    rest = x - a.astype(F32)
    b = rest.astype(BF16)
    return a, b, (rest - b.astype(F32)).astype(BF16)


MESH = pl.DeviceIdType.MESH
LEFT, RIGHT = slice(0, 384), slice(384, 768)


def mod4(value):
    return lax.rem(value + 8, 4)


def front_kernel(
    tokens_ref,
    params_hbm,
    params_ref,
    wq_ref,
    wk_ref,
    wv_ref,
    wo_ref,
    wi_ref,
    wc_ref,
    att_ref,
    conv_ref,
    own_ref,
    mate_ref,
    branch_ref,
    params_other_ref,
    att_other_ref,
    conv_other_ref,
    tok,
    wts,
    msg,
    recv,
    mate,
    gated,
    outgate,
    branch_out,
    branch_in,
    local_sem,
    spread_send,
    spread_recv,
    near_send,
    near_recv,
    far_send,
    far_recv,
    pass_send,
    pass_recv,
    tok_send,
    tok_recv,
    pair_send,
    pair_recv,
    msg_send,
    msg_recv,
    mate_send,
    mate_recv,
    other_send,
    other_recv,
    halo_send,
    halo_recv,
    branch_send,
    branch_recv,
):
    place, x, core = lax.axis_index("sp"), lax.axis_index("fs"), lax.axis_index("tp")
    y, z = lax.rem(place, 4), lax.div(place, 4)
    sibling = (place, x, 1 - core)
    mats = (wq_ref, wk_ref, wv_ref, wo_ref, wi_ref, wc_ref)

    def remote(src, dst, send, recv_sem, device):
        return pltpu.make_async_remote_copy(
            src_ref=src, dst_ref=dst, send_sem=send, recv_sem=recv_sem, device_id=device, device_id_type=MESH
        )

    own_tokens = pltpu.make_async_copy(tokens_ref, tok.at[x, core], local_sem.at[6])
    own_tokens.start()
    own_weights = []
    for m in range(6):
        for part in range(4):
            own_weights.append(
                pltpu.make_async_copy(
                    mats[m].at[pl.ds(part * 128, 128), pl.ds(pl.multiple_of(x * 128, 128), 128)],
                    wts.at[x, part, :, m * 128 : (m + 1) * 128],
                    local_sem.at[7 + 4 * m + part],
                )
            )
    for copy in own_weights:
        copy.start()

    barrier = pltpu.get_barrier_semaphore()
    for k in range(1, 4):
        pl.semaphore_signal(barrier, inc=1, device_id=(place, mod4(x + k), core), device_id_type=MESH)
    pl.semaphore_signal(barrier, inc=1, device_id=sibling, device_id_type=MESH)

    def greet(k, _):
        there = lax.rem(place + k, BLOCKS)
        pl.semaphore_signal(barrier, inc=1, device_id=(there, x, core), device_id_type=MESH)
        pl.semaphore_signal(barrier, inc=1, device_id=(there, x, 1 - core), device_id_type=MESH)
        return 0

    lax.fori_loop(1, BLOCKS, greet, 0)
    pl.semaphore_wait(barrier, 34)

    rows_at = pl.multiple_of(place * 32, 32)

    def spread(k, m):
        there = mod4(x + k)
        return remote(
            mats[m].at[pl.ds(rows_at, 32), pl.ds(pl.multiple_of(there * 128, 128), 128)],
            wts.at[x, z, pl.ds(pl.multiple_of(y * 32, 32), 32), m * 128 : (m + 1) * 128],
            spread_send.at[k - 1, m],
            spread_recv.at[k - 1, m],
            (place, there, core),
        )

    for k in range(1, 4):
        for m in range(6):
            spread(k, m).start()

    own_tokens.wait()
    top, bottom = pl.ds(0, HALF), pl.ds(HALF, HALF)

    def hop(slot, f, rows, by):
        piece = tok.at[f, core, rows]
        return remote(piece, piece, tok_send.at[slot], tok_recv.at[slot], (place, mod4(x + by), core))

    def pair(slot, f, rows):
        piece = tok.at[f, core, rows]
        return remote(piece, piece, pair_send.at[slot], pair_recv.at[slot], sibling)

    right_a, right_b = hop(0, x, top, 1), hop(1, x, bottom, 1)
    left_b, left_a = hop(2, x, bottom, -1), hop(3, x, top, -1)
    before, after, across = mod4(x - 1), mod4(x + 1), mod4(x + 2)
    on_right, on_left = hop(4, before, top, 1), hop(5, after, bottom, -1)
    for copy in (right_a, left_b, right_b, left_a):
        copy.start()
    pairs = [
        pair(0, x, top),
        pair(1, x, bottom),
        pair(2, before, top),
        pair(3, after, bottom),
        pair(4, before, bottom),
        pair(5, after, top),
        pair(6, across, top),
        pair(7, across, bottom),
    ]
    pairs[0].start()
    pairs[1].start()

    for k in range(1, 4):
        for m in range(6):
            spread(k, m).wait_recv()

    my_rows = pl.ds(pl.multiple_of(y * 32, 32), 32)

    def near(k, i, way):
        f = mod4(x + i)
        piece = wts.at[f, z, my_rows, (LEFT, RIGHT)[way]]
        there = (z * 4 + mod4(y + k), x, core) if way == 0 else (mod4(z + k) * 4 + y, x, core)
        at = (3 * way + k - 1) * 3 + i - 1
        return remote(piece, piece, near_send.at[at], near_recv.at[at], there)

    for k in range(1, 4):
        for i in range(1, 4):
            for way in range(2):
                near(k, i, way).start()
    for k in range(1, 4):
        for i in range(1, 4):
            for way in range(2):
                near(k, i, way).wait_recv()

    def far(by, i, way):
        f = mod4(x + i)
        if way == 0:
            piece, there = wts.at[f, z, :, LEFT], (mod4(z + by) * 4 + y, x, core)
        else:
            piece, there = wts.at[f, :, my_rows, RIGHT], (z * 4 + mod4(y + by), x, core)
        at = (2 * way + (by + 1) // 2) * 3 + i - 1
        return remote(piece, piece, far_send.at[at], far_recv.at[at], there)

    def onward(by, i, way):
        f = mod4(x + i)
        start = 0 if by == 1 else 1
        if way == 0:
            piece = wts.at[f, mod4(z - by), 64 * start : 64 * start + 64, LEFT]
            there = (mod4(z + by) * 4 + y, x, core)
        else:
            rows = pl.ds(pl.multiple_of(mod4(y - by) * 32, 32), 32)
            piece = wts.at[f, 2 * start : 2 * start + 2, rows, RIGHT]
            there = (z * 4 + mod4(y + by), x, core)
        at = (2 * way + (by + 1) // 2) * 3 + i - 1
        return remote(piece, piece, pass_send.at[at], pass_recv.at[at], there)

    kinds = [(by, i, way) for i in range(1, 4) for by in (1, -1) for way in range(2)]
    for kind in kinds:
        far(*kind).start()
    right_a.wait_recv()
    on_right.start()
    pairs[2].start()
    left_b.wait_recv()
    on_left.start()
    pairs[3].start()
    for kind in kinds:
        far(*kind).wait_recv()
        onward(*kind).start()
    others = [
        remote(att_ref, att_other_ref, other_send.at[0], other_recv.at[0], sibling),
        remote(conv_ref, conv_other_ref, other_send.at[1], other_recv.at[1], sibling),
        remote(params_hbm, params_other_ref, other_send.at[2], other_recv.at[2], sibling),
    ]
    for copy in own_weights:
        copy.wait()
    for kind in kinds:
        onward(*kind).wait_recv()

    def message(s, j, half):
        number = 2 * core + j
        there = mod4(s + number) * 4 + number
        at = 4 * s + 2 * j + half
        return remote(
            msg.at[at], recv.at[place], msg_send.at[at], msg_recv.at[place], (there, x, half)
        ), lax.abs(there - place) + lax.abs(half - core)

    def halo(s):
        return remote(
            gated.at[s, ROWS : ROWS + 8],
            gated.at[s, 0:8],
            halo_send.at[s],
            halo_recv.at[s],
            (lax.rem(place + 1, BLOCKS), x, core),
        )

    def to_home(at):
        s, half = lax.div(at, 2), lax.rem(at, 2)
        mine = 2 * x + core
        return remote(
            branch_out.at[at], branch_in.at[mine], branch_send.at[at], branch_recv.at[mine], (place, s, half)
        ), lax.abs(s - x) + lax.abs(half - core)

    def step(i, _):
        s = mod4(x + i + lax.div(i, 2) - 2 * lax.div(i, 3))

        @pl.when(i == 0)
        def _():
            pairs[0].wait_recv()
            pairs[1].wait_recv()

        @pl.when(i == 1)
        def _():
            right_b.wait_recv()
            pairs[4].start()
            left_a.wait_recv()
            pairs[5].start()
            pairs[3].wait_recv()
            pairs[5].wait_recv()

        @pl.when(i == 2)
        def _():
            pairs[2].wait_recv()
            pairs[4].wait_recv()

        @pl.when(i == 3)
        def _():
            on_right.wait_recv()
            pairs[6].start()
            on_left.wait_recv()
            pairs[7].start()
            for copy in others:
                copy.start()
            pairs[6].wait_recv()
            pairs[7].wait_recv()

        low = tok[s, 0].astype(F32)
        high = tok[s, 1].astype(F32)
        squares = jnp.sum(low * low, axis=1, keepdims=True) + jnp.sum(high * high, axis=1, keepdims=True)
        scale = lax.rsqrt(squares / D + epsilon)
        total = dot((low * params_ref[0:1, :]).astype(BF16), wts[0:2].reshape(1024, 768)) + dot(
            (high * params_ref[1:2, :]).astype(BF16), wts[2:4].reshape(1024, 768)
        )
        out = (total[:, 128:] * scale).astype(BF16)
        key, value = out[:, 0:128], out[:, 128:256]
        query = (total[:, 0:128] * (scale * (LOG2E / 8))).astype(BF16)
        for j in range(2):
            mine = slice(j * HD, (j + 1) * HD)
            both = jnp.concatenate((key[:, mine], value[:, mine]), axis=1)
            for half in range(2):
                r = half * HALF
                folded = jnp.concatenate((query[r : r + 96, mine], query[r + 96 : r + HALF, mine]), axis=1)
                msg[4 * s + 2 * j + half, 0:HALF, :] = both[r : r + HALF]
                msg[4 * s + 2 * j + half, HALF : HALF + 96, :] = folded
        outgate[s] = out[:, 256:384]
        gated[s, 8 : ROWS + 8, :] = out[:, 384:512].astype(F32) * out[:, 512:640].astype(F32)

        @pl.when(place < BLOCKS - 1)
        def _():
            halo(s).start()

        @pl.when(place == 0)
        def _():
            gated[s, 0:8, :] = jnp.zeros((8, 128), F32)

        for j in range(2):
            for half in range(2):
                copy, apart = message(s, j, half)

                @pl.when(apart > 0)
                def _():
                    copy.start()

                @pl.when(apart == 0)
                def _():
                    recv[place] = msg[4 * s + 2 * j + half]

        return 0

    lax.fori_loop(0, 4, step, 0)

    columns = pl.ds(pl.multiple_of(x * 128, 128), 128)

    def convolve(s, _):
        @pl.when(place > 0)
        def _():
            halo(s).wait_recv()

        convolved = sum(
            params_ref[4 + t : 5 + t, columns] * gated[s, 6 + t : 6 + t + ROWS, :] for t in range(3)
        )
        branch = (outgate[s].astype(F32) * convolved).astype(BF16)
        branch_out[2 * s] = branch[0:HALF]
        branch_out[2 * s + 1] = branch[HALF:ROWS]
        for half in range(2):
            copy, apart = to_home(2 * s + half)

            @pl.when(apart > 0)
            def _():
                copy.start()

            @pl.when(apart == 0)
            def _():
                branch_in[2 * x + core] = branch[half * HALF : (half + 1) * HALF]

        return 0

    lax.fori_loop(0, SEQS, convolve, 0)

    def to_mate(block):
        return remote(
            recv.at[block, 0:HALF], mate.at[block], mate_send.at[block], mate_recv.at[block], sibling
        )

    source_core = lax.div(y, 2)

    def arrive(k, _):
        block = lax.rem(place + k, BLOCKS)

        @pl.when(k + lax.abs(source_core - core) > 0)
        def _():
            remote(
                msg.at[0], recv.at[block], msg_send.at[0], msg_recv.at[block], (block, x, source_core)
            ).wait_recv()

        to_mate(block).start()
        return 0

    lax.fori_loop(0, BLOCKS, arrive, 0)
    own_out = pltpu.make_async_copy(recv, own_ref, local_sem.at[0])
    own_out.start()

    def arrived(block, _):
        to_mate(block).wait_recv()
        return 0

    lax.fori_loop(0, BLOCKS, arrived, 0)

    def branch_arrived(k, _):
        there = lax.rem(2 * x + core + k, 8)
        remote(
            branch_out.at[0],
            branch_in.at[there],
            branch_send.at[0],
            branch_recv.at[there],
            (place, lax.div(there, 2), lax.rem(there, 2)),
        ).wait_recv()
        return 0

    lax.fori_loop(1, 8, branch_arrived, 0)
    home_out = pltpu.make_async_copy(branch_in, branch_ref, local_sem.at[2])
    home_out.start()
    mate_out = pltpu.make_async_copy(mate, mate_ref, local_sem.at[1])
    mate_out.start()

    for k in range(1, 4):
        for m in range(6):
            spread(k, m).wait_send()
        for i in range(1, 4):
            for way in range(2):
                near(k, i, way).wait_send()
    for kind in kinds:
        far(*kind).wait_send()
        onward(*kind).wait_send()
    for copy in [right_a, right_b, left_a, left_b, on_right, on_left] + pairs:
        copy.wait_send()

    def left_here(at, _):
        s = lax.div(at, 4)
        j = lax.div(lax.rem(at, 4), 2)
        copy, apart = message(s, j, lax.rem(at, 2))

        @pl.when(apart > 0)
        def _():
            copy.wait_send()

        to_mate(at).wait_send()
        return 0

    lax.fori_loop(0, BLOCKS, left_here, 0)

    def branch_left(at, _):
        copy, apart = to_home(at)

        @pl.when(apart > 0)
        def _():
            copy.wait_send()

        return 0

    lax.fori_loop(0, 8, branch_left, 0)

    @pl.when(place < BLOCKS - 1)
    def _():
        for s in range(SEQS):
            halo(s).wait_send()

    home_out.wait()
    own_out.wait()
    mate_out.wait()
    for copy in others:
        copy.wait()


def front(tokens, params, mats, out_att, out_conv):
    hbm = pl.BlockSpec(memory_space=pl.ANY)
    vmem = pl.BlockSpec(memory_space=pltpu.VMEM)
    dma = lambda *shape: pltpu.SemaphoreType.DMA(shape)
    return pl.pallas_call(
        front_kernel,
        in_specs=[hbm, hbm, vmem] + [hbm] * 8,
        out_specs=[hbm] * 6,
        out_shape=[
            jax.ShapeDtypeStruct((BLOCKS, MESSAGE, 128), BF16),
            jax.ShapeDtypeStruct((BLOCKS, HALF, 128), BF16),
            jax.ShapeDtypeStruct((8, HALF, 128), BF16),
            jax.ShapeDtypeStruct(params.shape, F32),
            jax.ShapeDtypeStruct(out_att.shape, BF16),
            jax.ShapeDtypeStruct(out_conv.shape, BF16),
        ],
        scratch_shapes=[
            pltpu.VMEM((SEQS, 2, ROWS, 1024), BF16),
            pltpu.VMEM((4, 4, 128, 768), BF16),
            pltpu.VMEM((BLOCKS, MESSAGE, 128), BF16),
            pltpu.VMEM((BLOCKS, MESSAGE, 128), BF16),
            pltpu.VMEM((BLOCKS, HALF, 128), BF16),
            pltpu.VMEM((SEQS, ROWS + 8, 128), F32),
            pltpu.VMEM((SEQS, ROWS, 128), BF16),
            pltpu.VMEM((8, HALF, 128), BF16),
            pltpu.VMEM((8, HALF, 128), BF16),
            dma(31),
            dma(3, 6), dma(3, 6),
            dma(18), dma(18),
            dma(12), dma(12),
            dma(12), dma(12),
            dma(6), dma(6),
            dma(8), dma(8),
            dma(16), dma(16),
            dma(16), dma(16),
            dma(3), dma(3),
            dma(4), dma(4),
            dma(8), dma(8),
        ],
        compiler_params=pltpu.CompilerParams(
            collective_id=0, has_side_effects=True, vmem_limit_bytes=56 << 20
        ),
        name="front",
    )(tokens, params, params, *mats, out_att, out_conv)


def attend_kernel(
    offset_ref,
    own_ref,
    mate_ref,
    branch_ref,
    gain_ref,
    gain_other_ref,
    att_ref,
    att_other_ref,
    conv_ref,
    conv_other_ref,
    mixed_ref,
    mass_ref,
    keys,
    values,
    queries,
    score_a,
    score_b,
    decay_a,
    decay_b,
    weight_a,
    weight_b,
    total,
    att_out,
    att_in,
    mass_out,
    mass_in,
    att_weights,
    conv_weights,
    matrix,
    gains,
    att_send,
    att_recv,
    mass_send,
    mass_recv,
    local_sem,
):
    place, x, half = lax.axis_index("sp"), lax.axis_index("fs"), lax.axis_index("tp")
    number, row = lax.rem(place, 4), lax.div(place, 4)
    seq = mod4(row - number)

    barrier = pltpu.get_barrier_semaphore()

    def greet(k, _):
        n = lax.rem(k, 4)
        there, column = mod4(x + n) * 4 + n, lax.div(k, 4)
        for core in range(2):
            @pl.when(lax.abs(there - place) + lax.abs(column - x) + lax.abs(core - half) > 0)
            def _():
                pl.semaphore_signal(barrier, inc=1, device_id=(there, column, core), device_id_type=MESH)

        return 0

    lax.fori_loop(0, 16, greet, 0)
    fetches = [
        pltpu.make_async_copy(src, dst, local_sem.at[i])
        for i, (src, dst) in enumerate(
            [
                (att_ref, att_weights.at[half]),
                (att_other_ref, att_weights.at[1 - half]),
                (conv_ref, conv_weights.at[half]),
                (conv_other_ref, conv_weights.at[1 - half]),
                (gain_ref, gains.at[half]),
                (gain_other_ref, gains.at[1 - half]),
            ]
        )
    ]
    for copy in fetches:
        copy.start()

    def remote(src, dst, send, recv, device):
        return pltpu.make_async_remote_copy(
            src_ref=src, dst_ref=dst, send_sem=send, recv_sem=recv, device_id=device, device_id_type=MESH
        )

    def att_home(block):
        at = 4 * x + number
        apart = lax.abs(block - place) + lax.abs(seq - x)
        return remote(
            att_out.at[block], att_in.at[at], att_send.at[block], att_recv.at[at], (block, seq, half)
        ), apart

    def mass_home(block):
        at = 4 * x + 2 * lax.rem(number, 2) + half
        core = lax.div(number, 2)
        apart = lax.abs(block - place) + lax.abs(seq - x) + lax.abs(core - half)
        return remote(
            mass_out.at[block], mass_in.at[at], mass_send.at[block], mass_recv.at[at], (block, seq, core)
        ), apart

    lanes = lambda shape: lax.broadcasted_iota(jnp.int32, shape, 1)
    rows = lambda shape: lax.broadcasted_iota(jnp.int32, shape, 0)
    offset = jnp.full((HALF, 128), offset_ref[0] * LOG2E, F32)
    o1, o2, o3 = (part.astype(F32) for part in three_parts(offset))
    lane_q = lanes((HALF, 128))
    offset_row = jnp.where(
        lane_q == 0, -o1, jnp.where(lane_q == 1, -o2, jnp.where(lane_q == 2, -o3, 0.0))
    ).astype(BF16)
    square = (ROWS, HALF)
    source = lax.rem(rows(square), 8) * 48 + rows(square) // 8 - lanes(square)
    permute_own = (source == half * HALF).astype(F32).astype(BF16)
    permute_mate = (source == HALF - half * HALF).astype(F32).astype(BF16)
    take_high = (lanes((HD, 128)) == rows((HD, 128)) + HD).astype(F32).astype(BF16)
    ones = (lanes((ROWS, 128)) < 3).astype(F32).astype(BF16)
    low_lane = lanes((96, 128)) < HD
    for block in range(BLOCKS):
        pair = dot(permute_own, own_ref[block, 0:HALF, :]) + dot(permute_mate, mate_ref[block])
        pair = pair.astype(BF16)
        keys[block * ROWS : (block + 1) * ROWS, 0:128] = pair
        keys[block * ROWS : (block + 1) * ROWS, 128:256] = ones
        values[block] = dot_nt(take_high, pair).astype(BF16)
        packed = own_ref[block, HALF:MESSAGE, :].astype(F32)
        at = (block % 2) * HALF
        queries[block // 2, at : at + 96, 0:128] = jnp.where(low_lane, packed, 0.0).astype(BF16)
        queries[block // 2, at + 96 : at + HALF, 0:128] = jnp.where(
            low_lane, pltpu.roll(packed, HD, 1), 0.0
        ).astype(BF16)
        queries[block // 2, at : at + HALF, 128:256] = offset_row

    pl.semaphore_wait(barrier, 31 + lax.min(lax.abs(seq - x), 1))

    sub = rows((8, ROWS))
    lane = lanes((8, ROWS))
    where_q = lane + half * HALF + jnp.where(lane < HALF, 0, HALF)

    def score(z_ref, tile_index, block):
        begin = pl.multiple_of(block * ROWS, ROWS)
        z_ref[...] = dot_nt(keys[pl.ds(begin, ROWS), :], queries[tile_index])

    def fold(w_ref, block):
        total[...] += dot(values[block], w_ref[...])

    def decay(z_ref, d_ref, ahead):
        run = jnp.zeros((8, ROWS), F32)
        for r in reversed(range(48)):
            z = z_ref[8 * r : 8 * r + 8, :]
            soft = jnp.maximum(z, lax.log2(1.0 + jnp.exp2(jnp.minimum(z, 126.0))))
            if ahead is not None:
                valid = ahead > r
                soft = jnp.where(valid, soft, 0.0)
            run = run + soft
            value = jnp.exp2(z - run)
            if ahead is not None:
                value = jnp.where(valid, value, 0.0)
            d_ref[8 * r : 8 * r + 8, :] = value
        return run

    def weigh(d_ref, w_ref, run, carry):
        suffix = run
        for step in (1, 2, 4):
            moved = pltpu.roll(suffix, 8 - step, 0)
            suffix = suffix + jnp.where(sub < 8 - step, moved, 0.0)
        after = jnp.where(sub < 7, pltpu.roll(suffix, 7, 0), 0.0)
        kept = jnp.exp2(-(carry + after))
        for i in range(24):
            both = jnp.concatenate(
                (d_ref[16 * i : 16 * i + 8, :] * kept, d_ref[16 * i + 8 : 16 * i + 16, :] * kept), axis=0
            )
            w_ref[16 * i : 16 * i + 16, :] = both.astype(BF16)
        return carry + jnp.broadcast_to(suffix[0:1], (8, ROWS))

    def two_blocks(tile, pair, carry, run, aheads, next_tile, next_pair):
        score(score_b, tile, 2 * pair)
        if run is not None:
            carry = weigh(decay_b, weight_b, run, carry)
        run_a = decay(score_a, decay_a, aheads[0])
        if run is not None:
            fold(weight_b, 2 * pair + 2)
        score(score_a, next_tile, 2 * next_pair + 1)
        carry = weigh(decay_a, weight_a, run_a, carry)
        run_b = decay(score_b, decay_b, aheads[1])
        fold(weight_a, 2 * pair + 1)
        return carry, run_b

    last = BLOCKS // 2 - 1
    score(score_a, last, BLOCKS - 1)

    def one_tile(step, _):
        m = last - step
        total[...] = jnp.zeros_like(total)
        aheads = (where_q - ROWS - 48 * sub, where_q - 48 * sub)
        below = lax.max(m - 1, 0)
        state = two_blocks(m, m, jnp.zeros((8, ROWS), F32), None, aheads, m, below)

        def before(i, state):
            pair = m - 1 - i
            end = 1 - lax.min(pair, 1)
            return two_blocks(m, pair, *state, (None, None), m - end, pair - 1 + end * m)

        carry, run = lax.fori_loop(0, m, before, state)
        carry = weigh(decay_b, weight_b, run, carry)
        fold(weight_b, 0)
        attended = total[...]
        attended = jnp.concatenate((attended, attended), axis=0).T
        for part in range(2):
            block = 2 * m + part
            r = part * HALF
            folded = jnp.where(lanes((96, 128)) < HD, attended[r : r + 96], attended[r + 96 : r + HALF])
            folded = folded.astype(BF16)
            mass = carry[:, r : r + HALF]
            att_out[block] = folded
            mass_out[block, :, 0:HALF] = mass
            copy, apart = att_home(block)

            @pl.when(apart > 0)
            def _():
                copy.start()

            @pl.when(apart == 0)
            def _():
                att_in[4 * x + number] = folded

            mass_copy, mass_apart = mass_home(block)

            @pl.when(mass_apart > 0)
            def _():
                mass_copy.start()

            @pl.when(mass_apart == 0)
            def _():
                mass_in[4 * x + 2 * lax.rem(number, 2) + half, :, 0:HALF] = mass

        return 0

    lax.fori_loop(0, BLOCKS // 2, one_tile, 0)

    for copy in fetches:
        copy.wait()

    def branch_product(store, row_gain, projection, load):
        squares = jnp.zeros((HALF, 128), F32)
        for core in range(2):
            for part in range(4):
                piece = load(core, part)
                squares = squares + piece * piece
                gain = gains[core, 2:3, row_gain + 128 * part : row_gain + 128 * part + 128]
                at = 512 * core + 128 * part
                store[:, at : at + 128] = (piece * gain).astype(BF16)
        scale = lax.rsqrt(jnp.sum(squares, axis=1, keepdims=True) / ATT_WIDTH + epsilon)
        return scale * dot(store[...], projection[...].reshape(1024, D))

    mixed = branch_product(
        matrix.at[0], 512, conv_weights, lambda core, part: branch_ref[2 * part + core].astype(F32)
    )

    def landed(at, _):
        column, n = lax.div(at, 4), lax.rem(at, 4)
        there = mod4(x + n) * 4 + n
        apart = lax.abs(there - place) + lax.abs(column - x)

        @pl.when(apart > 0)
        def _():
            remote(
                att_out.at[0], att_in.at[at], att_send.at[0], att_recv.at[at], (there, column, half)
            ).wait_recv()

        n = 2 * half + lax.div(n, 2)
        core = lax.rem(at, 2)
        there = mod4(x + n) * 4 + n
        apart = lax.abs(there - place) + lax.abs(column - x) + lax.abs(core - half)

        @pl.when(apart > 0)
        def _():
            remote(
                mass_out.at[0], mass_in.at[at], mass_send.at[0], mass_recv.at[at], (there, column, core)
            ).wait_recv()

        return 0

    lax.fori_loop(0, 16, landed, 0)

    def heads(core, part):
        a = att_in[4 * part + 2 * core].astype(F32)
        b = att_in[4 * part + 2 * core + 1].astype(F32)
        low = lanes((96, 128)) < HD
        upper = jnp.where(low, a, pltpu.roll(b, HD, 1))
        lower = jnp.where(low, pltpu.roll(a, HD, 1), b)
        return jnp.concatenate((upper, lower), axis=0)

    mixed = mixed + branch_product(matrix.at[1], 0, att_weights, heads)
    mixed_ref[0] = mixed.astype(BF16)
    for part in range(2):
        kept = jnp.concatenate([mass_in[2 * n + part, 0:1, :] for n in range(8)], axis=0)
        mass = jnp.log(2.0 - jnp.exp2(-kept)).T
        mass_ref[0, part * HALF : (part + 1) * HALF, :] = mass[0:HALF]

    def left(block, _):
        copy, apart = att_home(block)

        @pl.when(apart > 0)
        def _():
            copy.wait_send()

        mass_copy, mass_apart = mass_home(block)

        @pl.when(mass_apart > 0)
        def _():
            mass_copy.wait_send()

        return 0

    lax.fori_loop(0, BLOCKS, left, 0)


def attend(offset, own, mate, branch, params, params_other, att, att_other, conv, conv_other):
    whole = pl.BlockSpec(memory_space=pltpu.VMEM)
    hbm = pl.BlockSpec(memory_space=pl.ANY)
    dma = lambda *shape: pltpu.SemaphoreType.DMA(shape)
    return pl.pallas_call(
        attend_kernel,
        in_specs=[pl.BlockSpec(memory_space=pltpu.SMEM), whole, whole, whole] + [hbm] * 6,
        out_specs=[whole, whole],
        out_shape=[
            jax.ShapeDtypeStruct((1, HALF, D), BF16),
            jax.ShapeDtypeStruct((1, ROWS, 8), F32),
        ],
        scratch_shapes=[
            pltpu.VMEM((BLOCKS * ROWS, 256), BF16),
            pltpu.VMEM((BLOCKS, HD, ROWS), BF16),
            pltpu.VMEM((BLOCKS // 2, ROWS, 256), BF16),
            pltpu.VMEM((ROWS, ROWS), F32),
            pltpu.VMEM((ROWS, ROWS), F32),
            pltpu.VMEM((ROWS, ROWS), F32),
            pltpu.VMEM((ROWS, ROWS), F32),
            pltpu.VMEM((ROWS, ROWS), BF16),
            pltpu.VMEM((ROWS, ROWS), BF16),
            pltpu.VMEM((HD, ROWS), F32),
            pltpu.VMEM((BLOCKS, 96, 128), BF16),
            pltpu.VMEM((BLOCKS, 96, 128), BF16),
            pltpu.VMEM((BLOCKS, 8, 256), F32),
            pltpu.VMEM((BLOCKS, 8, 256), F32),
            pltpu.VMEM((2, 512, D), BF16),
            pltpu.VMEM((2, 512, D), BF16),
            pltpu.VMEM((2, HALF, 1024), BF16),
            pltpu.VMEM((2, 8, 1024), F32),
            dma(16), dma(16), dma(16), dma(16), dma(6),
        ],
        compiler_params=pltpu.CompilerParams(
            collective_id=1, has_side_effects=True, vmem_limit_bytes=56 << 20
        ),
        name="attend",
    )(offset, own, mate, branch, params, params_other, att, att_other, conv, conv_other)


def per_device(
    tokens,
    in_gain,
    w_query,
    w_key,
    w_value,
    w_outgate,
    w_ingate,
    w_conv_in,
    score_offset,
    conv_taps,
    att_gain,
    conv_gain,
    out_att,
    out_conv,
):
    wide = lambda a: jnp.pad(a, ((0, 0), (0, 1024 - a.shape[1])))
    params = jnp.concatenate(
        (
            in_gain.reshape(2, 1024),
            jnp.concatenate((att_gain, conv_gain))[None],
            wide(score_offset[None]),
            wide(conv_taps),
            jnp.zeros((1, 1024), F32),
        ),
        axis=0,
    )
    own, mate, branch, params_other, att_other, conv_other = front(
        tokens[0], params, (w_query, w_key, w_value, w_outgate, w_ingate, w_conv_in), out_att, out_conv
    )
    number = lax.rem(lax.axis_index("sp"), 4)
    offsets = jnp.where(number // 2 == lax.axis_index("tp"), score_offset, params_other[3, :8])
    offset = lax.dynamic_slice_in_dim(offsets, 2 * lax.axis_index("fs") + lax.rem(number, 2), 1, 0)
    return tuple(
        attend(
            offset, own, mate, branch, params, params_other, out_att, att_other, out_conv, conv_other
        )
    )


def solution(mesh):
    return jax.shard_map(
        per_device,
        mesh=mesh,
        in_specs=(
            P("fs", "sp", "tp"),
            P(),
            P("fs", "tp"),
            P("fs", "tp"),
            P("fs", "tp"),
            P("fs", "tp"),
            P("fs", "tp"),
            P("fs", "tp"),
            P("tp"),
            P(None, "tp"),
            P("tp"),
            P("tp"),
            P("tp", None),
            P("tp", None),
        ),
        out_specs=(P("fs", ("sp", "tp"), None), P("fs", "sp", "tp")),
        check_vma=False,
    )
```

```python
import functools

import jax
import jax.numpy as jnp
from jax import lax
from jax.experimental import pallas as pl
from jax.experimental.pallas import tpu as pltpu
from jax.sharding import PartitionSpec as P

D = 2048
CONV_CH = 1024
ATT_WIDTH = 1024
SEQS = 4
ROWS = 384
HALF = 192
BLOCKS = 16
HD = 64
MESSAGE = HALF + HALF // 2
epsilon = 1e-06
LOG2E = 1.4426950408889634
F32 = jnp.float32
BF16 = jnp.bfloat16


def dot(a, b):
    return jnp.dot(a, b, preferred_element_type=F32)


def dot_nt(a, b):
    return lax.dot_general(a, b, (((1,), (1,)), ((), ())), preferred_element_type=F32)


def three_parts(x):
    a = x.astype(BF16)
    rest = x - a.astype(F32)
    b = rest.astype(BF16)
    return a, b, (rest - b.astype(F32)).astype(BF16)


MESH = pl.DeviceIdType.MESH
LEFT, RIGHT = slice(0, 384), slice(384, 768)


def mod4(value):
    return lax.rem(value + 8, 4)


def layer_kernel(
    tokens_ref,
    gain_ref,
    side_ref,
    taps_ref,
    wq_ref,
    wk_ref,
    wv_ref,
    wo_ref,
    wi_ref,
    wc_ref,
    att_ref,
    conv_ref,
    mixed_ref,
    mass_ref,
    tok,
    wts,
    msg,
    recv,
    mate,
    gated,
    outgate,
    branch_out,
    branch_in,
    keys,
    values,
    queries,
    score_a,
    score_b,
    decay_a,
    decay_b,
    weight_a,
    weight_b,
    total,
    att_out,
    att_in,
    mass_out,
    mass_in,
    att_weights,
    conv_weights,
    matrix,
    sides,
    local_sem,
    spread_send,
    spread_recv,
    near_send,
    near_recv,
    far_send,
    far_recv,
    pass_send,
    pass_recv,
    tok_send,
    tok_recv,
    pair_send,
    pair_recv,
    msg_send,
    msg_recv,
    mate_send,
    mate_recv,
    other_send,
    other_recv,
    halo_send,
    halo_recv,
    branch_send,
    branch_recv,
    att_send,
    att_recv,
    mass_send,
    mass_recv,
):
    place, x, core = lax.axis_index("sp"), lax.axis_index("fs"), lax.axis_index("tp")
    y, z = lax.rem(place, 4), lax.div(place, 4)
    sibling = (place, x, 1 - core)
    mats = (wq_ref, wk_ref, wv_ref, wo_ref, wi_ref, wc_ref)

    def remote(src, dst, send, recv_sem, device):
        return pltpu.make_async_remote_copy(
            src_ref=src, dst_ref=dst, send_sem=send, recv_sem=recv_sem, device_id=device, device_id_type=MESH
        )

    own_tokens = pltpu.make_async_copy(tokens_ref, tok.at[x, core], local_sem.at[6])
    own_tokens.start()
    own_weights = []
    for m in range(6):
        for part in range(4):
            own_weights.append(
                pltpu.make_async_copy(
                    mats[m].at[pl.ds(part * 128, 128), pl.ds(pl.multiple_of(x * 128, 128), 128)],
                    wts.at[x, part, :, m * 128 : (m + 1) * 128],
                    local_sem.at[7 + 4 * m + part],
                )
            )
    for copy in own_weights:
        copy.start()

    barrier = pltpu.get_barrier_semaphore()
    for k in range(1, 4):
        pl.semaphore_signal(barrier, inc=1, device_id=(place, mod4(x + k), core), device_id_type=MESH)
    pl.semaphore_signal(barrier, inc=1, device_id=sibling, device_id_type=MESH)

    def greet(k, _):
        there = lax.rem(place + k, BLOCKS)
        pl.semaphore_signal(barrier, inc=1, device_id=(there, x, core), device_id_type=MESH)
        pl.semaphore_signal(barrier, inc=1, device_id=(there, x, 1 - core), device_id_type=MESH)
        return 0

    lax.fori_loop(1, BLOCKS, greet, 0)
    number, row = y, z
    seq = mod4(row - number)

    def greet_far(k, _):
        n = lax.rem(k, 4)
        there, column = mod4(x + n) * 4 + n, lax.div(k, 4)
        for other in range(2):

            @pl.when(lax.abs(there - place) + lax.abs(column - x) + lax.abs(other - core) > 0)
            def _():
                pl.semaphore_signal(barrier, inc=1, device_id=(there, column, other), device_id_type=MESH)

        return 0

    lax.fori_loop(0, 16, greet_far, 0)
    pl.semaphore_wait(barrier, 65 + lax.min(lax.abs(seq - x), 1))

    rows_at = pl.multiple_of(place * 32, 32)

    def spread(k, m):
        there = mod4(x + k)
        return remote(
            mats[m].at[pl.ds(rows_at, 32), pl.ds(pl.multiple_of(there * 128, 128), 128)],
            wts.at[x, z, pl.ds(pl.multiple_of(y * 32, 32), 32), m * 128 : (m + 1) * 128],
            spread_send.at[k - 1, m],
            spread_recv.at[k - 1, m],
            (place, there, core),
        )

    for k in range(1, 4):
        for m in range(6):
            spread(k, m).start()

    side_out = remote(side_ref, sides.at[core], other_send.at[2], other_recv.at[2], sibling)
    side_out.start()
    sides[core] = side_ref[...]
    own_tokens.wait()
    top, bottom = pl.ds(0, HALF), pl.ds(HALF, HALF)

    def hop(slot, f, rows, by):
        piece = tok.at[f, core, rows]
        return remote(piece, piece, tok_send.at[slot], tok_recv.at[slot], (place, mod4(x + by), core))

    def pair(slot, f, rows):
        piece = tok.at[f, core, rows]
        return remote(piece, piece, pair_send.at[slot], pair_recv.at[slot], sibling)

    right_a, right_b = hop(0, x, top, 1), hop(1, x, bottom, 1)
    left_b, left_a = hop(2, x, bottom, -1), hop(3, x, top, -1)
    before, after, across = mod4(x - 1), mod4(x + 1), mod4(x + 2)
    on_right, on_left = hop(4, before, top, 1), hop(5, after, bottom, -1)
    for copy in (right_a, left_b, right_b, left_a):
        copy.start()
    pairs = [
        pair(0, x, top),
        pair(1, x, bottom),
        pair(2, before, top),
        pair(3, after, bottom),
        pair(4, before, bottom),
        pair(5, after, top),
        pair(6, across, top),
        pair(7, across, bottom),
    ]
    pairs[0].start()
    pairs[1].start()

    for k in range(1, 4):
        for m in range(6):
            spread(k, m).wait_recv()

    my_rows = pl.ds(pl.multiple_of(y * 32, 32), 32)

    def near(k, i, way):
        f = mod4(x + i)
        piece = wts.at[f, z, my_rows, (LEFT, RIGHT)[way]]
        there = (z * 4 + mod4(y + k), x, core) if way == 0 else (mod4(z + k) * 4 + y, x, core)
        at = (3 * way + k - 1) * 3 + i - 1
        return remote(piece, piece, near_send.at[at], near_recv.at[at], there)

    for k in range(1, 4):
        for i in range(1, 4):
            for way in range(2):
                near(k, i, way).start()
    for k in range(1, 4):
        for i in range(1, 4):
            for way in range(2):
                near(k, i, way).wait_recv()

    def far(by, i, way):
        f = mod4(x + i)
        if way == 0:
            piece, there = wts.at[f, z, :, LEFT], (mod4(z + by) * 4 + y, x, core)
        else:
            piece, there = wts.at[f, :, my_rows, RIGHT], (z * 4 + mod4(y + by), x, core)
        at = (2 * way + (by + 1) // 2) * 3 + i - 1
        return remote(piece, piece, far_send.at[at], far_recv.at[at], there)

    def onward(by, i, way):
        f = mod4(x + i)
        start = 0 if by == 1 else 1
        if way == 0:
            piece = wts.at[f, mod4(z - by), 64 * start : 64 * start + 64, LEFT]
            there = (mod4(z + by) * 4 + y, x, core)
        else:
            rows = pl.ds(pl.multiple_of(mod4(y - by) * 32, 32), 32)
            piece = wts.at[f, 2 * start : 2 * start + 2, rows, RIGHT]
            there = (z * 4 + mod4(y + by), x, core)
        at = (2 * way + (by + 1) // 2) * 3 + i - 1
        return remote(piece, piece, pass_send.at[at], pass_recv.at[at], there)

    kinds = [(by, i, way) for i in range(1, 4) for by in (1, -1) for way in range(2)]
    for kind in kinds:
        far(*kind).start()
    right_a.wait_recv()
    on_right.start()
    pairs[2].start()
    left_b.wait_recv()
    on_left.start()
    pairs[3].start()
    for kind in kinds:
        far(*kind).wait_recv()
        onward(*kind).start()
    others = [
        remote(att_ref, att_weights.at[core], other_send.at[0], other_recv.at[0], sibling),
        remote(conv_ref, conv_weights.at[core], other_send.at[1], other_recv.at[1], sibling),
    ]
    fetches = [
        pltpu.make_async_copy(att_ref, att_weights.at[core], local_sem.at[0]),
        pltpu.make_async_copy(conv_ref, conv_weights.at[core], local_sem.at[1]),
    ]
    for copy in own_weights:
        copy.wait()
    for kind in kinds:
        onward(*kind).wait_recv()

    def message(s, j, half):
        number = 2 * core + j
        there = mod4(s + number) * 4 + number
        at = 4 * s + 2 * j + half
        return remote(
            msg.at[at], recv.at[place], msg_send.at[at], msg_recv.at[place], (there, x, half)
        ), lax.abs(there - place) + lax.abs(half - core)

    def halo(s):
        return remote(
            gated.at[s, ROWS : ROWS + 8],
            gated.at[s, 0:8],
            halo_send.at[s],
            halo_recv.at[s],
            (lax.rem(place + 1, BLOCKS), x, core),
        )

    def to_home(at):
        s, half = lax.div(at, 2), lax.rem(at, 2)
        mine = 2 * x + core
        return remote(
            branch_out.at[at], branch_in.at[mine], branch_send.at[at], branch_recv.at[mine], (place, s, half)
        ), lax.abs(s - x) + lax.abs(half - core)

    def step(i, _):
        s = mod4(x + i + lax.div(i, 2) - 2 * lax.div(i, 3))

        @pl.when(i == 0)
        def _():
            pairs[0].wait_recv()
            pairs[1].wait_recv()

        @pl.when(i == 1)
        def _():
            right_b.wait_recv()
            pairs[4].start()
            left_a.wait_recv()
            pairs[5].start()
            pairs[3].wait_recv()
            pairs[5].wait_recv()

        @pl.when(i == 2)
        def _():
            pairs[2].wait_recv()
            pairs[4].wait_recv()

        @pl.when(i == 3)
        def _():
            on_right.wait_recv()
            pairs[6].start()
            on_left.wait_recv()
            pairs[7].start()
            for copy in others + fetches:
                copy.start()
            pairs[6].wait_recv()
            pairs[7].wait_recv()

        low = tok[s, 0].astype(F32)
        high = tok[s, 1].astype(F32)
        squares = jnp.sum(low * low, axis=1, keepdims=True) + jnp.sum(high * high, axis=1, keepdims=True)
        scale = lax.rsqrt(squares / D + epsilon)
        product = dot((low * gain_ref[0:1, 0:1024]).astype(BF16), wts[0:2].reshape(1024, 768)) + dot(
            (high * gain_ref[0:1, 1024:2048]).astype(BF16), wts[2:4].reshape(1024, 768)
        )
        out = (product[:, 128:] * scale).astype(BF16)
        key, value = out[:, 0:128], out[:, 128:256]
        query = (product[:, 0:128] * (scale * (LOG2E / 8))).astype(BF16)
        for j in range(2):
            mine = slice(j * HD, (j + 1) * HD)
            both = jnp.concatenate((key[:, mine], value[:, mine]), axis=1)
            for half in range(2):
                r = half * HALF
                folded = jnp.concatenate((query[r : r + 96, mine], query[r + 96 : r + HALF, mine]), axis=1)
                msg[4 * s + 2 * j + half, 0:HALF, :] = both[r : r + HALF]
                msg[4 * s + 2 * j + half, HALF : HALF + 96, :] = folded
        outgate[s] = out[:, 256:384]
        gated[s, 8 : ROWS + 8, :] = out[:, 384:512].astype(F32) * out[:, 512:640].astype(F32)

        @pl.when(place < BLOCKS - 1)
        def _():
            halo(s).start()

        @pl.when(place == 0)
        def _():
            gated[s, 0:8, :] = jnp.zeros((8, 128), F32)

        for j in range(2):
            for half in range(2):
                copy, apart = message(s, j, half)

                @pl.when(apart > 0)
                def _():
                    copy.start()

                @pl.when(apart == 0)
                def _():
                    recv[place] = msg[4 * s + 2 * j + half]

        return 0

    lax.fori_loop(0, 4, step, 0)

    columns = pl.ds(pl.multiple_of(x * 128, 128), 128)

    def convolve(s, _):
        @pl.when(place > 0)
        def _():
            halo(s).wait_recv()

        convolved = sum(
            taps_ref[t : t + 1, columns] * gated[s, 6 + t : 6 + t + ROWS, :] for t in range(3)
        )
        branch = (outgate[s].astype(F32) * convolved).astype(BF16)
        branch_out[2 * s] = branch[0:HALF]
        branch_out[2 * s + 1] = branch[HALF:ROWS]
        for half in range(2):
            copy, apart = to_home(2 * s + half)

            @pl.when(apart > 0)
            def _():
                copy.start()

            @pl.when(apart == 0)
            def _():
                branch_in[2 * x + core] = branch[half * HALF : (half + 1) * HALF]

        return 0

    lax.fori_loop(0, SEQS, convolve, 0)

    def to_mate(block):
        return remote(
            recv.at[block, 0:HALF], mate.at[block], mate_send.at[block], mate_recv.at[block], sibling
        )

    source_core = lax.div(y, 2)

    lanes = lambda shape: lax.broadcasted_iota(jnp.int32, shape, 1)
    rows = lambda shape: lax.broadcasted_iota(jnp.int32, shape, 0)
    side_out.wait_recv()
    place_of_head = lanes((1, 128)) == 2 * x + lax.rem(number, 2)
    offset_lane = sides[lax.div(number, 2), 0:1, 1024:1152]
    offset = jnp.sum(jnp.where(place_of_head, offset_lane, 0.0), axis=1, keepdims=True) * LOG2E
    offset = jnp.broadcast_to(offset, (HALF, 128))
    o1, o2, o3 = (part.astype(F32) for part in three_parts(offset))
    lane_q = lanes((HALF, 128))
    offset_row = jnp.where(
        lane_q == 0, -o1, jnp.where(lane_q == 1, -o2, jnp.where(lane_q == 2, -o3, 0.0))
    ).astype(BF16)
    square = (ROWS, HALF)
    source = lax.rem(rows(square), 8) * 48 + rows(square) // 8 - lanes(square)
    permute_own = (source == core * HALF).astype(F32).astype(BF16)
    permute_mate = (source == HALF - core * HALF).astype(F32).astype(BF16)
    take_high = (lanes((HD, 128)) == rows((HD, 128)) + HD).astype(F32).astype(BF16)
    ones = (lanes((ROWS, 128)) < 3).astype(F32).astype(BF16)
    low_lane = lanes((96, 128)) < HD

    def prepare(block):
        pair = dot(permute_own, recv[block, 0:HALF, :]) + dot(permute_mate, mate[block])
        pair = pair.astype(BF16)
        at = pl.ds(pl.multiple_of(block * ROWS, ROWS), ROWS)
        keys[at, 0:128] = pair
        keys[at, 128:256] = ones
        values[block] = dot_nt(take_high, pair).astype(BF16)
        packed = recv[block, HALF:MESSAGE, :].astype(F32)
        tile, first = lax.div(block, 2), lax.rem(block, 2) * HALF
        rows_of = lambda start, size: pl.ds(pl.multiple_of(first + start, 32), size)
        queries[tile, rows_of(0, 96), 0:128] = jnp.where(low_lane, packed, 0.0).astype(BF16)
        queries[tile, rows_of(96, 96), 0:128] = jnp.where(
            low_lane, pltpu.roll(packed, HD, 1), 0.0
        ).astype(BF16)
        queries[tile, rows_of(0, HALF), 128:256] = offset_row

    def arrive(k):
        block = lax.rem(place + k, BLOCKS)

        @pl.when(k + lax.abs(source_core - core) > 0)
        def _():
            remote(
                msg.at[0], recv.at[block], msg_send.at[0], msg_recv.at[block], (block, x, source_core)
            ).wait_recv()

        to_mate(block).start()

    def use(k):
        block = lax.rem(place + k, BLOCKS)
        to_mate(block).wait_recv()
        prepare(block)

    arrive(0)
    arrive(1)

    def arrive_and_use(k, _):
        arrive(k)
        use(k - 2)
        return 0

    lax.fori_loop(2, BLOCKS, arrive_and_use, 0)
    use(BLOCKS - 2)
    use(BLOCKS - 1)

    def att_home(block):
        at = 4 * x + number
        apart = lax.abs(block - place) + lax.abs(seq - x)
        return remote(
            att_out.at[block], att_in.at[at], att_send.at[block], att_recv.at[at], (block, seq, core)
        ), apart

    def mass_home(block):
        at = 4 * x + 2 * lax.rem(number, 2) + core
        goal = lax.div(number, 2)
        apart = lax.abs(block - place) + lax.abs(seq - x) + lax.abs(goal - core)
        return remote(
            mass_out.at[block], mass_in.at[at], mass_send.at[block], mass_recv.at[at], (block, seq, goal)
        ), apart

    sub = rows((8, ROWS))
    lane = lanes((8, ROWS))
    where_q = lane + core * HALF + jnp.where(lane < HALF, 0, HALF)

    def score(z_ref, tile_index, block):
        begin = pl.multiple_of(block * ROWS, ROWS)
        z_ref[...] = dot_nt(keys[pl.ds(begin, ROWS), :], queries[tile_index])

    def fold(w_ref, block):
        total[...] += dot(values[block], w_ref[...])

    def decay(z_ref, d_ref, ahead):
        run = jnp.zeros((8, ROWS), F32)
        for r in reversed(range(48)):
            z = z_ref[8 * r : 8 * r + 8, :]
            soft = jnp.maximum(z, lax.log2(1.0 + jnp.exp2(jnp.minimum(z, 126.0))))
            if ahead is not None:
                valid = ahead > r
                soft = jnp.where(valid, soft, 0.0)
            run = run + soft
            value = jnp.exp2(z - run)
            if ahead is not None:
                value = jnp.where(valid, value, 0.0)
            d_ref[8 * r : 8 * r + 8, :] = value
        return run

    def weigh(d_ref, w_ref, run, carry):
        suffix = run
        for step in (1, 2, 4):
            moved = pltpu.roll(suffix, 8 - step, 0)
            suffix = suffix + jnp.where(sub < 8 - step, moved, 0.0)
        after = jnp.where(sub < 7, pltpu.roll(suffix, 7, 0), 0.0)
        kept = jnp.exp2(-(carry + after))
        for i in range(24):
            both = jnp.concatenate(
                (d_ref[16 * i : 16 * i + 8, :] * kept, d_ref[16 * i + 8 : 16 * i + 16, :] * kept), axis=0
            )
            w_ref[16 * i : 16 * i + 16, :] = both.astype(BF16)
        return carry + jnp.broadcast_to(suffix[0:1], (8, ROWS))

    def two_blocks(tile, pair, carry, run, aheads, next_tile, next_pair):
        score(score_b, tile, 2 * pair)
        if run is not None:
            carry = weigh(decay_b, weight_b, run, carry)
        run_a = decay(score_a, decay_a, aheads[0])
        if run is not None:
            fold(weight_b, 2 * pair + 2)
        score(score_a, next_tile, 2 * next_pair + 1)
        carry = weigh(decay_a, weight_a, run_a, carry)
        run_b = decay(score_b, decay_b, aheads[1])
        fold(weight_a, 2 * pair + 1)
        return carry, run_b

    last = BLOCKS // 2 - 1
    score(score_a, last, BLOCKS - 1)

    def one_tile(step, _):
        m = last - step
        total[...] = jnp.zeros_like(total)
        aheads = (where_q - ROWS - 48 * sub, where_q - 48 * sub)
        below = lax.max(m - 1, 0)
        state = two_blocks(m, m, jnp.zeros((8, ROWS), F32), None, aheads, m, below)

        def earlier(i, state):
            pair = m - 1 - i
            end = 1 - lax.min(pair, 1)
            return two_blocks(m, pair, *state, (None, None), m - end, pair - 1 + end * m)

        carry, run = lax.fori_loop(0, m, earlier, state)
        carry = weigh(decay_b, weight_b, run, carry)
        fold(weight_b, 0)
        attended = total[...]
        attended = jnp.concatenate((attended, attended), axis=0).T
        for part in range(2):
            block = 2 * m + part
            r = part * HALF
            folded = jnp.where(lanes((96, 128)) < HD, attended[r : r + 96], attended[r + 96 : r + HALF])
            folded = folded.astype(BF16)
            mass = carry[:, r : r + HALF]
            att_out[block] = folded
            mass_out[block, :, 0:HALF] = mass
            copy, apart = att_home(block)

            @pl.when(apart > 0)
            def _():
                copy.start()

            @pl.when(apart == 0)
            def _():
                att_in[4 * x + number] = folded

            mass_copy, mass_apart = mass_home(block)

            @pl.when(mass_apart > 0)
            def _():
                mass_copy.start()

            @pl.when(mass_apart == 0)
            def _():
                mass_in[4 * x + 2 * lax.rem(number, 2) + core, :, 0:HALF] = mass

        return 0

    lax.fori_loop(0, BLOCKS // 2, one_tile, 0)

    for copy in fetches:
        copy.wait()
    for copy in others:
        copy.wait_recv()
    def branch_arrived(k, _):
        there = lax.rem(2 * x + core + k, 8)
        remote(
            branch_out.at[0],
            branch_in.at[there],
            branch_send.at[0],
            branch_recv.at[there],
            (place, lax.div(there, 2), lax.rem(there, 2)),
        ).wait_recv()
        return 0

    lax.fori_loop(1, 8, branch_arrived, 0)

    def branch_product(store, row_gain, projection, load):
        squares = jnp.zeros((HALF, 128), F32)
        for owner in range(2):
            for part in range(4):
                piece = load(owner, part)
                squares = squares + piece * piece
                gain = sides[owner, 0:1, row_gain + 128 * part : row_gain + 128 * part + 128]
                at = 512 * owner + 128 * part
                store[:, at : at + 128] = (piece * gain).astype(BF16)
        scale = lax.rsqrt(jnp.sum(squares, axis=1, keepdims=True) / ATT_WIDTH + epsilon)
        return scale * dot(store[...], projection[...].reshape(1024, D))

    mixed = branch_product(
        matrix.at[0], 512, conv_weights, lambda owner, part: branch_in[2 * part + owner].astype(F32)
    )

    def landed(at, _):
        column, n = lax.div(at, 4), lax.rem(at, 4)
        there = mod4(x + n) * 4 + n
        apart = lax.abs(there - place) + lax.abs(column - x)

        @pl.when(apart > 0)
        def _():
            remote(
                att_out.at[0], att_in.at[at], att_send.at[0], att_recv.at[at], (there, column, core)
            ).wait_recv()

        n = 2 * core + lax.div(n, 2)
        owner = lax.rem(at, 2)
        there = mod4(x + n) * 4 + n
        apart = lax.abs(there - place) + lax.abs(column - x) + lax.abs(owner - core)

        @pl.when(apart > 0)
        def _():
            remote(
                mass_out.at[0], mass_in.at[at], mass_send.at[0], mass_recv.at[at], (there, column, owner)
            ).wait_recv()

        return 0

    lax.fori_loop(0, 16, landed, 0)

    def heads(owner, part):
        a = att_in[4 * part + 2 * owner].astype(F32)
        b = att_in[4 * part + 2 * owner + 1].astype(F32)
        low = lanes((96, 128)) < HD
        upper = jnp.where(low, a, pltpu.roll(b, HD, 1))
        lower = jnp.where(low, pltpu.roll(a, HD, 1), b)
        return jnp.concatenate((upper, lower), axis=0)

    mixed = mixed + branch_product(matrix.at[1], 0, att_weights, heads)
    mixed_ref[0] = mixed.astype(BF16)
    for part in range(2):
        kept = jnp.concatenate([mass_in[2 * n + part, 0:1, :] for n in range(8)], axis=0)
        mass = jnp.log(2.0 - jnp.exp2(-kept))
        mass_ref[0, :, part * HALF : (part + 1) * HALF] = mass[:, 0:HALF]

    def left(block, _):
        copy, apart = att_home(block)

        @pl.when(apart > 0)
        def _():
            copy.wait_send()

        mass_copy, mass_apart = mass_home(block)

        @pl.when(mass_apart > 0)
        def _():
            mass_copy.wait_send()

        return 0

    lax.fori_loop(0, BLOCKS, left, 0)


    for k in range(1, 4):
        for m in range(6):
            spread(k, m).wait_send()
        for i in range(1, 4):
            for way in range(2):
                near(k, i, way).wait_send()
    for kind in kinds:
        far(*kind).wait_send()
        onward(*kind).wait_send()
    for copy in [right_a, right_b, left_a, left_b, on_right, on_left] + pairs:
        copy.wait_send()

    def left_here(at, _):
        s = lax.div(at, 4)
        j = lax.div(lax.rem(at, 4), 2)
        copy, apart = message(s, j, lax.rem(at, 2))

        @pl.when(apart > 0)
        def _():
            copy.wait_send()

        to_mate(at).wait_send()
        return 0

    lax.fori_loop(0, BLOCKS, left_here, 0)

    def branch_left(at, _):
        copy, apart = to_home(at)

        @pl.when(apart > 0)
        def _():
            copy.wait_send()

        return 0

    lax.fori_loop(0, 8, branch_left, 0)

    @pl.when(place < BLOCKS - 1)
    def _():
        for s in range(SEQS):
            halo(s).wait_send()

    side_out.wait_send()
    for copy in others:
        copy.wait_send()


def layer(tokens, gain, side, taps, mats, out_att, out_conv):
    hbm = pl.BlockSpec(memory_space=pl.ANY)
    vmem = pl.BlockSpec(memory_space=pltpu.VMEM)
    dma = lambda *shape: pltpu.SemaphoreType.DMA(shape)
    return pl.pallas_call(
        layer_kernel,
        in_specs=[hbm, vmem, vmem, vmem] + [hbm] * 8,
        out_specs=[vmem, vmem],
        out_shape=[
            jax.ShapeDtypeStruct((1, HALF, D), BF16),
            jax.ShapeDtypeStruct((1, 8, ROWS), F32),
        ],
        scratch_shapes=[
            pltpu.VMEM((SEQS, 2, ROWS, 1024), BF16),
            pltpu.VMEM((4, 4, 128, 768), BF16),
            pltpu.VMEM((BLOCKS, MESSAGE, 128), BF16),
            pltpu.VMEM((BLOCKS, MESSAGE, 128), BF16),
            pltpu.VMEM((BLOCKS, HALF, 128), BF16),
            pltpu.VMEM((SEQS, ROWS + 8, 128), F32),
            pltpu.VMEM((SEQS, ROWS, 128), BF16),
            pltpu.VMEM((8, HALF, 128), BF16),
            pltpu.VMEM((8, HALF, 128), BF16),
            pltpu.VMEM((BLOCKS * ROWS, 256), BF16),
            pltpu.VMEM((BLOCKS, HD, ROWS), BF16),
            pltpu.VMEM((BLOCKS // 2, ROWS, 256), BF16),
            pltpu.VMEM((ROWS, ROWS), F32),
            pltpu.VMEM((ROWS, ROWS), F32),
            pltpu.VMEM((ROWS, ROWS), F32),
            pltpu.VMEM((ROWS, ROWS), F32),
            pltpu.VMEM((ROWS, ROWS), BF16),
            pltpu.VMEM((ROWS, ROWS), BF16),
            pltpu.VMEM((HD, ROWS), F32),
            pltpu.VMEM((BLOCKS, 96, 128), BF16),
            pltpu.VMEM((BLOCKS, 96, 128), BF16),
            pltpu.VMEM((BLOCKS, 8, 256), F32),
            pltpu.VMEM((BLOCKS, 8, 256), F32),
            pltpu.VMEM((2, 512, D), BF16),
            pltpu.VMEM((2, 512, D), BF16),
            pltpu.VMEM((2, HALF, 1024), BF16),
            pltpu.VMEM((2, 1, 1152), F32),
            dma(31),
            dma(3, 6), dma(3, 6),
            dma(18), dma(18),
            dma(12), dma(12),
            dma(12), dma(12),
            dma(6), dma(6),
            dma(8), dma(8),
            dma(16), dma(16),
            dma(16), dma(16),
            dma(3), dma(3),
            dma(4), dma(4),
            dma(8), dma(8),
            dma(16), dma(16),
            dma(16), dma(16),
        ],
        compiler_params=pltpu.CompilerParams(
            collective_id=0, has_side_effects=True, vmem_limit_bytes=58 << 20
        ),
        name="layer",
    )(tokens, gain, side, taps, *mats, out_att, out_conv)


def per_device(
    tokens,
    in_gain,
    w_query,
    w_key,
    w_value,
    w_outgate,
    w_ingate,
    w_conv_in,
    score_offset,
    conv_taps,
    att_gain,
    conv_gain,
    out_att,
    out_conv,
):
    side = jnp.concatenate((att_gain, conv_gain, score_offset, jnp.zeros((120,), F32)))
    mixed, mass = layer(
        tokens[0],
        in_gain.reshape(1, D),
        side.reshape(1, 1152),
        conv_taps,
        (w_query, w_key, w_value, w_outgate, w_ingate, w_conv_in),
        out_att,
        out_conv,
    )
    return mixed, jnp.swapaxes(mass, 1, 2)


def solution(mesh):
    return jax.shard_map(
        per_device,
        mesh=mesh,
        in_specs=(
            P("fs", "sp", "tp"),
            P(),
            P("fs", "tp"),
            P("fs", "tp"),
            P("fs", "tp"),
            P("fs", "tp"),
            P("fs", "tp"),
            P("fs", "tp"),
            P("tp"),
            P(None, "tp"),
            P("tp"),
            P("tp"),
            P("tp", None),
            P("tp", None),
        ),
        out_specs=(P("fs", ("sp", "tp"), None), P("fs", "sp", "tp")),
        check_vma=False,
    )
```

```python
import functools

import jax
import jax.numpy as jnp
from jax import lax
from jax.experimental import pallas as pl
from jax.experimental.pallas import tpu as pltpu
from jax.sharding import PartitionSpec as P

D = 2048
CONV_CH = 1024
ATT_WIDTH = 1024
SEQS = 4
ROWS = 384
HALF = 192
BLOCKS = 16
HD = 64
MESSAGE = HALF + HALF // 2
epsilon = 1e-06
LOG2E = 1.4426950408889634
F32 = jnp.float32
BF16 = jnp.bfloat16


def dot(a, b):
    return jnp.dot(a, b, preferred_element_type=F32)


def dot_nt(a, b):
    return lax.dot_general(a, b, (((1,), (1,)), ((), ())), preferred_element_type=F32)


def three_parts(x):
    a = x.astype(BF16)
    rest = x - a.astype(F32)
    b = rest.astype(BF16)
    return a, b, (rest - b.astype(F32)).astype(BF16)


MESH = pl.DeviceIdType.MESH
LEFT, RIGHT = slice(0, 384), slice(384, 768)


def mod4(value):
    return lax.rem(value + 8, 4)


def layer_kernel(
    tokens_ref,
    gain_ref,
    att_gain_ref,
    conv_gain_ref,
    offset_ref,
    taps_ref,
    wq_ref,
    wk_ref,
    wv_ref,
    wo_ref,
    wi_ref,
    wc_ref,
    att_ref,
    conv_ref,
    mixed_ref,
    mass_ref,
    tok,
    wts,
    msg,
    recv,
    mate,
    gated,
    outgate,
    branch_out,
    branch_in,
    keys,
    values,
    queries,
    scores,
    decays,
    weights,
    total,
    att_out,
    att_in,
    mass_out,
    mass_in,
    att_weights,
    conv_weights,
    matrix,
    side,
    sides,
    local_sem,
    spread_send,
    spread_recv,
    near_send,
    near_recv,
    far_send,
    far_recv,
    pass_send,
    pass_recv,
    tok_send,
    tok_recv,
    pair_send,
    pair_recv,
    msg_send,
    msg_recv,
    mate_send,
    mate_recv,
    other_send,
    other_recv,
    halo_send,
    halo_recv,
    branch_send,
    branch_recv,
    att_send,
    att_recv,
    mass_send,
    mass_recv,
):
    place, x, core = lax.axis_index("sp"), lax.axis_index("fs"), lax.axis_index("tp")
    y, z = lax.rem(place, 4), lax.div(place, 4)
    sibling = (place, x, 1 - core)
    mats = (wq_ref, wk_ref, wv_ref, wo_ref, wi_ref, wc_ref)

    def remote(src, dst, send, recv_sem, device):
        return pltpu.make_async_remote_copy(
            src_ref=src, dst_ref=dst, send_sem=send, recv_sem=recv_sem, device_id=device, device_id_type=MESH
        )

    own_tokens = pltpu.make_async_copy(tokens_ref, tok.at[x, core], local_sem.at[6])
    own_tokens.start()
    own_weights = []
    for m in range(6):
        for part in range(4):
            own_weights.append(
                pltpu.make_async_copy(
                    mats[m].at[pl.ds(part * 128, 128), pl.ds(pl.multiple_of(x * 128, 128), 128)],
                    wts.at[x, part, :, m * 128 : (m + 1) * 128],
                    local_sem.at[7 + 4 * m + part],
                )
            )
    for copy in own_weights:
        copy.start()

    side[:, 0:512] = att_gain_ref[...]
    side[:, 512:1024] = conv_gain_ref[...]
    side[:, 1024:1152] = jnp.zeros((1, 128), F32)
    side[:, 1024:1032] = offset_ref[...]
    sides[core] = side[...]
    barrier = pltpu.get_barrier_semaphore()
    for k in range(1, 4):
        pl.semaphore_signal(barrier, inc=1, device_id=(place, mod4(x + k), core), device_id_type=MESH)
    pl.semaphore_signal(barrier, inc=1, device_id=sibling, device_id_type=MESH)

    def greet(k, _):
        there = lax.rem(place + k, BLOCKS)
        pl.semaphore_signal(barrier, inc=1, device_id=(there, x, core), device_id_type=MESH)
        pl.semaphore_signal(barrier, inc=1, device_id=(there, x, 1 - core), device_id_type=MESH)
        return 0

    lax.fori_loop(1, BLOCKS, greet, 0)
    number, row = y, z
    seq = mod4(row - number)

    def greet_far(k, _):
        n = lax.rem(k, 4)
        there, column = mod4(x + n) * 4 + n, lax.div(k, 4)
        for other in range(2):

            @pl.when(lax.abs(there - place) + lax.abs(column - x) + lax.abs(other - core) > 0)
            def _():
                pl.semaphore_signal(barrier, inc=1, device_id=(there, column, other), device_id_type=MESH)

        return 0

    lax.fori_loop(0, 16, greet_far, 0)
    pl.semaphore_wait(barrier, 65 + lax.min(lax.abs(seq - x), 1))

    rows_at = pl.multiple_of(place * 32, 32)

    def spread(k, m):
        there = mod4(x + k)
        return remote(
            mats[m].at[pl.ds(rows_at, 32), pl.ds(pl.multiple_of(there * 128, 128), 128)],
            wts.at[x, z, pl.ds(pl.multiple_of(y * 32, 32), 32), m * 128 : (m + 1) * 128],
            spread_send.at[k - 1, m],
            spread_recv.at[k - 1, m],
            (place, there, core),
        )

    for k in range(1, 4):
        for m in range(6):
            spread(k, m).start()

    side_out = remote(side, sides.at[core], other_send.at[2], other_recv.at[2], sibling)
    side_out.start()
    own_tokens.wait()
    top, bottom = pl.ds(0, HALF), pl.ds(HALF, HALF)

    def hop(slot, f, rows, by):
        piece = tok.at[f, core, rows]
        return remote(piece, piece, tok_send.at[slot], tok_recv.at[slot], (place, mod4(x + by), core))

    def pair(slot, f, rows):
        piece = tok.at[f, core, rows]
        return remote(piece, piece, pair_send.at[slot], pair_recv.at[slot], sibling)

    right_a, right_b = hop(0, x, top, 1), hop(1, x, bottom, 1)
    left_b, left_a = hop(2, x, bottom, -1), hop(3, x, top, -1)
    before, after, across = mod4(x - 1), mod4(x + 1), mod4(x + 2)
    on_right, on_left = hop(4, before, top, 1), hop(5, after, bottom, -1)
    for copy in (right_a, left_b, right_b, left_a):
        copy.start()
    pairs = [
        pair(0, x, top),
        pair(1, x, bottom),
        pair(2, before, top),
        pair(3, after, bottom),
        pair(4, before, bottom),
        pair(5, after, top),
        pair(6, across, top),
        pair(7, across, bottom),
    ]
    pairs[0].start()
    pairs[1].start()

    for k in range(1, 4):
        for m in range(6):
            spread(k, m).wait_recv()

    my_rows = pl.ds(pl.multiple_of(y * 32, 32), 32)

    def near(k, i, way):
        f = mod4(x + i)
        piece = wts.at[f, z, my_rows, (LEFT, RIGHT)[way]]
        there = (z * 4 + mod4(y + k), x, core) if way == 0 else (mod4(z + k) * 4 + y, x, core)
        at = (3 * way + k - 1) * 3 + i - 1
        return remote(piece, piece, near_send.at[at], near_recv.at[at], there)

    for k in range(1, 4):
        for i in range(1, 4):
            for way in range(2):
                near(k, i, way).start()
    for k in range(1, 4):
        for i in range(1, 4):
            for way in range(2):
                near(k, i, way).wait_recv()

    def far(by, i, way):
        f = mod4(x + i)
        if way == 0:
            piece, there = wts.at[f, z, :, LEFT], (mod4(z + by) * 4 + y, x, core)
        else:
            piece, there = wts.at[f, :, my_rows, RIGHT], (z * 4 + mod4(y + by), x, core)
        at = (2 * way + (by + 1) // 2) * 3 + i - 1
        return remote(piece, piece, far_send.at[at], far_recv.at[at], there)

    def onward(by, i, way):
        f = mod4(x + i)
        start = 0 if by == 1 else 1
        if way == 0:
            piece = wts.at[f, mod4(z - by), 64 * start : 64 * start + 64, LEFT]
            there = (mod4(z + by) * 4 + y, x, core)
        else:
            rows = pl.ds(pl.multiple_of(mod4(y - by) * 32, 32), 32)
            piece = wts.at[f, 2 * start : 2 * start + 2, rows, RIGHT]
            there = (z * 4 + mod4(y + by), x, core)
        at = (2 * way + (by + 1) // 2) * 3 + i - 1
        return remote(piece, piece, pass_send.at[at], pass_recv.at[at], there)

    kinds = [(by, i, way) for i in range(1, 4) for by in (1, -1) for way in range(2)]
    for kind in kinds:
        far(*kind).start()
    right_a.wait_recv()
    on_right.start()
    pairs[2].start()
    left_b.wait_recv()
    on_left.start()
    pairs[3].start()
    for kind in kinds:
        far(*kind).wait_recv()
        onward(*kind).start()
    others = [
        remote(att_ref, att_weights.at[core], other_send.at[0], other_recv.at[0], sibling),
        remote(conv_ref, conv_weights.at[core], other_send.at[1], other_recv.at[1], sibling),
    ]
    fetches = [
        pltpu.make_async_copy(att_ref, att_weights.at[core], local_sem.at[0]),
        pltpu.make_async_copy(conv_ref, conv_weights.at[core], local_sem.at[1]),
    ]
    for copy in own_weights:
        copy.wait()
    for kind in kinds:
        onward(*kind).wait_recv()

    def message(s, j, half):
        number = 2 * core + j
        there = mod4(s + number) * 4 + number
        at = 4 * s + 2 * j + half
        return remote(
            msg.at[at], recv.at[place], msg_send.at[at], msg_recv.at[place], (there, x, half)
        ), lax.abs(there - place) + lax.abs(half - core)

    def halo(s):
        return remote(
            gated.at[s, ROWS : ROWS + 8],
            gated.at[s, 0:8],
            halo_send.at[s],
            halo_recv.at[s],
            (lax.rem(place + 1, BLOCKS), x, core),
        )

    def to_home(at):
        s, half = lax.div(at, 2), lax.rem(at, 2)
        mine = 2 * x + core
        return remote(
            branch_out.at[at], branch_in.at[mine], branch_send.at[at], branch_recv.at[mine], (place, s, half)
        ), lax.abs(s - x) + lax.abs(half - core)

    def step(i, _):
        s = mod4(x + i + lax.div(i, 2) - 2 * lax.div(i, 3))

        @pl.when(i == 0)
        def _():
            pairs[0].wait_recv()
            pairs[1].wait_recv()

        @pl.when(i == 1)
        def _():
            right_b.wait_recv()
            pairs[4].start()
            left_a.wait_recv()
            pairs[5].start()
            pairs[3].wait_recv()
            pairs[5].wait_recv()

        @pl.when(i == 2)
        def _():
            pairs[2].wait_recv()
            pairs[4].wait_recv()

        @pl.when(i == 3)
        def _():
            on_right.wait_recv()
            pairs[6].start()
            on_left.wait_recv()
            pairs[7].start()
            for copy in others + fetches:
                copy.start()
            pairs[6].wait_recv()
            pairs[7].wait_recv()

        low = tok[s, 0].astype(F32)
        high = tok[s, 1].astype(F32)
        squares = jnp.sum(low * low, axis=1, keepdims=True) + jnp.sum(high * high, axis=1, keepdims=True)
        scale = lax.rsqrt(squares / D + epsilon)
        product = dot((low * gain_ref[0:1, 0:1024]).astype(BF16), wts[0:2].reshape(1024, 768)) + dot(
            (high * gain_ref[0:1, 1024:2048]).astype(BF16), wts[2:4].reshape(1024, 768)
        )
        out = (product[:, 128:] * scale).astype(BF16)
        key, value = out[:, 0:128], out[:, 128:256]
        query = (product[:, 0:128] * (scale * (LOG2E / 8))).astype(BF16)
        for j in range(2):
            mine = slice(j * HD, (j + 1) * HD)
            both = jnp.concatenate((key[:, mine], value[:, mine]), axis=1)
            for half in range(2):
                r = half * HALF
                folded = jnp.concatenate((query[r : r + 96, mine], query[r + 96 : r + HALF, mine]), axis=1)
                msg[4 * s + 2 * j + half, 0:HALF, :] = both[r : r + HALF]
                msg[4 * s + 2 * j + half, HALF : HALF + 96, :] = folded
        outgate[s] = out[:, 256:384]
        gated[s, 8 : ROWS + 8, :] = out[:, 384:512].astype(F32) * out[:, 512:640].astype(F32)

        @pl.when(place < BLOCKS - 1)
        def _():
            halo(s).start()

        @pl.when(place == 0)
        def _():
            gated[s, 0:8, :] = jnp.zeros((8, 128), F32)

        for j in range(2):
            for half in range(2):
                copy, apart = message(s, j, half)

                @pl.when(apart > 0)
                def _():
                    copy.start()

                @pl.when(apart == 0)
                def _():
                    recv[place] = msg[4 * s + 2 * j + half]

        return 0

    lax.fori_loop(0, 4, step, 0)

    columns = pl.ds(pl.multiple_of(x * 128, 128), 128)

    def convolve(s, _):
        @pl.when(place > 0)
        def _():
            halo(s).wait_recv()

        convolved = sum(
            taps_ref[t : t + 1, columns] * gated[s, 6 + t : 6 + t + ROWS, :] for t in range(3)
        )
        branch = (outgate[s].astype(F32) * convolved).astype(BF16)
        branch_out[2 * s] = branch[0:HALF]
        branch_out[2 * s + 1] = branch[HALF:ROWS]
        for half in range(2):
            copy, apart = to_home(2 * s + half)

            @pl.when(apart > 0)
            def _():
                copy.start()

            @pl.when(apart == 0)
            def _():
                branch_in[2 * x + core] = branch[half * HALF : (half + 1) * HALF]

        return 0

    lax.fori_loop(0, SEQS, convolve, 0)

    def to_mate(block):
        return remote(
            recv.at[block, 0:HALF], mate.at[block], mate_send.at[block], mate_recv.at[block], sibling
        )

    source_core = lax.div(y, 2)

    lanes = lambda shape: lax.broadcasted_iota(jnp.int32, shape, 1)
    rows = lambda shape: lax.broadcasted_iota(jnp.int32, shape, 0)
    side_out.wait_recv()
    place_of_head = lanes((1, 128)) == 2 * x + lax.rem(number, 2)
    offset_lane = sides[lax.div(number, 2), 0:1, 1024:1152]
    offset = jnp.sum(jnp.where(place_of_head, offset_lane, 0.0), axis=1, keepdims=True) * LOG2E
    offset = jnp.broadcast_to(offset, (HALF, 128))
    o1, o2, o3 = (part.astype(F32) for part in three_parts(offset))
    lane_q = lanes((HALF, 128))
    offset_row = jnp.where(
        lane_q == 0, -o1, jnp.where(lane_q == 1, -o2, jnp.where(lane_q == 2, -o3, 0.0))
    ).astype(BF16)
    square = (ROWS, HALF)
    source = lax.rem(rows(square), 8) * 48 + rows(square) // 8 - lanes(square)
    permute_own = (source == core * HALF).astype(F32).astype(BF16)
    permute_mate = (source == HALF - core * HALF).astype(F32).astype(BF16)
    take_high = (lanes((HD, 128)) == rows((HD, 128)) + HD).astype(F32).astype(BF16)
    ones = (lanes((ROWS, 128)) < 3).astype(F32).astype(BF16)
    low_lane = lanes((96, 128)) < HD

    def prepare(block):
        pair = dot(permute_own, recv[block, 0:HALF, :]) + dot(permute_mate, mate[block])
        pair = pair.astype(BF16)
        at = pl.ds(pl.multiple_of(block * ROWS, ROWS), ROWS)
        keys[at, 0:128] = pair
        keys[at, 128:256] = ones
        values[block] = dot_nt(take_high, pair).astype(BF16)
        packed = recv[block, HALF:MESSAGE, :].astype(F32)
        tile, first = lax.div(block, 2), lax.rem(block, 2) * HALF
        rows_of = lambda start, size: pl.ds(pl.multiple_of(first + start, 32), size)
        queries[tile, rows_of(0, 96), 0:128] = jnp.where(low_lane, packed, 0.0).astype(BF16)
        queries[tile, rows_of(96, 96), 0:128] = jnp.where(
            low_lane, pltpu.roll(packed, HD, 1), 0.0
        ).astype(BF16)
        queries[tile, rows_of(0, HALF), 128:256] = offset_row

    def arrive(k):
        block = lax.rem(place + k, BLOCKS)

        @pl.when(k + lax.abs(source_core - core) > 0)
        def _():
            remote(
                msg.at[0], recv.at[block], msg_send.at[0], msg_recv.at[block], (block, x, source_core)
            ).wait_recv()

        to_mate(block).start()

    def use(k):
        block = lax.rem(place + k, BLOCKS)
        to_mate(block).wait_recv()
        prepare(block)

    arrive(0)
    arrive(1)

    def arrive_and_use(k, _):
        arrive(k)
        use(k - 2)
        return 0

    lax.fori_loop(2, BLOCKS, arrive_and_use, 0)
    use(BLOCKS - 2)
    use(BLOCKS - 1)

    def att_home(block):
        at = 4 * x + number
        apart = lax.abs(block - place) + lax.abs(seq - x)
        return remote(
            att_out.at[block], att_in.at[at], att_send.at[block], att_recv.at[at], (block, seq, core)
        ), apart

    def mass_home(block):
        at = 4 * x + 2 * lax.rem(number, 2) + core
        goal = lax.div(number, 2)
        apart = lax.abs(block - place) + lax.abs(seq - x) + lax.abs(goal - core)
        return remote(
            mass_out.at[block], mass_in.at[at], mass_send.at[block], mass_recv.at[at], (block, seq, goal)
        ), apart

    sub = rows((8, ROWS))
    lane = lanes((8, ROWS))
    where_q = lane + core * HALF + jnp.where(lane < HALF, 0, HALF)

    def score(z_ref, tile_index, block):
        begin = pl.multiple_of(block * ROWS, ROWS)
        z_ref[...] = dot_nt(keys[pl.ds(begin, ROWS), :], queries[tile_index])

    def fold(w_ref, block):
        total[...] += dot(values[block], w_ref[...])

    def decay(z_ref, d_ref, ahead):
        run = jnp.zeros((8, ROWS), F32)
        for r in reversed(range(48)):
            z = z_ref[8 * r : 8 * r + 8, :]
            soft = jnp.maximum(z, lax.log2(1.0 + jnp.exp2(jnp.minimum(z, 126.0))))
            if ahead is not None:
                valid = ahead > r
                soft = jnp.where(valid, soft, 0.0)
            run = run + soft
            value = jnp.exp2(z - run)
            if ahead is not None:
                value = jnp.where(valid, value, 0.0)
            d_ref[8 * r : 8 * r + 8, :] = value
        return run

    def weigh(d_ref, w_ref, run, carry):
        suffix = run
        for step in (1, 2, 4):
            moved = pltpu.roll(suffix, 8 - step, 0)
            suffix = suffix + jnp.where(sub < 8 - step, moved, 0.0)
        after = jnp.where(sub < 7, pltpu.roll(suffix, 7, 0), 0.0)
        kept = jnp.exp2(-(carry + after))
        for i in range(24):
            both = jnp.concatenate(
                (d_ref[16 * i : 16 * i + 8, :] * kept, d_ref[16 * i + 8 : 16 * i + 16, :] * kept), axis=0
            )
            w_ref[16 * i : 16 * i + 16, :] = both.astype(BF16)
        return carry + jnp.broadcast_to(suffix[0:1], (8, ROWS))

    def run_blocks(tile, top, carry, run, aheads, next_tile, next_top):
        count = len(aheads)
        slots = (0, 1, 2, 3) if count == 4 else (0, 3)
        if count == 4:
            score(scores[3], tile, top - 3)
        else:
            score(scores[2], next_tile, lax.max(next_top - 2, 0))
        if run is not None:
            carry = weigh(decays[3], weights[3], run, carry)
        for i in range(count):
            slot = slots[i]
            run = decay(scores[i], decays[slot], aheads[i])
            if i > 0:
                fold(weights[slots[i - 1]], top - i + 1)
            elif aheads[0] is None:
                fold(weights[3], top + 1)
            if i < 3:
                score(scores[i], next_tile, lax.max(next_top - i, 0))
            if i < count - 1:
                carry = weigh(decays[slot], weights[slot], run, carry)
        return carry, run

    last = BLOCKS // 2 - 1
    for i in range(3):
        score(scores[i], last, BLOCKS - 1 - i)

    def one_tile(m, odd):
        total[...] = jnp.zeros_like(total)
        aheads = (where_q - ROWS - 48 * sub, where_q - 48 * sub)
        aheads = aheads + (None, None) if odd else aheads
        begin = 2 * m - 3 if odd else 2 * m - 1
        rest = lax.div(m, 2)
        more = lax.min(rest, 1)
        below = lax.max(m - 1, 0)

        def following(top, stay):
            return stay * m + (1 - stay) * below, stay * top + (1 - stay) * (2 * m - 1)

        state = run_blocks(m, 2 * m + 1, jnp.zeros((8, ROWS), F32), None, aheads, *following(begin, more))

        def earlier(i, state):
            top = begin - 4 * i
            stay = lax.min(lax.div(top, 4), 1)
            return run_blocks(m, top, *state, (None,) * 4, *following(top - 4, stay))

        carry, run = lax.fori_loop(0, rest, earlier, state)
        carry = weigh(decays[3], weights[3], run, carry)
        fold(weights[3], 0)
        attended = total[...]
        attended = jnp.concatenate((attended, attended), axis=0).T
        for part in range(2):
            block = 2 * m + part
            r = part * HALF
            folded = jnp.where(lanes((96, 128)) < HD, attended[r : r + 96], attended[r + 96 : r + HALF])
            folded = folded.astype(BF16)
            mass = carry[:, r : r + HALF]
            att_out[block] = folded
            mass_out[block, :, 0:HALF] = mass
            copy, apart = att_home(block)

            @pl.when(apart > 0)
            def _():
                copy.start()

            @pl.when(apart == 0)
            def _():
                att_in[4 * x + number] = folded

            mass_copy, mass_apart = mass_home(block)

            @pl.when(mass_apart > 0)
            def _():
                mass_copy.start()

            @pl.when(mass_apart == 0)
            def _():
                mass_in[4 * x + 2 * lax.rem(number, 2) + core, :, 0:HALF] = mass

    def two_tiles(step, _):
        one_tile(last - 2 * step, True)
        one_tile(last - 1 - 2 * step, False)
        return 0

    lax.fori_loop(0, BLOCKS // 4, two_tiles, 0)

    for copy in fetches:
        copy.wait()
    for copy in others:
        copy.wait_recv()
    def branch_arrived(k, _):
        there = lax.rem(2 * x + core + k, 8)
        remote(
            branch_out.at[0],
            branch_in.at[there],
            branch_send.at[0],
            branch_recv.at[there],
            (place, lax.div(there, 2), lax.rem(there, 2)),
        ).wait_recv()
        return 0

    lax.fori_loop(1, 8, branch_arrived, 0)

    def branch_product(store, row_gain, projection, load):
        squares = jnp.zeros((HALF, 128), F32)
        for owner in range(2):
            for part in range(4):
                piece = load(owner, part)
                squares = squares + piece * piece
                gain = sides[owner, 0:1, row_gain + 128 * part : row_gain + 128 * part + 128]
                at = 512 * owner + 128 * part
                store[:, at : at + 128] = (piece * gain).astype(BF16)
        scale = lax.rsqrt(jnp.sum(squares, axis=1, keepdims=True) / ATT_WIDTH + epsilon)
        return scale * dot(store[...], projection[...].reshape(1024, D))

    mixed = branch_product(
        matrix.at[0], 512, conv_weights, lambda owner, part: branch_in[2 * part + owner].astype(F32)
    )

    def landed(at, _):
        column, n = lax.div(at, 4), lax.rem(at, 4)
        there = mod4(x + n) * 4 + n
        apart = lax.abs(there - place) + lax.abs(column - x)

        @pl.when(apart > 0)
        def _():
            remote(
                att_out.at[0], att_in.at[at], att_send.at[0], att_recv.at[at], (there, column, core)
            ).wait_recv()

        n = 2 * core + lax.div(n, 2)
        owner = lax.rem(at, 2)
        there = mod4(x + n) * 4 + n
        apart = lax.abs(there - place) + lax.abs(column - x) + lax.abs(owner - core)

        @pl.when(apart > 0)
        def _():
            remote(
                mass_out.at[0], mass_in.at[at], mass_send.at[0], mass_recv.at[at], (there, column, owner)
            ).wait_recv()

        return 0

    lax.fori_loop(0, 16, landed, 0)

    def heads(owner, part):
        a = att_in[4 * part + 2 * owner].astype(F32)
        b = att_in[4 * part + 2 * owner + 1].astype(F32)
        low = lanes((96, 128)) < HD
        upper = jnp.where(low, a, pltpu.roll(b, HD, 1))
        lower = jnp.where(low, pltpu.roll(a, HD, 1), b)
        return jnp.concatenate((upper, lower), axis=0)

    mixed = mixed + branch_product(matrix.at[1], 0, att_weights, heads)
    mixed_ref[0] = mixed.astype(BF16)
    for part in range(2):
        kept = jnp.concatenate([mass_in[2 * n + part, 0:1, :] for n in range(8)], axis=0)
        mass = jnp.log(2.0 - jnp.exp2(-kept))
        mass_ref[0, :, part * HALF : (part + 1) * HALF] = mass[:, 0:HALF]

    def left(block, _):
        copy, apart = att_home(block)

        @pl.when(apart > 0)
        def _():
            copy.wait_send()

        mass_copy, mass_apart = mass_home(block)

        @pl.when(mass_apart > 0)
        def _():
            mass_copy.wait_send()

        return 0

    lax.fori_loop(0, BLOCKS, left, 0)


    for k in range(1, 4):
        for m in range(6):
            spread(k, m).wait_send()
        for i in range(1, 4):
            for way in range(2):
                near(k, i, way).wait_send()
    for kind in kinds:
        far(*kind).wait_send()
        onward(*kind).wait_send()
    for copy in [right_a, right_b, left_a, left_b, on_right, on_left] + pairs:
        copy.wait_send()

    def left_here(at, _):
        s = lax.div(at, 4)
        j = lax.div(lax.rem(at, 4), 2)
        copy, apart = message(s, j, lax.rem(at, 2))

        @pl.when(apart > 0)
        def _():
            copy.wait_send()

        to_mate(at).wait_send()
        return 0

    lax.fori_loop(0, BLOCKS, left_here, 0)

    def branch_left(at, _):
        copy, apart = to_home(at)

        @pl.when(apart > 0)
        def _():
            copy.wait_send()

        return 0

    lax.fori_loop(0, 8, branch_left, 0)

    @pl.when(place < BLOCKS - 1)
    def _():
        for s in range(SEQS):
            halo(s).wait_send()

    side_out.wait_send()
    for copy in others:
        copy.wait_send()


def layer(tokens, gain, att_gain, conv_gain, offset, taps, mats, out_att, out_conv):
    hbm = pl.BlockSpec(memory_space=pl.ANY)
    vmem = pl.BlockSpec(memory_space=pltpu.VMEM)
    dma = lambda *shape: pltpu.SemaphoreType.DMA(shape)
    return pl.pallas_call(
        layer_kernel,
        in_specs=[hbm] + [vmem] * 5 + [hbm] * 8,
        out_specs=[vmem, vmem],
        out_shape=[
            jax.ShapeDtypeStruct((1, HALF, D), BF16),
            jax.ShapeDtypeStruct((1, 8, ROWS), F32),
        ],
        scratch_shapes=[
            pltpu.VMEM((SEQS, 2, ROWS, 1024), BF16),
            pltpu.VMEM((4, 4, 128, 768), BF16),
            pltpu.VMEM((BLOCKS, MESSAGE, 128), BF16),
            pltpu.VMEM((BLOCKS, MESSAGE, 128), BF16),
            pltpu.VMEM((BLOCKS, HALF, 128), BF16),
            pltpu.VMEM((SEQS, ROWS + 8, 128), F32),
            pltpu.VMEM((SEQS, ROWS, 128), BF16),
            pltpu.VMEM((8, HALF, 128), BF16),
            pltpu.VMEM((8, HALF, 128), BF16),
            pltpu.VMEM((BLOCKS * ROWS, 256), BF16),
            pltpu.VMEM((BLOCKS, HD, ROWS), BF16),
            pltpu.VMEM((BLOCKS // 2, ROWS, 256), BF16),
            [pltpu.VMEM((ROWS, ROWS), F32)] * 4,
            [pltpu.VMEM((ROWS, ROWS), F32)] * 4,
            [pltpu.VMEM((ROWS, ROWS), BF16)] * 4,
            pltpu.VMEM((HD, ROWS), F32),
            pltpu.VMEM((BLOCKS, 96, 128), BF16),
            pltpu.VMEM((BLOCKS, 96, 128), BF16),
            pltpu.VMEM((BLOCKS, 8, 256), F32),
            pltpu.VMEM((BLOCKS, 8, 256), F32),
            pltpu.VMEM((2, 512, D), BF16),
            pltpu.VMEM((2, 512, D), BF16),
            pltpu.VMEM((2, HALF, 1024), BF16),
            pltpu.VMEM((1, 1152), F32),
            pltpu.VMEM((2, 1, 1152), F32),
            dma(31),
            dma(3, 6), dma(3, 6),
            dma(18), dma(18),
            dma(12), dma(12),
            dma(12), dma(12),
            dma(6), dma(6),
            dma(8), dma(8),
            dma(16), dma(16),
            dma(16), dma(16),
            dma(3), dma(3),
            dma(4), dma(4),
            dma(8), dma(8),
            dma(16), dma(16),
            dma(16), dma(16),
        ],
        compiler_params=pltpu.CompilerParams(
            collective_id=0, has_side_effects=True, vmem_limit_bytes=58 << 20
        ),
        name="layer",
    )(tokens, gain, att_gain, conv_gain, offset, taps, *mats, out_att, out_conv)


def per_device(
    tokens,
    in_gain,
    w_query,
    w_key,
    w_value,
    w_outgate,
    w_ingate,
    w_conv_in,
    score_offset,
    conv_taps,
    att_gain,
    conv_gain,
    out_att,
    out_conv,
):
    mixed, mass = layer(
        tokens[0],
        in_gain.reshape(1, D),
        att_gain.reshape(1, 512),
        conv_gain.reshape(1, 512),
        score_offset.reshape(1, 8),
        conv_taps,
        (w_query, w_key, w_value, w_outgate, w_ingate, w_conv_in),
        out_att,
        out_conv,
    )
    return mixed, jnp.swapaxes(mass, 1, 2)


def solution(mesh):
    return jax.shard_map(
        per_device,
        mesh=mesh,
        in_specs=(
            P("fs", "sp", "tp"),
            P(),
            P("fs", "tp"),
            P("fs", "tp"),
            P("fs", "tp"),
            P("fs", "tp"),
            P("fs", "tp"),
            P("fs", "tp"),
            P("tp"),
            P(None, "tp"),
            P("tp"),
            P("tp"),
            P("tp", None),
            P("tp", None),
        ),
        out_specs=(P("fs", ("sp", "tp"), None), P("fs", "sp", "tp")),
        check_vma=False,
    )
```

```python
import functools

import jax
import jax.numpy as jnp
from jax import lax
from jax.experimental import pallas as pl
from jax.experimental.pallas import tpu as pltpu
from jax.sharding import PartitionSpec as P

D = 2048
CONV_CH = 1024
ATT_WIDTH = 1024
SEQS = 4
ROWS = 384
HALF = 192
BLOCKS = 16
HD = 64
MESSAGE = HALF + HALF // 2
epsilon = 1e-06
LOG2E = 1.4426950408889634
F32 = jnp.float32
BF16 = jnp.bfloat16


def dot(a, b):
    return jnp.dot(a, b, preferred_element_type=F32)


def dot_nt(a, b):
    return lax.dot_general(a, b, (((1,), (1,)), ((), ())), preferred_element_type=F32)


def three_parts(x):
    a = x.astype(BF16)
    rest = x - a.astype(F32)
    b = rest.astype(BF16)
    return a, b, (rest - b.astype(F32)).astype(BF16)


MESH = pl.DeviceIdType.MESH
LEFT, RIGHT = slice(0, 384), slice(384, 768)


def mod4(value):
    return lax.rem(value + 8, 4)


def layer_kernel(
    tokens_ref,
    gain_ref,
    att_gain_ref,
    conv_gain_ref,
    offset_ref,
    taps_ref,
    wq_ref,
    wk_ref,
    wv_ref,
    wo_ref,
    wi_ref,
    wc_ref,
    att_ref,
    conv_ref,
    mixed_ref,
    mass_ref,
    tok,
    wts,
    msg,
    recv,
    mate,
    gated,
    outgate,
    branch_out,
    branch_in,
    keys,
    values,
    queries,
    scores,
    decays,
    weights,
    total,
    att_out,
    att_in,
    mass_out,
    mass_in,
    att_weights,
    conv_weights,
    matrix,
    side,
    sides,
    local_sem,
    spread_send,
    spread_recv,
    near_send,
    near_recv,
    far_send,
    far_recv,
    pass_send,
    pass_recv,
    tok_send,
    tok_recv,
    pair_send,
    pair_recv,
    msg_send,
    msg_recv,
    mate_send,
    mate_recv,
    other_send,
    other_recv,
    halo_send,
    halo_recv,
    branch_send,
    branch_recv,
    att_send,
    att_recv,
    mass_send,
    mass_recv,
):
    place, x, core = lax.axis_index("sp"), lax.axis_index("fs"), lax.axis_index("tp")
    y, z = lax.rem(place, 4), lax.div(place, 4)
    sibling = (place, x, 1 - core)
    mats = (wq_ref, wk_ref, wv_ref, wo_ref, wi_ref, wc_ref)

    def remote(src, dst, send, recv_sem, device):
        return pltpu.make_async_remote_copy(
            src_ref=src, dst_ref=dst, send_sem=send, recv_sem=recv_sem, device_id=device, device_id_type=MESH
        )

    own_tokens = pltpu.make_async_copy(tokens_ref, tok.at[x, core], local_sem.at[6])
    own_tokens.start()
    own_weights = []
    for m in range(6):
        for part in range(4):
            own_weights.append(
                pltpu.make_async_copy(
                    mats[m].at[pl.ds(part * 128, 128), pl.ds(pl.multiple_of(x * 128, 128), 128)],
                    wts.at[x, part, :, m * 128 : (m + 1) * 128],
                    local_sem.at[7 + 4 * m + part],
                )
            )
    for copy in own_weights:
        copy.start()

    side[:, 0:512] = att_gain_ref[...]
    side[:, 512:1024] = conv_gain_ref[...]
    side[:, 1024:1152] = jnp.zeros((1, 128), F32)
    side[:, 1024:1032] = offset_ref[...]
    sides[core] = side[...]
    barrier = pltpu.get_barrier_semaphore()
    for k in range(1, 4):
        pl.semaphore_signal(barrier, inc=1, device_id=(place, mod4(x + k), core), device_id_type=MESH)
    pl.semaphore_signal(barrier, inc=1, device_id=sibling, device_id_type=MESH)

    def greet(k, _):
        there = lax.rem(place + k, BLOCKS)
        pl.semaphore_signal(barrier, inc=1, device_id=(there, x, core), device_id_type=MESH)
        pl.semaphore_signal(barrier, inc=1, device_id=(there, x, 1 - core), device_id_type=MESH)
        return 0

    lax.fori_loop(1, BLOCKS, greet, 0)
    number, row = y, z
    seq = mod4(row - number)

    def greet_far(k, _):
        n = lax.rem(k, 4)
        there, column = mod4(x + n) * 4 + n, lax.div(k, 4)
        for other in range(2):

            @pl.when(lax.abs(there - place) + lax.abs(column - x) + lax.abs(other - core) > 0)
            def _():
                pl.semaphore_signal(barrier, inc=1, device_id=(there, column, other), device_id_type=MESH)

        return 0

    lax.fori_loop(0, 16, greet_far, 0)
    pl.semaphore_wait(barrier, 65 + lax.min(lax.abs(seq - x), 1))

    rows_at = pl.multiple_of(place * 32, 32)

    def spread(k, m):
        there = mod4(x + k)
        return remote(
            mats[m].at[pl.ds(rows_at, 32), pl.ds(pl.multiple_of(there * 128, 128), 128)],
            wts.at[x, z, pl.ds(pl.multiple_of(y * 32, 32), 32), m * 128 : (m + 1) * 128],
            spread_send.at[k - 1, m],
            spread_recv.at[k - 1, m],
            (place, there, core),
        )

    for k in range(1, 4):
        for m in range(6):
            spread(k, m).start()

    side_out = remote(side, sides.at[core], other_send.at[2], other_recv.at[2], sibling)
    side_out.start()
    own_tokens.wait()
    top, bottom = pl.ds(0, HALF), pl.ds(HALF, HALF)
    quarters = [pl.ds(96 * i, 96) for i in range(4)]
    odd = lax.rem(y + z, 2)

    def hop(slot, f, rows, by):
        piece = tok.at[f, core, rows]
        return remote(piece, piece, tok_send.at[slot], tok_recv.at[slot], (place, mod4(x + by), core))

    def pair(slot, f, rows):
        piece = tok.at[f, core, rows]
        return remote(piece, piece, pair_send.at[slot], pair_recv.at[slot], sibling)

    right_a, left_b = hop(0, x, top, 1), hop(2, x, bottom, -1)
    right_next, right_last = hop(1, x, quarters[2], 1), hop(6, x, quarters[3], 1)
    left_next, left_last = hop(3, x, quarters[1], -1), hop(7, x, quarters[0], -1)
    before, after, across = mod4(x - 1), mod4(x + 1), mod4(x + 2)
    on_right, on_left = hop(4, before, top, 1), hop(5, after, bottom, -1)
    for copy in (right_a, left_b, right_next, left_next):
        copy.start()

    @pl.when(odd == 0)
    def _():
        right_last.start()
        left_last.start()

    pairs = [
        pair(0, x, top),
        pair(1, x, bottom),
        pair(2, before, top),
        pair(3, after, bottom),
        pair(4, before, bottom),
        pair(5, after, top),
        pair(6, across, top),
        pair(7, across, bottom),
    ]
    pairs[0].start()
    pairs[1].start()

    for k in range(1, 4):
        for m in range(6):
            spread(k, m).wait_recv()

    my_rows = pl.ds(pl.multiple_of(y * 32, 32), 32)

    def near(k, i, way):
        f = mod4(x + i)
        piece = wts.at[f, z, my_rows, (LEFT, RIGHT)[way]]
        there = (z * 4 + mod4(y + k), x, core) if way == 0 else (mod4(z + k) * 4 + y, x, core)
        at = (3 * way + k - 1) * 3 + i - 1
        return remote(piece, piece, near_send.at[at], near_recv.at[at], there)

    for k in range(1, 4):
        for i in range(1, 4):
            for way in range(2):
                near(k, i, way).start()
    for k in range(1, 4):
        for i in range(1, 4):
            for way in range(2):
                near(k, i, way).wait_recv()

    def far(by, i, way):
        f = mod4(x + i)
        if way == 0:
            piece, there = wts.at[f, z, :, LEFT], (mod4(z + by) * 4 + y, x, core)
        else:
            piece, there = wts.at[f, :, my_rows, RIGHT], (z * 4 + mod4(y + by), x, core)
        at = (2 * way + (by + 1) // 2) * 3 + i - 1
        return remote(piece, piece, far_send.at[at], far_recv.at[at], there)

    def onward(by, i, way):
        f = mod4(x + i)
        start = 0 if by == 1 else 1
        if way == 0:
            piece = wts.at[f, mod4(z - by), 64 * start : 64 * start + 64, LEFT]
            there = (mod4(z + by) * 4 + y, x, core)
        else:
            rows = pl.ds(pl.multiple_of(mod4(y - by) * 32, 32), 32)
            piece = wts.at[f, 2 * start : 2 * start + 2, rows, RIGHT]
            there = (z * 4 + mod4(y + by), x, core)
        at = (2 * way + (by + 1) // 2) * 3 + i - 1
        return remote(piece, piece, pass_send.at[at], pass_recv.at[at], there)

    kinds = [(by, i, way) for i in range(1, 4) for by in (1, -1) for way in range(2)]
    for kind in kinds:
        far(*kind).start()
    right_a.wait_recv()
    on_right.start()

    @pl.when(odd == 1)
    def _():
        right_last.start()

    pairs[2].start()
    left_b.wait_recv()
    on_left.start()

    @pl.when(odd == 1)
    def _():
        left_last.start()

    pairs[3].start()
    for kind in kinds:
        far(*kind).wait_recv()
        onward(*kind).start()
    others = [
        remote(att_ref, att_weights.at[core], other_send.at[0], other_recv.at[0], sibling),
        remote(conv_ref, conv_weights.at[core], other_send.at[1], other_recv.at[1], sibling),
    ]
    fetches = [
        pltpu.make_async_copy(att_ref, att_weights.at[core], local_sem.at[0]),
        pltpu.make_async_copy(conv_ref, conv_weights.at[core], local_sem.at[1]),
    ]
    for copy in own_weights:
        copy.wait()
    for kind in kinds:
        onward(*kind).wait_recv()

    def message(s, j, half):
        number = 2 * core + j
        there = mod4(s + number) * 4 + number
        at = 4 * s + 2 * j + half
        return remote(
            msg.at[at], recv.at[place], msg_send.at[at], msg_recv.at[place], (there, x, half)
        ), lax.abs(there - place) + lax.abs(half - core)

    def halo(s):
        return remote(
            gated.at[s, ROWS : ROWS + 8],
            gated.at[s, 0:8],
            halo_send.at[s],
            halo_recv.at[s],
            (lax.rem(place + 1, BLOCKS), x, core),
        )

    def to_home(at):
        s, half = lax.div(at, 2), lax.rem(at, 2)
        mine = 2 * x + core
        return remote(
            branch_out.at[at], branch_in.at[mine], branch_send.at[at], branch_recv.at[mine], (place, s, half)
        ), lax.abs(s - x) + lax.abs(half - core)

    def step(i, _):
        usual = i + lax.div(i, 2) - 2 * lax.div(i, 3)
        other = lax.rem(2 * i, 3) + 3 * lax.div(i, 3)
        s = mod4(x + (1 - odd) * usual + odd * other)

        @pl.when(i == 0)
        def _():
            pairs[0].wait_recv()
            pairs[1].wait_recv()

        @pl.when(i == 1 + odd)
        def _():
            right_next.wait_recv()
            right_last.wait_recv()
            pairs[4].start()
            left_next.wait_recv()
            left_last.wait_recv()
            pairs[5].start()

        @pl.when(i == 3 - 2 * odd)
        def _():
            on_right.wait_recv()
            pairs[6].start()
            on_left.wait_recv()
            pairs[7].start()

        @pl.when(i == 3)
        def _():
            for copy in others + fetches:
                copy.start()

        @pl.when(i == 1 + odd)
        def _():
            pairs[3].wait_recv()
            pairs[5].wait_recv()

        @pl.when(i == 2 + odd)
        def _():
            pairs[2].wait_recv()
            pairs[4].wait_recv()

        @pl.when(i == 3 - 2 * odd)
        def _():
            pairs[6].wait_recv()
            pairs[7].wait_recv()

        low = tok[s, 0].astype(F32)
        high = tok[s, 1].astype(F32)
        squares = jnp.sum(low * low, axis=1, keepdims=True) + jnp.sum(high * high, axis=1, keepdims=True)
        scale = lax.rsqrt(squares / D + epsilon)
        product = dot((low * gain_ref[0:1, 0:1024]).astype(BF16), wts[0:2].reshape(1024, 768)) + dot(
            (high * gain_ref[0:1, 1024:2048]).astype(BF16), wts[2:4].reshape(1024, 768)
        )
        out = (product[:, 128:] * scale).astype(BF16)
        key, value = out[:, 0:128], out[:, 128:256]
        query = (product[:, 0:128] * (scale * (LOG2E / 8))).astype(BF16)
        for j in range(2):
            mine = slice(j * HD, (j + 1) * HD)
            both = jnp.concatenate((key[:, mine], value[:, mine]), axis=1)
            for half in range(2):
                r = half * HALF
                folded = jnp.concatenate((query[r : r + 96, mine], query[r + 96 : r + HALF, mine]), axis=1)
                msg[4 * s + 2 * j + half, 0:HALF, :] = both[r : r + HALF]
                msg[4 * s + 2 * j + half, HALF : HALF + 96, :] = folded
        outgate[s] = out[:, 256:384]
        gated[s, 8 : ROWS + 8, :] = out[:, 384:512].astype(F32) * out[:, 512:640].astype(F32)

        @pl.when(place < BLOCKS - 1)
        def _():
            halo(s).start()

        @pl.when(place == 0)
        def _():
            gated[s, 0:8, :] = jnp.zeros((8, 128), F32)

        for j in range(2):
            for half in range(2):
                copy, apart = message(s, j, half)

                @pl.when(apart > 0)
                def _():
                    copy.start()

                @pl.when(apart == 0)
                def _():
                    recv[place] = msg[4 * s + 2 * j + half]

        return 0

    lax.fori_loop(0, 4, step, 0)

    columns = pl.ds(pl.multiple_of(x * 128, 128), 128)

    def convolve(s, _):
        @pl.when(place > 0)
        def _():
            halo(s).wait_recv()

        convolved = sum(
            taps_ref[t : t + 1, columns] * gated[s, 6 + t : 6 + t + ROWS, :] for t in range(3)
        )
        branch = (outgate[s].astype(F32) * convolved).astype(BF16)
        branch_out[2 * s] = branch[0:HALF]
        branch_out[2 * s + 1] = branch[HALF:ROWS]
        for half in range(2):
            copy, apart = to_home(2 * s + half)

            @pl.when(apart > 0)
            def _():
                copy.start()

            @pl.when(apart == 0)
            def _():
                branch_in[2 * x + core] = branch[half * HALF : (half + 1) * HALF]

        return 0

    lax.fori_loop(0, SEQS, convolve, 0)

    def to_mate(block):
        return remote(
            recv.at[block, 0:HALF], mate.at[block], mate_send.at[block], mate_recv.at[block], sibling
        )

    source_core = lax.div(y, 2)

    lanes = lambda shape: lax.broadcasted_iota(jnp.int32, shape, 1)
    rows = lambda shape: lax.broadcasted_iota(jnp.int32, shape, 0)
    side_out.wait_recv()
    place_of_head = lanes((1, 128)) == 2 * x + lax.rem(number, 2)
    offset_lane = sides[lax.div(number, 2), 0:1, 1024:1152]
    offset = jnp.sum(jnp.where(place_of_head, offset_lane, 0.0), axis=1, keepdims=True) * LOG2E
    offset = jnp.broadcast_to(offset, (HALF, 128))
    o1, o2, o3 = (part.astype(F32) for part in three_parts(offset))
    lane_q = lanes((HALF, 128))
    offset_row = jnp.where(
        lane_q == 0, -o1, jnp.where(lane_q == 1, -o2, jnp.where(lane_q == 2, -o3, 0.0))
    ).astype(BF16)
    square = (ROWS, HALF)
    source = lax.rem(rows(square), 8) * 48 + rows(square) // 8 - lanes(square)
    permute_own = (source == core * HALF).astype(F32).astype(BF16)
    permute_mate = (source == HALF - core * HALF).astype(F32).astype(BF16)
    take_high = (lanes((HD, 128)) == rows((HD, 128)) + HD).astype(F32).astype(BF16)
    ones = (lanes((ROWS, 128)) < 3).astype(F32).astype(BF16)
    low_lane = lanes((96, 128)) < HD

    def prepare(block):
        pair = dot(permute_own, recv[block, 0:HALF, :]) + dot(permute_mate, mate[block])
        pair = pair.astype(BF16)
        at = pl.ds(pl.multiple_of(block * ROWS, ROWS), ROWS)
        keys[at, 0:128] = pair
        keys[at, 128:256] = ones
        values[block] = dot_nt(take_high, pair).astype(BF16)
        packed = recv[block, HALF:MESSAGE, :].astype(F32)
        tile, first = lax.div(block, 2), lax.rem(block, 2) * HALF
        rows_of = lambda start, size: pl.ds(pl.multiple_of(first + start, 32), size)
        queries[tile, rows_of(0, 96), 0:128] = jnp.where(low_lane, packed, 0.0).astype(BF16)
        queries[tile, rows_of(96, 96), 0:128] = jnp.where(
            low_lane, pltpu.roll(packed, HD, 1), 0.0
        ).astype(BF16)
        queries[tile, rows_of(0, HALF), 128:256] = offset_row

    def arrive(k):
        block = lax.rem(place + k, BLOCKS)

        @pl.when(k + lax.abs(source_core - core) > 0)
        def _():
            remote(
                msg.at[0], recv.at[block], msg_send.at[0], msg_recv.at[block], (block, x, source_core)
            ).wait_recv()

        to_mate(block).start()

    def use(k):
        block = lax.rem(place + k, BLOCKS)
        to_mate(block).wait_recv()
        prepare(block)

    arrive(0)
    arrive(1)

    def arrive_and_use(k, _):
        arrive(k)
        use(k - 2)
        return 0

    lax.fori_loop(2, BLOCKS, arrive_and_use, 0)
    use(BLOCKS - 2)
    use(BLOCKS - 1)

    def att_home(block):
        at = 4 * x + number
        apart = lax.abs(block - place) + lax.abs(seq - x)
        return remote(
            att_out.at[block], att_in.at[at], att_send.at[block], att_recv.at[at], (block, seq, core)
        ), apart

    def mass_home(block):
        at = 4 * x + 2 * lax.rem(number, 2) + core
        goal = lax.div(number, 2)
        apart = lax.abs(block - place) + lax.abs(seq - x) + lax.abs(goal - core)
        return remote(
            mass_out.at[block], mass_in.at[at], mass_send.at[block], mass_recv.at[at], (block, seq, goal)
        ), apart

    sub = rows((8, ROWS))
    lane = lanes((8, ROWS))
    where_q = lane + core * HALF + jnp.where(lane < HALF, 0, HALF)

    def score(z_ref, tile_index, block):
        begin = pl.multiple_of(block * ROWS, ROWS)
        z_ref[...] = dot_nt(keys[pl.ds(begin, ROWS), :], queries[tile_index])

    def fold(w_ref, block):
        total[...] += dot(values[block], w_ref[...])

    def decay(z_ref, d_ref, ahead):
        run = jnp.zeros((8, ROWS), F32)
        for r in reversed(range(48)):
            z = z_ref[8 * r : 8 * r + 8, :]
            soft = jnp.maximum(z, lax.log2(1.0 + jnp.exp2(jnp.minimum(z, 126.0))))
            if ahead is not None:
                valid = ahead > r
                soft = jnp.where(valid, soft, 0.0)
            run = run + soft
            value = jnp.exp2(z - run)
            if ahead is not None:
                value = jnp.where(valid, value, 0.0)
            d_ref[8 * r : 8 * r + 8, :] = value
        return run

    def weigh(d_ref, w_ref, run, carry):
        suffix = run
        for step in (1, 2, 4):
            moved = pltpu.roll(suffix, 8 - step, 0)
            suffix = suffix + jnp.where(sub < 8 - step, moved, 0.0)
        after = jnp.where(sub < 7, pltpu.roll(suffix, 7, 0), 0.0)
        kept = jnp.exp2(-(carry + after))
        for i in range(24):
            both = jnp.concatenate(
                (d_ref[16 * i : 16 * i + 8, :] * kept, d_ref[16 * i + 8 : 16 * i + 16, :] * kept), axis=0
            )
            w_ref[16 * i : 16 * i + 16, :] = both.astype(BF16)
        return carry + jnp.broadcast_to(suffix[0:1], (8, ROWS))

    def run_blocks(tile, top, carry, run, aheads, next_tile, next_top):
        count = len(aheads)
        slots = (0, 1, 2, 3) if count == 4 else (0, 3)
        if count == 4:
            score(scores[3], tile, top - 3)
        else:
            score(scores[2], next_tile, lax.max(next_top - 2, 0))
        if run is not None:
            carry = weigh(decays[3], weights[3], run, carry)
        for i in range(count):
            slot = slots[i]
            run = decay(scores[i], decays[slot], aheads[i])
            if i > 0:
                fold(weights[slots[i - 1]], top - i + 1)
            elif aheads[0] is None:
                fold(weights[3], top + 1)
            if i < 3:
                score(scores[i], next_tile, lax.max(next_top - i, 0))
            if i < count - 1:
                carry = weigh(decays[slot], weights[slot], run, carry)
        return carry, run

    last = BLOCKS // 2 - 1
    for i in range(3):
        score(scores[i], last, BLOCKS - 1 - i)

    def one_tile(m, odd):
        total[...] = jnp.zeros_like(total)
        aheads = (where_q - ROWS - 48 * sub, where_q - 48 * sub)
        aheads = aheads + (None, None) if odd else aheads
        begin = 2 * m - 3 if odd else 2 * m - 1
        rest = lax.div(m, 2)
        more = lax.min(rest, 1)
        below = lax.max(m - 1, 0)

        def following(top, stay):
            return stay * m + (1 - stay) * below, stay * top + (1 - stay) * (2 * m - 1)

        state = run_blocks(m, 2 * m + 1, jnp.zeros((8, ROWS), F32), None, aheads, *following(begin, more))

        def earlier(i, state):
            top = begin - 4 * i
            stay = lax.min(lax.div(top, 4), 1)
            return run_blocks(m, top, *state, (None,) * 4, *following(top - 4, stay))

        carry, run = lax.fori_loop(0, rest, earlier, state)
        carry = weigh(decays[3], weights[3], run, carry)
        fold(weights[3], 0)
        attended = total[...]
        attended = jnp.concatenate((attended, attended), axis=0).T
        for part in range(2):
            block = 2 * m + part
            r = part * HALF
            folded = jnp.where(lanes((96, 128)) < HD, attended[r : r + 96], attended[r + 96 : r + HALF])
            folded = folded.astype(BF16)
            mass = carry[:, r : r + HALF]
            att_out[block] = folded
            mass_out[block, :, 0:HALF] = mass
            copy, apart = att_home(block)

            @pl.when(apart > 0)
            def _():
                copy.start()

            @pl.when(apart == 0)
            def _():
                att_in[4 * x + number] = folded

            mass_copy, mass_apart = mass_home(block)

            @pl.when(mass_apart > 0)
            def _():
                mass_copy.start()

            @pl.when(mass_apart == 0)
            def _():
                mass_in[4 * x + 2 * lax.rem(number, 2) + core, :, 0:HALF] = mass

    def two_tiles(step, _):
        one_tile(last - 2 * step, True)
        one_tile(last - 1 - 2 * step, False)
        return 0

    lax.fori_loop(0, BLOCKS // 4, two_tiles, 0)

    for copy in fetches:
        copy.wait()
    for copy in others:
        copy.wait_recv()
    def branch_arrived(k, _):
        there = lax.rem(2 * x + core + k, 8)
        remote(
            branch_out.at[0],
            branch_in.at[there],
            branch_send.at[0],
            branch_recv.at[there],
            (place, lax.div(there, 2), lax.rem(there, 2)),
        ).wait_recv()
        return 0

    lax.fori_loop(1, 8, branch_arrived, 0)

    def branch_product(store, row_gain, projection, load):
        squares = jnp.zeros((HALF, 128), F32)
        for owner in range(2):
            for part in range(4):
                piece = load(owner, part)
                squares = squares + piece * piece
                gain = sides[owner, 0:1, row_gain + 128 * part : row_gain + 128 * part + 128]
                at = 512 * owner + 128 * part
                store[:, at : at + 128] = (piece * gain).astype(BF16)
        scale = lax.rsqrt(jnp.sum(squares, axis=1, keepdims=True) / ATT_WIDTH + epsilon)
        return scale * dot(store[...], projection[...].reshape(1024, D))

    mixed = branch_product(
        matrix.at[0], 512, conv_weights, lambda owner, part: branch_in[2 * part + owner].astype(F32)
    )

    def landed(at, _):
        column, n = lax.div(at, 4), lax.rem(at, 4)
        there = mod4(x + n) * 4 + n
        apart = lax.abs(there - place) + lax.abs(column - x)

        @pl.when(apart > 0)
        def _():
            remote(
                att_out.at[0], att_in.at[at], att_send.at[0], att_recv.at[at], (there, column, core)
            ).wait_recv()

        n = 2 * core + lax.div(n, 2)
        owner = lax.rem(at, 2)
        there = mod4(x + n) * 4 + n
        apart = lax.abs(there - place) + lax.abs(column - x) + lax.abs(owner - core)

        @pl.when(apart > 0)
        def _():
            remote(
                mass_out.at[0], mass_in.at[at], mass_send.at[0], mass_recv.at[at], (there, column, owner)
            ).wait_recv()

        return 0

    lax.fori_loop(0, 16, landed, 0)

    def heads(owner, part):
        a = att_in[4 * part + 2 * owner].astype(F32)
        b = att_in[4 * part + 2 * owner + 1].astype(F32)
        low = lanes((96, 128)) < HD
        upper = jnp.where(low, a, pltpu.roll(b, HD, 1))
        lower = jnp.where(low, pltpu.roll(a, HD, 1), b)
        return jnp.concatenate((upper, lower), axis=0)

    mixed = mixed + branch_product(matrix.at[1], 0, att_weights, heads)
    mixed_ref[0] = mixed.astype(BF16)
    for part in range(2):
        kept = jnp.concatenate([mass_in[2 * n + part, 0:1, :] for n in range(8)], axis=0)
        mass = jnp.log(2.0 - jnp.exp2(-kept))
        mass_ref[0, :, part * HALF : (part + 1) * HALF] = mass[:, 0:HALF]

    def left(block, _):
        copy, apart = att_home(block)

        @pl.when(apart > 0)
        def _():
            copy.wait_send()

        mass_copy, mass_apart = mass_home(block)

        @pl.when(mass_apart > 0)
        def _():
            mass_copy.wait_send()

        return 0

    lax.fori_loop(0, BLOCKS, left, 0)


    for k in range(1, 4):
        for m in range(6):
            spread(k, m).wait_send()
        for i in range(1, 4):
            for way in range(2):
                near(k, i, way).wait_send()
    for kind in kinds:
        far(*kind).wait_send()
        onward(*kind).wait_send()
    for copy in [right_a, right_next, right_last, left_b, left_next, left_last, on_right, on_left] + pairs:
        copy.wait_send()

    def left_here(at, _):
        s = lax.div(at, 4)
        j = lax.div(lax.rem(at, 4), 2)
        copy, apart = message(s, j, lax.rem(at, 2))

        @pl.when(apart > 0)
        def _():
            copy.wait_send()

        to_mate(at).wait_send()
        return 0

    lax.fori_loop(0, BLOCKS, left_here, 0)

    def branch_left(at, _):
        copy, apart = to_home(at)

        @pl.when(apart > 0)
        def _():
            copy.wait_send()

        return 0

    lax.fori_loop(0, 8, branch_left, 0)

    @pl.when(place < BLOCKS - 1)
    def _():
        for s in range(SEQS):
            halo(s).wait_send()

    side_out.wait_send()
    for copy in others:
        copy.wait_send()


def layer(tokens, gain, att_gain, conv_gain, offset, taps, mats, out_att, out_conv):
    hbm = pl.BlockSpec(memory_space=pl.ANY)
    vmem = pl.BlockSpec(memory_space=pltpu.VMEM)
    dma = lambda *shape: pltpu.SemaphoreType.DMA(shape)
    return pl.pallas_call(
        layer_kernel,
        in_specs=[hbm] + [vmem] * 5 + [hbm] * 8,
        out_specs=[vmem, vmem],
        out_shape=[
            jax.ShapeDtypeStruct((1, HALF, D), BF16),
            jax.ShapeDtypeStruct((1, 8, ROWS), F32),
        ],
        scratch_shapes=[
            pltpu.VMEM((SEQS, 2, ROWS, 1024), BF16),
            pltpu.VMEM((4, 4, 128, 768), BF16),
            pltpu.VMEM((BLOCKS, MESSAGE, 128), BF16),
            pltpu.VMEM((BLOCKS, MESSAGE, 128), BF16),
            pltpu.VMEM((BLOCKS, HALF, 128), BF16),
            pltpu.VMEM((SEQS, ROWS + 8, 128), F32),
            pltpu.VMEM((SEQS, ROWS, 128), BF16),
            pltpu.VMEM((8, HALF, 128), BF16),
            pltpu.VMEM((8, HALF, 128), BF16),
            pltpu.VMEM((BLOCKS * ROWS, 256), BF16),
            pltpu.VMEM((BLOCKS, HD, ROWS), BF16),
            pltpu.VMEM((BLOCKS // 2, ROWS, 256), BF16),
            [pltpu.VMEM((ROWS, ROWS), F32)] * 4,
            [pltpu.VMEM((ROWS, ROWS), F32)] * 4,
            [pltpu.VMEM((ROWS, ROWS), BF16)] * 4,
            pltpu.VMEM((HD, ROWS), F32),
            pltpu.VMEM((BLOCKS, 96, 128), BF16),
            pltpu.VMEM((BLOCKS, 96, 128), BF16),
            pltpu.VMEM((BLOCKS, 8, 256), F32),
            pltpu.VMEM((BLOCKS, 8, 256), F32),
            pltpu.VMEM((2, 512, D), BF16),
            pltpu.VMEM((2, 512, D), BF16),
            pltpu.VMEM((2, HALF, 1024), BF16),
            pltpu.VMEM((1, 1152), F32),
            pltpu.VMEM((2, 1, 1152), F32),
            dma(31),
            dma(3, 6), dma(3, 6),
            dma(18), dma(18),
            dma(12), dma(12),
            dma(12), dma(12),
            dma(8), dma(8),
            dma(8), dma(8),
            dma(16), dma(16),
            dma(16), dma(16),
            dma(3), dma(3),
            dma(4), dma(4),
            dma(8), dma(8),
            dma(16), dma(16),
            dma(16), dma(16),
        ],
        compiler_params=pltpu.CompilerParams(
            collective_id=0, has_side_effects=True, vmem_limit_bytes=58 << 20
        ),
        name="layer",
    )(tokens, gain, att_gain, conv_gain, offset, taps, *mats, out_att, out_conv)


def per_device(
    tokens,
    in_gain,
    w_query,
    w_key,
    w_value,
    w_outgate,
    w_ingate,
    w_conv_in,
    score_offset,
    conv_taps,
    att_gain,
    conv_gain,
    out_att,
    out_conv,
):
    mixed, mass = layer(
        tokens[0],
        in_gain.reshape(1, D),
        att_gain.reshape(1, 512),
        conv_gain.reshape(1, 512),
        score_offset.reshape(1, 8),
        conv_taps,
        (w_query, w_key, w_value, w_outgate, w_ingate, w_conv_in),
        out_att,
        out_conv,
    )
    return mixed, jnp.swapaxes(mass, 1, 2)


def solution(mesh):
    return jax.shard_map(
        per_device,
        mesh=mesh,
        in_specs=(
            P("fs", "sp", "tp"),
            P(),
            P("fs", "tp"),
            P("fs", "tp"),
            P("fs", "tp"),
            P("fs", "tp"),
            P("fs", "tp"),
            P("fs", "tp"),
            P("tp"),
            P(None, "tp"),
            P("tp"),
            P("tp"),
            P("tp", None),
            P("tp", None),
        ),
        out_specs=(P("fs", ("sp", "tp"), None), P("fs", "sp", "tp")),
        check_vma=False,
    )
```

```python
import functools

import jax
import jax.numpy as jnp
from jax import lax
from jax.experimental import pallas as pl
from jax.experimental.pallas import tpu as pltpu
from jax.sharding import PartitionSpec as P

D = 2048
CONV_CH = 1024
ATT_WIDTH = 1024
SEQS = 4
ROWS = 384
HALF = 192
BLOCKS = 16
HD = 64
MESSAGE = HALF + HALF // 2
epsilon = 1e-06
LOG2E = 1.4426950408889634
F32 = jnp.float32
BF16 = jnp.bfloat16


def dot(a, b):
    return jnp.dot(a, b, preferred_element_type=F32)


def dot_nt(a, b):
    return lax.dot_general(a, b, (((1,), (1,)), ((), ())), preferred_element_type=F32)


def three_parts(x):
    a = x.astype(BF16)
    rest = x - a.astype(F32)
    b = rest.astype(BF16)
    return a, b, (rest - b.astype(F32)).astype(BF16)


MESH = pl.DeviceIdType.MESH
LEFT, RIGHT = slice(0, 384), slice(384, 768)


def mod4(value):
    return lax.rem(value + 8, 4)


def layer_kernel(
    tokens_ref,
    gain_ref,
    att_gain_ref,
    conv_gain_ref,
    offset_ref,
    taps_ref,
    wq_ref,
    wk_ref,
    wv_ref,
    wo_ref,
    wi_ref,
    wc_ref,
    att_ref,
    conv_ref,
    mixed_ref,
    mass_ref,
    tok,
    wts,
    msg,
    recv,
    mate,
    gated,
    outgate,
    branch_out,
    branch_in,
    keys,
    values,
    queries,
    scores,
    decays,
    weights,
    total,
    att_out,
    att_in,
    mass_out,
    mass_in,
    att_weights,
    conv_weights,
    matrix,
    side,
    sides,
    local_sem,
    spread_send,
    spread_recv,
    near_send,
    near_recv,
    far_send,
    far_recv,
    pass_send,
    pass_recv,
    tok_send,
    tok_recv,
    pair_send,
    pair_recv,
    msg_send,
    msg_recv,
    mate_send,
    mate_recv,
    other_send,
    other_recv,
    halo_send,
    halo_recv,
    branch_send,
    branch_recv,
    att_send,
    att_recv,
    mass_send,
    mass_recv,
):
    place, x, core = lax.axis_index("sp"), lax.axis_index("fs"), lax.axis_index("tp")
    y, z = lax.rem(place, 4), lax.div(place, 4)
    sibling = (place, x, 1 - core)
    mats = (wq_ref, wk_ref, wv_ref, wo_ref, wi_ref, wc_ref)

    def remote(src, dst, send, recv_sem, device):
        return pltpu.make_async_remote_copy(
            src_ref=src, dst_ref=dst, send_sem=send, recv_sem=recv_sem, device_id=device, device_id_type=MESH
        )

    own_tokens = pltpu.make_async_copy(tokens_ref, tok.at[x, core], local_sem.at[6])
    own_tokens.start()
    own_weights = []
    for m in range(6):
        for part in range(4):
            own_weights.append(
                pltpu.make_async_copy(
                    mats[m].at[pl.ds(part * 128, 128), pl.ds(pl.multiple_of(x * 128, 128), 128)],
                    wts.at[x, part, :, m * 128 : (m + 1) * 128],
                    local_sem.at[7 + 4 * m + part],
                )
            )
    for copy in own_weights:
        copy.start()

    side[:, 0:512] = att_gain_ref[...]
    side[:, 512:1024] = conv_gain_ref[...]
    side[:, 1024:1152] = jnp.zeros((1, 128), F32)
    side[:, 1024:1032] = offset_ref[...]
    sides[core] = side[...]
    barrier = pltpu.get_barrier_semaphore()
    for k in range(1, 4):
        pl.semaphore_signal(barrier, inc=1, device_id=(place, mod4(x + k), core), device_id_type=MESH)
    pl.semaphore_signal(barrier, inc=1, device_id=sibling, device_id_type=MESH)

    def greet(k, _):
        there = lax.rem(place + k, BLOCKS)
        pl.semaphore_signal(barrier, inc=1, device_id=(there, x, core), device_id_type=MESH)
        pl.semaphore_signal(barrier, inc=1, device_id=(there, x, 1 - core), device_id_type=MESH)
        return 0

    lax.fori_loop(1, BLOCKS, greet, 0)
    number, row = y, z
    seq = mod4(row - number)

    def greet_far(k, _):
        n = lax.rem(k, 4)
        there, column = mod4(x + n) * 4 + n, lax.div(k, 4)
        for other in range(2):

            @pl.when(lax.abs(there - place) + lax.abs(column - x) + lax.abs(other - core) > 0)
            def _():
                pl.semaphore_signal(barrier, inc=1, device_id=(there, column, other), device_id_type=MESH)

        return 0

    lax.fori_loop(0, 16, greet_far, 0)
    pl.semaphore_wait(barrier, 65 + lax.min(lax.abs(seq - x), 1))

    rows_at = pl.multiple_of(place * 32, 32)

    def spread(k, m):
        there = mod4(x + k)
        return remote(
            mats[m].at[pl.ds(rows_at, 32), pl.ds(pl.multiple_of(there * 128, 128), 128)],
            wts.at[x, z, pl.ds(pl.multiple_of(y * 32, 32), 32), m * 128 : (m + 1) * 128],
            spread_send.at[k - 1, m],
            spread_recv.at[k - 1, m],
            (place, there, core),
        )

    for k in range(1, 4):
        for m in range(6):
            spread(k, m).start()

    side_out = remote(side, sides.at[core], other_send.at[2], other_recv.at[2], sibling)
    side_out.start()
    own_tokens.wait()
    top, bottom = pl.ds(0, HALF), pl.ds(HALF, HALF)
    quarters = [pl.ds(96 * i, 96) for i in range(4)]
    odd = lax.rem(y + z, 2)

    def hop(slot, f, rows, by):
        piece = tok.at[f, core, rows]
        return remote(piece, piece, tok_send.at[slot], tok_recv.at[slot], (place, mod4(x + by), core))

    def pair(slot, f, rows):
        piece = tok.at[f, core, rows]
        return remote(piece, piece, pair_send.at[slot], pair_recv.at[slot], sibling)

    right_a, left_b = hop(0, x, top, 1), hop(2, x, bottom, -1)
    right_next, right_last = hop(1, x, quarters[2], 1), hop(6, x, quarters[3], 1)
    left_next, left_last = hop(3, x, quarters[1], -1), hop(7, x, quarters[0], -1)
    before, after, across = mod4(x - 1), mod4(x + 1), mod4(x + 2)
    on_right, on_left = hop(4, before, top, 1), hop(5, after, bottom, -1)
    for copy in (right_a, left_b, right_next, left_next):
        copy.start()

    @pl.when(odd == 0)
    def _():
        right_last.start()
        left_last.start()

    pairs = [
        pair(0, x, top),
        pair(1, x, bottom),
        pair(2, before, top),
        pair(3, after, bottom),
        pair(4, before, bottom),
        pair(5, after, top),
        pair(6, across, top),
        pair(7, across, bottom),
    ]
    pairs[0].start()
    pairs[1].start()

    for k in range(1, 4):
        for m in range(6):
            spread(k, m).wait_recv()

    my_rows = pl.ds(pl.multiple_of(y * 32, 32), 32)

    def near(k, i, way):
        f = mod4(x + i)
        piece = wts.at[f, z, my_rows, (LEFT, RIGHT)[way]]
        there = (z * 4 + mod4(y + k), x, core) if way == 0 else (mod4(z + k) * 4 + y, x, core)
        at = (3 * way + k - 1) * 3 + i - 1
        return remote(piece, piece, near_send.at[at], near_recv.at[at], there)

    for k in range(1, 4):
        for i in range(1, 4):
            for way in range(2):
                near(k, i, way).start()
    for k in range(1, 4):
        for i in range(1, 4):
            for way in range(2):
                near(k, i, way).wait_recv()

    def far(by, i, way):
        f = mod4(x + i)
        if way == 0:
            piece, there = wts.at[f, z, :, LEFT], (mod4(z + by) * 4 + y, x, core)
        else:
            piece, there = wts.at[f, :, my_rows, RIGHT], (z * 4 + mod4(y + by), x, core)
        at = (2 * way + (by + 1) // 2) * 3 + i - 1
        return remote(piece, piece, far_send.at[at], far_recv.at[at], there)

    def onward(by, i, way):
        f = mod4(x + i)
        start = 0 if by == 1 else 1
        if way == 0:
            piece = wts.at[f, mod4(z - by), 64 * start : 64 * start + 64, LEFT]
            there = (mod4(z + by) * 4 + y, x, core)
        else:
            rows = pl.ds(pl.multiple_of(mod4(y - by) * 32, 32), 32)
            piece = wts.at[f, 2 * start : 2 * start + 2, rows, RIGHT]
            there = (z * 4 + mod4(y + by), x, core)
        at = (2 * way + (by + 1) // 2) * 3 + i - 1
        return remote(piece, piece, pass_send.at[at], pass_recv.at[at], there)

    kinds = [(by, i, way) for i in range(1, 4) for by in (1, -1) for way in range(2)]
    for kind in kinds:
        far(*kind).start()
    right_a.wait_recv()
    on_right.start()

    @pl.when(odd == 1)
    def _():
        right_last.start()

    pairs[2].start()
    left_b.wait_recv()
    on_left.start()

    @pl.when(odd == 1)
    def _():
        left_last.start()

    pairs[3].start()
    for kind in kinds:
        far(*kind).wait_recv()
        onward(*kind).start()
    others = [
        remote(att_ref, att_weights.at[core], other_send.at[0], other_recv.at[0], sibling),
        remote(conv_ref, conv_weights.at[core], other_send.at[1], other_recv.at[1], sibling),
    ]
    fetches = [
        pltpu.make_async_copy(att_ref, att_weights.at[core], local_sem.at[0]),
        pltpu.make_async_copy(conv_ref, conv_weights.at[core], local_sem.at[1]),
    ]
    for copy in own_weights:
        copy.wait()
    for kind in kinds:
        onward(*kind).wait_recv()

    def message(s, j, half):
        number = 2 * core + j
        there = mod4(s + number) * 4 + number
        at = 4 * s + 2 * j + half
        return remote(
            msg.at[at], recv.at[place], msg_send.at[at], msg_recv.at[place], (there, x, half)
        ), lax.abs(there - place) + lax.abs(half - core)

    def halo(s):
        return remote(
            gated.at[s, ROWS : ROWS + 8],
            gated.at[s, 0:8],
            halo_send.at[s],
            halo_recv.at[s],
            (lax.rem(place + 1, BLOCKS), x, core),
        )

    def to_home(at):
        s, half = lax.div(at, 2), lax.rem(at, 2)
        mine = 2 * x + core
        return remote(
            branch_out.at[at], branch_in.at[mine], branch_send.at[at], branch_recv.at[mine], (place, s, half)
        ), lax.abs(s - x) + lax.abs(half - core)

    def step(i, _):
        usual = i + lax.div(i, 2) - 2 * lax.div(i, 3)
        other = lax.rem(2 * i, 3) + 3 * lax.div(i, 3)
        s = mod4(x + (1 - odd) * usual + odd * other)

        @pl.when(i == 0)
        def _():
            pairs[0].wait_recv()
            pairs[1].wait_recv()

        @pl.when(i == 1 + odd)
        def _():
            right_next.wait_recv()
            right_last.wait_recv()
            pairs[4].start()
            left_next.wait_recv()
            left_last.wait_recv()
            pairs[5].start()

        @pl.when(i == 3 - 2 * odd)
        def _():
            on_right.wait_recv()
            pairs[6].start()
            on_left.wait_recv()
            pairs[7].start()

        @pl.when(i == 1 + odd)
        def _():
            pairs[3].wait_recv()
            pairs[5].wait_recv()

        @pl.when(i == 2 + odd)
        def _():
            pairs[2].wait_recv()
            pairs[4].wait_recv()

        @pl.when(i == 3 - 2 * odd)
        def _():
            pairs[6].wait_recv()
            pairs[7].wait_recv()

        low = tok[s, 0].astype(F32)
        high = tok[s, 1].astype(F32)
        squares = jnp.sum(low * low, axis=1, keepdims=True) + jnp.sum(high * high, axis=1, keepdims=True)
        scale = lax.rsqrt(squares / D + epsilon)
        product = dot((low * gain_ref[0:1, 0:1024]).astype(BF16), wts[0:2].reshape(1024, 768)) + dot(
            (high * gain_ref[0:1, 1024:2048]).astype(BF16), wts[2:4].reshape(1024, 768)
        )
        out = (product[:, 128:] * scale).astype(BF16)
        key, value = out[:, 0:128], out[:, 128:256]
        query = (product[:, 0:128] * (scale * (LOG2E / 8))).astype(BF16)
        for j in range(2):
            mine = slice(j * HD, (j + 1) * HD)
            both = jnp.concatenate((key[:, mine], value[:, mine]), axis=1)
            for half in range(2):
                r = half * HALF
                folded = jnp.concatenate((query[r : r + 96, mine], query[r + 96 : r + HALF, mine]), axis=1)
                msg[4 * s + 2 * j + half, 0:HALF, :] = both[r : r + HALF]
                msg[4 * s + 2 * j + half, HALF : HALF + 96, :] = folded
        outgate[s] = out[:, 256:384]
        gated[s, 8 : ROWS + 8, :] = out[:, 384:512].astype(F32) * out[:, 512:640].astype(F32)

        @pl.when(place < BLOCKS - 1)
        def _():
            halo(s).start()

        @pl.when(place == 0)
        def _():
            gated[s, 0:8, :] = jnp.zeros((8, 128), F32)

        for j in range(2):
            for half in range(2):
                copy, apart = message(s, j, half)

                @pl.when(apart > 0)
                def _():
                    copy.start()

                @pl.when(apart == 0)
                def _():
                    recv[place] = msg[4 * s + 2 * j + half]

        return 0

    lax.fori_loop(0, 4, step, 0)

    columns = pl.ds(pl.multiple_of(x * 128, 128), 128)

    def convolve(s, _):
        @pl.when(place > 0)
        def _():
            halo(s).wait_recv()

        convolved = sum(
            taps_ref[t : t + 1, columns] * gated[s, 6 + t : 6 + t + ROWS, :] for t in range(3)
        )
        branch = (outgate[s].astype(F32) * convolved).astype(BF16)
        branch_out[2 * s] = branch[0:HALF]
        branch_out[2 * s + 1] = branch[HALF:ROWS]
        for half in range(2):
            copy, apart = to_home(2 * s + half)

            @pl.when(apart > 0)
            def _():
                copy.start()

            @pl.when(apart == 0)
            def _():
                branch_in[2 * x + core] = branch[half * HALF : (half + 1) * HALF]

        return 0

    lax.fori_loop(0, SEQS, convolve, 0)

    def to_mate(block):
        return remote(
            recv.at[block, 0:HALF], mate.at[block], mate_send.at[block], mate_recv.at[block], sibling
        )

    source_core = lax.div(y, 2)

    lanes = lambda shape: lax.broadcasted_iota(jnp.int32, shape, 1)
    rows = lambda shape: lax.broadcasted_iota(jnp.int32, shape, 0)
    side_out.wait_recv()
    place_of_head = lanes((1, 128)) == 2 * x + lax.rem(number, 2)
    offset_lane = sides[lax.div(number, 2), 0:1, 1024:1152]
    offset = jnp.sum(jnp.where(place_of_head, offset_lane, 0.0), axis=1, keepdims=True) * LOG2E
    offset = jnp.broadcast_to(offset, (HALF, 128))
    o1, o2, o3 = (part.astype(F32) for part in three_parts(offset))
    lane_q = lanes((HALF, 128))
    offset_row = jnp.where(
        lane_q == 0, -o1, jnp.where(lane_q == 1, -o2, jnp.where(lane_q == 2, -o3, 0.0))
    ).astype(BF16)
    square = (ROWS, HALF)
    source = lax.rem(rows(square), 8) * 48 + rows(square) // 8 - lanes(square)
    permute_own = (source == core * HALF).astype(F32).astype(BF16)
    permute_mate = (source == HALF - core * HALF).astype(F32).astype(BF16)
    take_high = (lanes((HD, 128)) == rows((HD, 128)) + HD).astype(F32).astype(BF16)
    ones = (lanes((ROWS, 128)) < 3).astype(F32).astype(BF16)
    low_lane = lanes((96, 128)) < HD

    def prepare(block):
        pair = dot(permute_own, recv[block, 0:HALF, :]) + dot(permute_mate, mate[block])
        pair = pair.astype(BF16)
        at = pl.ds(pl.multiple_of(block * ROWS, ROWS), ROWS)
        keys[at, 0:128] = pair
        keys[at, 128:256] = ones
        values[block] = dot_nt(take_high, pair).astype(BF16)
        packed = recv[block, HALF:MESSAGE, :].astype(F32)
        tile, first = lax.div(block, 2), lax.rem(block, 2) * HALF
        rows_of = lambda start, size: pl.ds(pl.multiple_of(first + start, 32), size)
        queries[tile, rows_of(0, 96), 0:128] = jnp.where(low_lane, packed, 0.0).astype(BF16)
        queries[tile, rows_of(96, 96), 0:128] = jnp.where(
            low_lane, pltpu.roll(packed, HD, 1), 0.0
        ).astype(BF16)
        queries[tile, rows_of(0, HALF), 128:256] = offset_row

    def arrive(k):
        block = lax.rem(place + k, BLOCKS)

        @pl.when(k + lax.abs(source_core - core) > 0)
        def _():
            remote(
                msg.at[0], recv.at[block], msg_send.at[0], msg_recv.at[block], (block, x, source_core)
            ).wait_recv()

        to_mate(block).start()

    def use(k):
        block = lax.rem(place + k, BLOCKS)
        to_mate(block).wait_recv()
        prepare(block)

    arrive(0)
    arrive(1)

    def arrive_and_use(k, _):
        arrive(k)
        use(k - 2)
        return 0

    lax.fori_loop(2, BLOCKS, arrive_and_use, 0)
    for copy in others + fetches:
        copy.start()
    use(BLOCKS - 2)
    use(BLOCKS - 1)

    def att_home(block):
        at = 4 * x + number
        apart = lax.abs(block - place) + lax.abs(seq - x)
        return remote(
            att_out.at[block], att_in.at[at], att_send.at[block], att_recv.at[at], (block, seq, core)
        ), apart

    def mass_home(block):
        at = 4 * x + 2 * lax.rem(number, 2) + core
        goal = lax.div(number, 2)
        apart = lax.abs(block - place) + lax.abs(seq - x) + lax.abs(goal - core)
        return remote(
            mass_out.at[block], mass_in.at[at], mass_send.at[block], mass_recv.at[at], (block, seq, goal)
        ), apart

    sub = rows((8, ROWS))
    lane = lanes((8, ROWS))
    where_q = lane + core * HALF + jnp.where(lane < HALF, 0, HALF)

    def score(z_ref, tile_index, block):
        begin = pl.multiple_of(block * ROWS, ROWS)
        z_ref[...] = dot_nt(keys[pl.ds(begin, ROWS), :], queries[tile_index])

    def fold(w_ref, block):
        total[...] += dot(values[block], w_ref[...])

    def decay(z_ref, d_ref, ahead, last_block):
        skip = 128 if last_block else 0
        if last_block:
            ahead = ahead[:, skip:]
            d_ref[:, 0:skip] = jnp.zeros((ROWS, skip), F32)
        run = jnp.zeros((8, ROWS - skip), F32)
        for r in reversed(range(48)):
            z = z_ref[8 * r : 8 * r + 8, skip:]
            soft = jnp.maximum(z, lax.log2(1.0 + jnp.exp2(jnp.minimum(z, 126.0))))
            if ahead is not None:
                valid = ahead > r
                soft = jnp.where(valid, soft, 0.0)
            run = run + soft
            value = jnp.exp2(z - run)
            if ahead is not None:
                value = jnp.where(valid, value, 0.0)
            d_ref[8 * r : 8 * r + 8, skip:] = value
        if last_block:
            run = jnp.concatenate((jnp.zeros((8, skip), F32), run), axis=1)
        return run

    def weigh(d_ref, w_ref, run, carry):
        suffix = run
        for step in (1, 2, 4):
            moved = pltpu.roll(suffix, 8 - step, 0)
            suffix = suffix + jnp.where(sub < 8 - step, moved, 0.0)
        after = jnp.where(sub < 7, pltpu.roll(suffix, 7, 0), 0.0)
        kept = jnp.exp2(-(carry + after))
        for i in range(24):
            both = jnp.concatenate(
                (d_ref[16 * i : 16 * i + 8, :] * kept, d_ref[16 * i + 8 : 16 * i + 16, :] * kept), axis=0
            )
            w_ref[16 * i : 16 * i + 16, :] = both.astype(BF16)
        return carry + jnp.broadcast_to(suffix[0:1], (8, ROWS))

    def run_blocks(tile, top, carry, run, aheads, next_tile, next_top):
        count = len(aheads)
        slots = (0, 1, 2, 3) if count == 4 else (0, 3)
        if count == 4:
            score(scores[3], tile, top - 3)
        else:
            score(scores[2], next_tile, lax.max(next_top - 2, 0))
        if run is not None:
            carry = weigh(decays[3], weights[3], run, carry)
        for i in range(count):
            slot = slots[i]
            run = decay(scores[i], decays[slot], aheads[i], i == 0 and aheads[0] is not None)
            if i > 0:
                fold(weights[slots[i - 1]], top - i + 1)
            elif aheads[0] is None:
                fold(weights[3], top + 1)
            if i < 3:
                score(scores[i], next_tile, lax.max(next_top - i, 0))
            if i < count - 1:
                carry = weigh(decays[slot], weights[slot], run, carry)
        return carry, run

    last = BLOCKS // 2 - 1
    for i in range(3):
        score(scores[i], last, BLOCKS - 1 - i)

    def one_tile(m, odd):
        total[...] = jnp.zeros_like(total)
        aheads = (where_q - ROWS - 48 * sub, where_q - 48 * sub)
        aheads = aheads + (None, None) if odd else aheads
        begin = 2 * m - 3 if odd else 2 * m - 1
        rest = lax.div(m, 2)
        more = lax.min(rest, 1)
        below = lax.max(m - 1, 0)

        def following(top, stay):
            return stay * m + (1 - stay) * below, stay * top + (1 - stay) * (2 * m - 1)

        state = run_blocks(m, 2 * m + 1, jnp.zeros((8, ROWS), F32), None, aheads, *following(begin, more))

        def earlier(i, state):
            top = begin - 4 * i
            stay = lax.min(lax.div(top, 4), 1)
            return run_blocks(m, top, *state, (None,) * 4, *following(top - 4, stay))

        carry, run = lax.fori_loop(0, rest, earlier, state)
        carry = weigh(decays[3], weights[3], run, carry)
        fold(weights[3], 0)
        attended = total[...]
        attended = jnp.concatenate((attended, attended), axis=0).T
        for part in range(2):
            block = 2 * m + part
            r = part * HALF
            folded = jnp.where(lanes((96, 128)) < HD, attended[r : r + 96], attended[r + 96 : r + HALF])
            folded = folded.astype(BF16)
            mass = carry[:, r : r + HALF]
            att_out[block] = folded
            mass_out[block, :, 0:HALF] = mass
            copy, apart = att_home(block)

            @pl.when(apart > 0)
            def _():
                copy.start()

            @pl.when(apart == 0)
            def _():
                att_in[4 * x + number] = folded

            mass_copy, mass_apart = mass_home(block)

            @pl.when(mass_apart > 0)
            def _():
                mass_copy.start()

            @pl.when(mass_apart == 0)
            def _():
                mass_in[4 * x + 2 * lax.rem(number, 2) + core, :, 0:HALF] = mass

    def two_tiles(step, _):
        one_tile(last - 2 * step, True)
        one_tile(last - 1 - 2 * step, False)
        return 0

    lax.fori_loop(0, BLOCKS // 4, two_tiles, 0)

    for copy in fetches:
        copy.wait()
    for copy in others:
        copy.wait_recv()
    def branch_arrived(k, _):
        there = lax.rem(2 * x + core + k, 8)
        remote(
            branch_out.at[0],
            branch_in.at[there],
            branch_send.at[0],
            branch_recv.at[there],
            (place, lax.div(there, 2), lax.rem(there, 2)),
        ).wait_recv()
        return 0

    lax.fori_loop(1, 8, branch_arrived, 0)

    def branch_product(store, row_gain, projection, load):
        squares = jnp.zeros((HALF, 128), F32)
        for owner in range(2):
            for part in range(4):
                piece = load(owner, part)
                squares = squares + piece * piece
                gain = sides[owner, 0:1, row_gain + 128 * part : row_gain + 128 * part + 128]
                at = 512 * owner + 128 * part
                store[:, at : at + 128] = (piece * gain).astype(BF16)
        scale = lax.rsqrt(jnp.sum(squares, axis=1, keepdims=True) / ATT_WIDTH + epsilon)
        return scale * dot(store[...], projection[...].reshape(1024, D))

    mixed = branch_product(
        matrix.at[0], 512, conv_weights, lambda owner, part: branch_in[2 * part + owner].astype(F32)
    )

    def landed(at, _):
        column, n = lax.div(at, 4), lax.rem(at, 4)
        there = mod4(x + n) * 4 + n
        apart = lax.abs(there - place) + lax.abs(column - x)

        @pl.when(apart > 0)
        def _():
            remote(
                att_out.at[0], att_in.at[at], att_send.at[0], att_recv.at[at], (there, column, core)
            ).wait_recv()

        n = 2 * core + lax.div(n, 2)
        owner = lax.rem(at, 2)
        there = mod4(x + n) * 4 + n
        apart = lax.abs(there - place) + lax.abs(column - x) + lax.abs(owner - core)

        @pl.when(apart > 0)
        def _():
            remote(
                mass_out.at[0], mass_in.at[at], mass_send.at[0], mass_recv.at[at], (there, column, owner)
            ).wait_recv()

        return 0

    lax.fori_loop(0, 16, landed, 0)

    def heads(owner, part):
        a = att_in[4 * part + 2 * owner].astype(F32)
        b = att_in[4 * part + 2 * owner + 1].astype(F32)
        low = lanes((96, 128)) < HD
        upper = jnp.where(low, a, pltpu.roll(b, HD, 1))
        lower = jnp.where(low, pltpu.roll(a, HD, 1), b)
        return jnp.concatenate((upper, lower), axis=0)

    mixed = mixed + branch_product(matrix.at[1], 0, att_weights, heads)
    mixed_ref[0] = mixed.astype(BF16)
    for part in range(2):
        kept = jnp.concatenate([mass_in[2 * n + part, 0:1, :] for n in range(8)], axis=0)
        mass = jnp.log(2.0 - jnp.exp2(-kept))
        mass_ref[0, :, part * HALF : (part + 1) * HALF] = mass[:, 0:HALF]

    def left(block, _):
        copy, apart = att_home(block)

        @pl.when(apart > 0)
        def _():
            copy.wait_send()

        mass_copy, mass_apart = mass_home(block)

        @pl.when(mass_apart > 0)
        def _():
            mass_copy.wait_send()

        return 0

    lax.fori_loop(0, BLOCKS, left, 0)


    for k in range(1, 4):
        for m in range(6):
            spread(k, m).wait_send()
        for i in range(1, 4):
            for way in range(2):
                near(k, i, way).wait_send()
    for kind in kinds:
        far(*kind).wait_send()
        onward(*kind).wait_send()
    for copy in [right_a, right_next, right_last, left_b, left_next, left_last, on_right, on_left] + pairs:
        copy.wait_send()

    def left_here(at, _):
        s = lax.div(at, 4)
        j = lax.div(lax.rem(at, 4), 2)
        copy, apart = message(s, j, lax.rem(at, 2))

        @pl.when(apart > 0)
        def _():
            copy.wait_send()

        to_mate(at).wait_send()
        return 0

    lax.fori_loop(0, BLOCKS, left_here, 0)

    def branch_left(at, _):
        copy, apart = to_home(at)

        @pl.when(apart > 0)
        def _():
            copy.wait_send()

        return 0

    lax.fori_loop(0, 8, branch_left, 0)

    @pl.when(place < BLOCKS - 1)
    def _():
        for s in range(SEQS):
            halo(s).wait_send()

    side_out.wait_send()
    for copy in others:
        copy.wait_send()


def layer(tokens, gain, att_gain, conv_gain, offset, taps, mats, out_att, out_conv):
    hbm = pl.BlockSpec(memory_space=pl.ANY)
    vmem = pl.BlockSpec(memory_space=pltpu.VMEM)
    dma = lambda *shape: pltpu.SemaphoreType.DMA(shape)
    return pl.pallas_call(
        layer_kernel,
        in_specs=[hbm] + [vmem] * 5 + [hbm] * 8,
        out_specs=[vmem, vmem],
        out_shape=[
            jax.ShapeDtypeStruct((1, HALF, D), BF16),
            jax.ShapeDtypeStruct((1, 8, ROWS), F32),
        ],
        scratch_shapes=[
            pltpu.VMEM((SEQS, 2, ROWS, 1024), BF16),
            pltpu.VMEM((4, 4, 128, 768), BF16),
            pltpu.VMEM((BLOCKS, MESSAGE, 128), BF16),
            pltpu.VMEM((BLOCKS, MESSAGE, 128), BF16),
            pltpu.VMEM((BLOCKS, HALF, 128), BF16),
            pltpu.VMEM((SEQS, ROWS + 8, 128), F32),
            pltpu.VMEM((SEQS, ROWS, 128), BF16),
            pltpu.VMEM((8, HALF, 128), BF16),
            pltpu.VMEM((8, HALF, 128), BF16),
            pltpu.VMEM((BLOCKS * ROWS, 256), BF16),
            pltpu.VMEM((BLOCKS, HD, ROWS), BF16),
            pltpu.VMEM((BLOCKS // 2, ROWS, 256), BF16),
            [pltpu.VMEM((ROWS, ROWS), F32)] * 4,
            [pltpu.VMEM((ROWS, ROWS), F32)] * 4,
            [pltpu.VMEM((ROWS, ROWS), BF16)] * 4,
            pltpu.VMEM((HD, ROWS), F32),
            pltpu.VMEM((BLOCKS, 96, 128), BF16),
            pltpu.VMEM((BLOCKS, 96, 128), BF16),
            pltpu.VMEM((BLOCKS, 8, 256), F32),
            pltpu.VMEM((BLOCKS, 8, 256), F32),
            pltpu.VMEM((2, 512, D), BF16),
            pltpu.VMEM((2, 512, D), BF16),
            pltpu.VMEM((2, HALF, 1024), BF16),
            pltpu.VMEM((1, 1152), F32),
            pltpu.VMEM((2, 1, 1152), F32),
            dma(31),
            dma(3, 6), dma(3, 6),
            dma(18), dma(18),
            dma(12), dma(12),
            dma(12), dma(12),
            dma(8), dma(8),
            dma(8), dma(8),
            dma(16), dma(16),
            dma(16), dma(16),
            dma(3), dma(3),
            dma(4), dma(4),
            dma(8), dma(8),
            dma(16), dma(16),
            dma(16), dma(16),
        ],
        compiler_params=pltpu.CompilerParams(
            collective_id=0, has_side_effects=True, vmem_limit_bytes=58 << 20
        ),
        name="layer",
    )(tokens, gain, att_gain, conv_gain, offset, taps, *mats, out_att, out_conv)


def per_device(
    tokens,
    in_gain,
    w_query,
    w_key,
    w_value,
    w_outgate,
    w_ingate,
    w_conv_in,
    score_offset,
    conv_taps,
    att_gain,
    conv_gain,
    out_att,
    out_conv,
):
    mixed, mass = layer(
        tokens[0],
        in_gain.reshape(1, D),
        att_gain.reshape(1, 512),
        conv_gain.reshape(1, 512),
        score_offset.reshape(1, 8),
        conv_taps,
        (w_query, w_key, w_value, w_outgate, w_ingate, w_conv_in),
        out_att,
        out_conv,
    )
    return mixed, jnp.swapaxes(mass, 1, 2)


def solution(mesh):
    return jax.shard_map(
        per_device,
        mesh=mesh,
        in_specs=(
            P("fs", "sp", "tp"),
            P(),
            P("fs", "tp"),
            P("fs", "tp"),
            P("fs", "tp"),
            P("fs", "tp"),
            P("fs", "tp"),
            P("fs", "tp"),
            P("tp"),
            P(None, "tp"),
            P("tp"),
            P("tp"),
            P("tp", None),
            P("tp", None),
        ),
        out_specs=(P("fs", ("sp", "tp"), None), P("fs", "sp", "tp")),
        check_vma=False,
    )
```

```python
import functools

import jax
import jax.numpy as jnp
from jax import lax
from jax.experimental import pallas as pl
from jax.experimental.pallas import tpu as pltpu
from jax.sharding import PartitionSpec as P

D = 2048
CONV_CH = 1024
ATT_WIDTH = 1024
SEQS = 4
ROWS = 384
HALF = 192
BLOCKS = 16
HD = 64
MESSAGE = HALF + HALF // 2
epsilon = 1e-06
LOG2E = 1.4426950408889634
F32 = jnp.float32
BF16 = jnp.bfloat16


def dot(a, b):
    return jnp.dot(a, b, preferred_element_type=F32)


def dot_nt(a, b):
    return lax.dot_general(a, b, (((1,), (1,)), ((), ())), preferred_element_type=F32)


def three_parts(x):
    a = x.astype(BF16)
    rest = x - a.astype(F32)
    b = rest.astype(BF16)
    return a, b, (rest - b.astype(F32)).astype(BF16)


MESH = pl.DeviceIdType.MESH
LEFT, RIGHT = slice(0, 384), slice(384, 768)


def mod4(value):
    return lax.rem(value + 8, 4)


def layer_kernel(
    tokens_ref,
    gain_ref,
    att_gain_ref,
    conv_gain_ref,
    offset_ref,
    taps_ref,
    wq_ref,
    wk_ref,
    wv_ref,
    wo_ref,
    wi_ref,
    wc_ref,
    att_ref,
    conv_ref,
    mixed_ref,
    mass_ref,
    tok,
    wts,
    msg,
    recv,
    mate,
    gated,
    outgate,
    branch_out,
    branch_in,
    keys,
    values,
    queries,
    scores,
    decays,
    weights,
    total,
    att_out,
    att_in,
    mass_out,
    mass_in,
    att_weights,
    conv_weights,
    matrix,
    side,
    sides,
    local_sem,
    spread_send,
    spread_recv,
    near_send,
    near_recv,
    far_send,
    far_recv,
    pass_send,
    pass_recv,
    tok_send,
    tok_recv,
    pair_send,
    pair_recv,
    msg_send,
    msg_recv,
    mate_send,
    mate_recv,
    other_send,
    other_recv,
    halo_send,
    halo_recv,
    branch_send,
    branch_recv,
    att_send,
    att_recv,
    mass_send,
    mass_recv,
):
    place, x, core = lax.axis_index("sp"), lax.axis_index("fs"), lax.axis_index("tp")
    y, z = lax.rem(place, 4), lax.div(place, 4)
    sibling = (place, x, 1 - core)
    mats = (wq_ref, wk_ref, wv_ref, wo_ref, wi_ref, wc_ref)

    def remote(src, dst, send, recv_sem, device):
        return pltpu.make_async_remote_copy(
            src_ref=src, dst_ref=dst, send_sem=send, recv_sem=recv_sem, device_id=device, device_id_type=MESH
        )

    own_tokens = pltpu.make_async_copy(tokens_ref, tok.at[x, core], local_sem.at[6])
    own_tokens.start()
    own_weights = []
    for m in range(6):
        for part in range(4):
            own_weights.append(
                pltpu.make_async_copy(
                    mats[m].at[pl.ds(part * 128, 128), pl.ds(pl.multiple_of(x * 128, 128), 128)],
                    wts.at[x, part, :, m * 128 : (m + 1) * 128],
                    local_sem.at[7 + 4 * m + part],
                )
            )
    for copy in own_weights:
        copy.start()

    side[:, 0:512] = att_gain_ref[...]
    side[:, 512:1024] = conv_gain_ref[...]
    side[:, 1024:1152] = jnp.zeros((1, 128), F32)
    side[:, 1024:1032] = offset_ref[...]
    sides[core] = side[...]
    barrier = pltpu.get_barrier_semaphore()
    for k in range(1, 4):
        pl.semaphore_signal(barrier, inc=1, device_id=(place, mod4(x + k), core), device_id_type=MESH)
    pl.semaphore_signal(barrier, inc=1, device_id=sibling, device_id_type=MESH)

    def greet(k, _):
        there = lax.rem(place + k, BLOCKS)
        pl.semaphore_signal(barrier, inc=1, device_id=(there, x, core), device_id_type=MESH)
        pl.semaphore_signal(barrier, inc=1, device_id=(there, x, 1 - core), device_id_type=MESH)
        return 0

    lax.fori_loop(1, BLOCKS, greet, 0)
    number, row = y, z
    seq = mod4(row - number)

    def greet_far(k, _):
        n = lax.rem(k, 4)
        there, column = mod4(x + n) * 4 + n, lax.div(k, 4)
        for other in range(2):

            @pl.when(lax.abs(there - place) + lax.abs(column - x) + lax.abs(other - core) > 0)
            def _():
                pl.semaphore_signal(barrier, inc=1, device_id=(there, column, other), device_id_type=MESH)

        return 0

    lax.fori_loop(0, 16, greet_far, 0)
    pl.semaphore_wait(barrier, 65 + lax.min(lax.abs(seq - x), 1))

    rows_at = pl.multiple_of(place * 32, 32)

    def spread(k, m):
        there = mod4(x + k)
        return remote(
            mats[m].at[pl.ds(rows_at, 32), pl.ds(pl.multiple_of(there * 128, 128), 128)],
            wts.at[x, z, pl.ds(pl.multiple_of(y * 32, 32), 32), m * 128 : (m + 1) * 128],
            spread_send.at[k - 1, m],
            spread_recv.at[k - 1, m],
            (place, there, core),
        )

    for k in range(1, 4):
        for m in range(6):
            spread(k, m).start()

    side_out = remote(side, sides.at[core], other_send.at[2], other_recv.at[2], sibling)
    side_out.start()
    own_tokens.wait()
    top, bottom = pl.ds(0, HALF), pl.ds(HALF, HALF)
    quarters = [pl.ds(96 * i, 96) for i in range(4)]
    odd = lax.rem(y + z, 2)

    def hop(slot, f, rows, by):
        piece = tok.at[f, core, rows]
        return remote(piece, piece, tok_send.at[slot], tok_recv.at[slot], (place, mod4(x + by), core))

    def pair(slot, f, rows):
        piece = tok.at[f, core, rows]
        return remote(piece, piece, pair_send.at[slot], pair_recv.at[slot], sibling)

    right_a, left_b = hop(0, x, top, 1), hop(2, x, bottom, -1)
    right_next, right_last = hop(1, x, quarters[2], 1), hop(6, x, quarters[3], 1)
    left_next, left_last = hop(3, x, quarters[1], -1), hop(7, x, quarters[0], -1)
    before, after, across = mod4(x - 1), mod4(x + 1), mod4(x + 2)
    on_right, on_left = hop(4, before, top, 1), hop(5, after, bottom, -1)
    for copy in (right_a, left_b, right_next, left_next):
        copy.start()

    @pl.when(odd == 0)
    def _():
        right_last.start()
        left_last.start()

    pairs = [
        pair(0, x, top),
        pair(1, x, bottom),
        pair(2, before, top),
        pair(3, after, bottom),
        pair(4, before, bottom),
        pair(5, after, top),
        pair(6, across, top),
        pair(7, across, bottom),
    ]
    pairs[0].start()
    pairs[1].start()

    my_rows = pl.ds(pl.multiple_of(y * 32, 32), 32)

    def near(k, i, way):
        f = mod4(x + i)
        piece = wts.at[f, z, my_rows, (LEFT, RIGHT)[way]]
        there = (z * 4 + mod4(y + k), x, core) if way == 0 else (mod4(z + k) * 4 + y, x, core)
        at = (3 * way + k - 1) * 3 + i - 1
        return remote(piece, piece, near_send.at[at], near_recv.at[at], there)

    pieces = (3, 1, 2)
    for i in pieces:
        for m in range(6):
            spread(4 - i, m).wait_recv()
        for k in range(1, 4):
            for way in range(2):
                near(k, i, way).start()

    def far(by, i, way):
        f = mod4(x + i)
        if way == 0:
            piece, there = wts.at[f, z, :, LEFT], (mod4(z + by) * 4 + y, x, core)
        else:
            piece, there = wts.at[f, :, my_rows, RIGHT], (z * 4 + mod4(y + by), x, core)
        at = (2 * way + (by + 1) // 2) * 3 + i - 1
        return remote(piece, piece, far_send.at[at], far_recv.at[at], there)

    def onward(by, i, way):
        f = mod4(x + i)
        start = 0 if by == 1 else 1
        if way == 0:
            piece = wts.at[f, mod4(z - by), 64 * start : 64 * start + 64, LEFT]
            there = (mod4(z + by) * 4 + y, x, core)
        else:
            rows = pl.ds(pl.multiple_of(mod4(y - by) * 32, 32), 32)
            piece = wts.at[f, 2 * start : 2 * start + 2, rows, RIGHT]
            there = (z * 4 + mod4(y + by), x, core)
        at = (2 * way + (by + 1) // 2) * 3 + i - 1
        return remote(piece, piece, pass_send.at[at], pass_recv.at[at], there)

    kinds = [(by, i, way) for i in pieces for by in (1, -1) for way in range(2)]
    for i in pieces:
        for k in range(1, 4):
            for way in range(2):
                near(k, i, way).wait_recv()
        for by in (1, -1):
            for way in range(2):
                far(by, i, way).start()
    right_a.wait_recv()
    on_right.start()

    @pl.when(odd == 1)
    def _():
        right_last.start()

    pairs[2].start()
    left_b.wait_recv()
    on_left.start()

    @pl.when(odd == 1)
    def _():
        left_last.start()

    pairs[3].start()
    for kind in kinds:
        far(*kind).wait_recv()
        onward(*kind).start()
    others = [
        remote(att_ref, att_weights.at[core], other_send.at[0], other_recv.at[0], sibling),
        remote(conv_ref, conv_weights.at[core], other_send.at[1], other_recv.at[1], sibling),
    ]
    fetches = [
        pltpu.make_async_copy(att_ref, att_weights.at[core], local_sem.at[0]),
        pltpu.make_async_copy(conv_ref, conv_weights.at[core], local_sem.at[1]),
    ]
    for copy in own_weights:
        copy.wait()
    for kind in kinds:
        onward(*kind).wait_recv()

    def message(s, j, half):
        number = 2 * core + j
        there = mod4(s + number) * 4 + number
        at = 4 * s + 2 * j + half
        return remote(
            msg.at[at], recv.at[place], msg_send.at[at], msg_recv.at[place], (there, x, half)
        ), lax.abs(there - place) + lax.abs(half - core)

    def halo(s):
        return remote(
            gated.at[s, ROWS : ROWS + 8],
            gated.at[s, 0:8],
            halo_send.at[s],
            halo_recv.at[s],
            (lax.rem(place + 1, BLOCKS), x, core),
        )

    def to_home(at):
        s, half = lax.div(at, 2), lax.rem(at, 2)
        mine = 2 * x + core
        return remote(
            branch_out.at[at], branch_in.at[mine], branch_send.at[at], branch_recv.at[mine], (place, s, half)
        ), lax.abs(s - x) + lax.abs(half - core)

    def step(i, _):
        usual = i + lax.div(i, 2) - 2 * lax.div(i, 3)
        other = lax.rem(2 * i, 3) + 3 * lax.div(i, 3)
        s = mod4(x + (1 - odd) * usual + odd * other)

        @pl.when(i == 0)
        def _():
            pairs[0].wait_recv()
            pairs[1].wait_recv()

        @pl.when(i == 1 + odd)
        def _():
            right_next.wait_recv()
            right_last.wait_recv()
            pairs[4].start()
            left_next.wait_recv()
            left_last.wait_recv()
            pairs[5].start()

        @pl.when(i == 3 - 2 * odd)
        def _():
            on_right.wait_recv()
            pairs[6].start()
            on_left.wait_recv()
            pairs[7].start()

        @pl.when(i == 1 + odd)
        def _():
            pairs[3].wait_recv()
            pairs[5].wait_recv()

        @pl.when(i == 2 + odd)
        def _():
            pairs[2].wait_recv()
            pairs[4].wait_recv()

        @pl.when(i == 3 - 2 * odd)
        def _():
            pairs[6].wait_recv()
            pairs[7].wait_recv()

        low = tok[s, 0].astype(F32)
        high = tok[s, 1].astype(F32)
        squares = jnp.sum(low * low, axis=1, keepdims=True) + jnp.sum(high * high, axis=1, keepdims=True)
        scale = lax.rsqrt(squares / D + epsilon)
        product = dot((low * gain_ref[0:1, 0:1024]).astype(BF16), wts[0:2].reshape(1024, 768)) + dot(
            (high * gain_ref[0:1, 1024:2048]).astype(BF16), wts[2:4].reshape(1024, 768)
        )
        out = (product[:, 128:] * scale).astype(BF16)
        key, value = out[:, 0:128], out[:, 128:256]
        query = (product[:, 0:128] * (scale * (LOG2E / 8))).astype(BF16)
        for j in range(2):
            mine = slice(j * HD, (j + 1) * HD)
            both = jnp.concatenate((key[:, mine], value[:, mine]), axis=1)
            for half in range(2):
                r = half * HALF
                folded = jnp.concatenate((query[r : r + 96, mine], query[r + 96 : r + HALF, mine]), axis=1)
                msg[4 * s + 2 * j + half, 0:HALF, :] = both[r : r + HALF]
                msg[4 * s + 2 * j + half, HALF : HALF + 96, :] = folded
        outgate[s] = out[:, 256:384]
        gated[s, 8 : ROWS + 8, :] = out[:, 384:512].astype(F32) * out[:, 512:640].astype(F32)

        @pl.when(place < BLOCKS - 1)
        def _():
            halo(s).start()

        @pl.when(place == 0)
        def _():
            gated[s, 0:8, :] = jnp.zeros((8, 128), F32)

        for j in range(2):
            for half in range(2):
                copy, apart = message(s, j, half)

                @pl.when(apart > 0)
                def _():
                    copy.start()

                @pl.when(apart == 0)
                def _():
                    recv[place] = msg[4 * s + 2 * j + half]

        return 0

    lax.fori_loop(0, 4, step, 0)

    columns = pl.ds(pl.multiple_of(x * 128, 128), 128)

    def convolve(s, _):
        @pl.when(place > 0)
        def _():
            halo(s).wait_recv()

        convolved = sum(
            taps_ref[t : t + 1, columns] * gated[s, 6 + t : 6 + t + ROWS, :] for t in range(3)
        )
        branch = (outgate[s].astype(F32) * convolved).astype(BF16)
        branch_out[2 * s] = branch[0:HALF]
        branch_out[2 * s + 1] = branch[HALF:ROWS]
        for half in range(2):
            copy, apart = to_home(2 * s + half)

            @pl.when(apart > 0)
            def _():
                copy.start()

            @pl.when(apart == 0)
            def _():
                branch_in[2 * x + core] = branch[half * HALF : (half + 1) * HALF]

        return 0

    lax.fori_loop(0, SEQS, convolve, 0)

    def to_mate(block):
        return remote(
            recv.at[block, 0:HALF], mate.at[block], mate_send.at[block], mate_recv.at[block], sibling
        )

    source_core = lax.div(y, 2)

    lanes = lambda shape: lax.broadcasted_iota(jnp.int32, shape, 1)
    rows = lambda shape: lax.broadcasted_iota(jnp.int32, shape, 0)
    side_out.wait_recv()
    place_of_head = lanes((1, 128)) == 2 * x + lax.rem(number, 2)
    offset_lane = sides[lax.div(number, 2), 0:1, 1024:1152]
    offset = jnp.sum(jnp.where(place_of_head, offset_lane, 0.0), axis=1, keepdims=True) * LOG2E
    offset = jnp.broadcast_to(offset, (HALF, 128))
    o1, o2, o3 = (part.astype(F32) for part in three_parts(offset))
    lane_q = lanes((HALF, 128))
    offset_row = jnp.where(
        lane_q == 0, -o1, jnp.where(lane_q == 1, -o2, jnp.where(lane_q == 2, -o3, 0.0))
    ).astype(BF16)
    square = (ROWS, HALF)
    source = lax.rem(rows(square), 8) * 48 + rows(square) // 8 - lanes(square)
    permute_own = (source == core * HALF).astype(F32).astype(BF16)
    permute_mate = (source == HALF - core * HALF).astype(F32).astype(BF16)
    take_high = (lanes((HD, 128)) == rows((HD, 128)) + HD).astype(F32).astype(BF16)
    ones = (lanes((ROWS, 128)) < 3).astype(F32).astype(BF16)
    low_lane = lanes((96, 128)) < HD

    def prepare(block):
        pair = dot(permute_own, recv[block, 0:HALF, :]) + dot(permute_mate, mate[block])
        pair = pair.astype(BF16)
        at = pl.ds(pl.multiple_of(block * ROWS, ROWS), ROWS)
        keys[at, 0:128] = pair
        keys[at, 128:256] = ones
        values[block] = dot_nt(take_high, pair).astype(BF16)
        packed = recv[block, HALF:MESSAGE, :].astype(F32)
        tile, first = lax.div(block, 2), lax.rem(block, 2) * HALF
        rows_of = lambda start, size: pl.ds(pl.multiple_of(first + start, 32), size)
        queries[tile, rows_of(0, 96), 0:128] = jnp.where(low_lane, packed, 0.0).astype(BF16)
        queries[tile, rows_of(96, 96), 0:128] = jnp.where(
            low_lane, pltpu.roll(packed, HD, 1), 0.0
        ).astype(BF16)
        queries[tile, rows_of(0, HALF), 128:256] = offset_row

    def arrive(k):
        block = lax.rem(place + k, BLOCKS)

        @pl.when(k + lax.abs(source_core - core) > 0)
        def _():
            remote(
                msg.at[0], recv.at[block], msg_send.at[0], msg_recv.at[block], (block, x, source_core)
            ).wait_recv()

        to_mate(block).start()

    def use(k):
        block = lax.rem(place + k, BLOCKS)
        to_mate(block).wait_recv()
        prepare(block)

    arrive(0)
    arrive(1)

    def arrive_and_use(k, _):
        arrive(k)
        use(k - 2)
        return 0

    lax.fori_loop(2, BLOCKS, arrive_and_use, 0)
    for copy in others + fetches:
        copy.start()
    use(BLOCKS - 2)
    use(BLOCKS - 1)

    def att_home(block):
        at = 4 * x + number
        apart = lax.abs(block - place) + lax.abs(seq - x)
        return remote(
            att_out.at[block], att_in.at[at], att_send.at[block], att_recv.at[at], (block, seq, core)
        ), apart

    def mass_home(block):
        at = 4 * x + 2 * lax.rem(number, 2) + core
        goal = lax.div(number, 2)
        apart = lax.abs(block - place) + lax.abs(seq - x) + lax.abs(goal - core)
        return remote(
            mass_out.at[block], mass_in.at[at], mass_send.at[block], mass_recv.at[at], (block, seq, goal)
        ), apart

    sub = rows((8, ROWS))
    lane = lanes((8, ROWS))
    where_q = lane + core * HALF + jnp.where(lane < HALF, 0, HALF)

    def score(z_ref, tile_index, block):
        begin = pl.multiple_of(block * ROWS, ROWS)
        z_ref[...] = dot_nt(keys[pl.ds(begin, ROWS), :], queries[tile_index])

    def fold(w_ref, block):
        total[...] += dot(values[block], w_ref[...])

    def decay(z_ref, d_ref, ahead, last_block):
        skip = 128 if last_block else 0
        if last_block:
            ahead = ahead[:, skip:]
            d_ref[:, 0:skip] = jnp.zeros((ROWS, skip), F32)
        run = jnp.zeros((8, ROWS - skip), F32)
        for r in reversed(range(48)):
            z = z_ref[8 * r : 8 * r + 8, skip:]
            soft = jnp.maximum(z, lax.log2(1.0 + jnp.exp2(jnp.minimum(z, 126.0))))
            if ahead is not None:
                valid = ahead > r
                soft = jnp.where(valid, soft, 0.0)
            run = run + soft
            value = jnp.exp2(z - run)
            if ahead is not None:
                value = jnp.where(valid, value, 0.0)
            d_ref[8 * r : 8 * r + 8, skip:] = value
        if last_block:
            run = jnp.concatenate((jnp.zeros((8, skip), F32), run), axis=1)
        return run

    def weigh(d_ref, w_ref, run, carry):
        suffix = run
        for step in (1, 2, 4):
            moved = pltpu.roll(suffix, 8 - step, 0)
            suffix = suffix + jnp.where(sub < 8 - step, moved, 0.0)
        after = jnp.where(sub < 7, pltpu.roll(suffix, 7, 0), 0.0)
        kept = jnp.exp2(-(carry + after))
        for i in range(24):
            both = jnp.concatenate(
                (d_ref[16 * i : 16 * i + 8, :] * kept, d_ref[16 * i + 8 : 16 * i + 16, :] * kept), axis=0
            )
            w_ref[16 * i : 16 * i + 16, :] = both.astype(BF16)
        return carry + jnp.broadcast_to(suffix[0:1], (8, ROWS))

    def run_blocks(tile, top, carry, run, aheads, next_tile, next_top):
        count = len(aheads)
        slots = (0, 1, 2, 3) if count == 4 else (0, 3)
        if count == 4:
            score(scores[3], tile, top - 3)
        else:
            score(scores[2], next_tile, lax.max(next_top - 2, 0))
        if run is not None:
            carry = weigh(decays[3], weights[3], run, carry)
        for i in range(count):
            slot = slots[i]
            run = decay(scores[i], decays[slot], aheads[i], i == 0 and aheads[0] is not None)
            if i > 0:
                fold(weights[slots[i - 1]], top - i + 1)
            elif aheads[0] is None:
                fold(weights[3], top + 1)
            if i < 3:
                score(scores[i], next_tile, lax.max(next_top - i, 0))
            if i < count - 1:
                carry = weigh(decays[slot], weights[slot], run, carry)
        return carry, run

    last = BLOCKS // 2 - 1
    for i in range(3):
        score(scores[i], last, BLOCKS - 1 - i)

    def one_tile(m, odd):
        total[...] = jnp.zeros_like(total)
        aheads = (where_q - ROWS - 48 * sub, where_q - 48 * sub)
        aheads = aheads + (None, None) if odd else aheads
        begin = 2 * m - 3 if odd else 2 * m - 1
        rest = lax.div(m, 2)
        more = lax.min(rest, 1)
        below = lax.max(m - 1, 0)

        def following(top, stay):
            return stay * m + (1 - stay) * below, stay * top + (1 - stay) * (2 * m - 1)

        state = run_blocks(m, 2 * m + 1, jnp.zeros((8, ROWS), F32), None, aheads, *following(begin, more))

        def earlier(i, state):
            top = begin - 4 * i
            stay = lax.min(lax.div(top, 4), 1)
            return run_blocks(m, top, *state, (None,) * 4, *following(top - 4, stay))

        carry, run = lax.fori_loop(0, rest, earlier, state)
        carry = weigh(decays[3], weights[3], run, carry)
        fold(weights[3], 0)
        attended = total[...]
        attended = jnp.concatenate((attended, attended), axis=0).T
        for part in range(2):
            block = 2 * m + part
            r = part * HALF
            folded = jnp.where(lanes((96, 128)) < HD, attended[r : r + 96], attended[r + 96 : r + HALF])
            folded = folded.astype(BF16)
            mass = carry[:, r : r + HALF]
            att_out[block] = folded
            mass_out[block, :, 0:HALF] = mass
            copy, apart = att_home(block)

            @pl.when(apart > 0)
            def _():
                copy.start()

            @pl.when(apart == 0)
            def _():
                att_in[4 * x + number] = folded

            mass_copy, mass_apart = mass_home(block)

            @pl.when(mass_apart > 0)
            def _():
                mass_copy.start()

            @pl.when(mass_apart == 0)
            def _():
                mass_in[4 * x + 2 * lax.rem(number, 2) + core, :, 0:HALF] = mass

    def two_tiles(step, _):
        one_tile(last - 2 * step, True)
        one_tile(last - 1 - 2 * step, False)
        return 0

    lax.fori_loop(0, BLOCKS // 4, two_tiles, 0)

    for copy in fetches:
        copy.wait()
    for copy in others:
        copy.wait_recv()
    def branch_arrived(k, _):
        there = lax.rem(2 * x + core + k, 8)
        remote(
            branch_out.at[0],
            branch_in.at[there],
            branch_send.at[0],
            branch_recv.at[there],
            (place, lax.div(there, 2), lax.rem(there, 2)),
        ).wait_recv()
        return 0

    lax.fori_loop(1, 8, branch_arrived, 0)

    def branch_product(store, row_gain, projection, load):
        squares = jnp.zeros((HALF, 128), F32)
        for owner in range(2):
            for part in range(4):
                piece = load(owner, part)
                squares = squares + piece * piece
                gain = sides[owner, 0:1, row_gain + 128 * part : row_gain + 128 * part + 128]
                at = 512 * owner + 128 * part
                store[:, at : at + 128] = (piece * gain).astype(BF16)
        scale = lax.rsqrt(jnp.sum(squares, axis=1, keepdims=True) / ATT_WIDTH + epsilon)
        return scale * dot(store[...], projection[...].reshape(1024, D))

    mixed = branch_product(
        matrix.at[0], 512, conv_weights, lambda owner, part: branch_in[2 * part + owner].astype(F32)
    )

    def landed(at, _):
        column, n = lax.div(at, 4), lax.rem(at, 4)
        there = mod4(x + n) * 4 + n
        apart = lax.abs(there - place) + lax.abs(column - x)

        @pl.when(apart > 0)
        def _():
            remote(
                att_out.at[0], att_in.at[at], att_send.at[0], att_recv.at[at], (there, column, core)
            ).wait_recv()

        n = 2 * core + lax.div(n, 2)
        owner = lax.rem(at, 2)
        there = mod4(x + n) * 4 + n
        apart = lax.abs(there - place) + lax.abs(column - x) + lax.abs(owner - core)

        @pl.when(apart > 0)
        def _():
            remote(
                mass_out.at[0], mass_in.at[at], mass_send.at[0], mass_recv.at[at], (there, column, owner)
            ).wait_recv()

        return 0

    lax.fori_loop(0, 16, landed, 0)

    def heads(owner, part):
        a = att_in[4 * part + 2 * owner].astype(F32)
        b = att_in[4 * part + 2 * owner + 1].astype(F32)
        low = lanes((96, 128)) < HD
        upper = jnp.where(low, a, pltpu.roll(b, HD, 1))
        lower = jnp.where(low, pltpu.roll(a, HD, 1), b)
        return jnp.concatenate((upper, lower), axis=0)

    mixed = mixed + branch_product(matrix.at[1], 0, att_weights, heads)
    mixed_ref[0] = mixed.astype(BF16)
    for part in range(2):
        kept = jnp.concatenate([mass_in[2 * n + part, 0:1, :] for n in range(8)], axis=0)
        mass = jnp.log(2.0 - jnp.exp2(-kept))
        mass_ref[0, :, part * HALF : (part + 1) * HALF] = mass[:, 0:HALF]

    def left(block, _):
        copy, apart = att_home(block)

        @pl.when(apart > 0)
        def _():
            copy.wait_send()

        mass_copy, mass_apart = mass_home(block)

        @pl.when(mass_apart > 0)
        def _():
            mass_copy.wait_send()

        return 0

    lax.fori_loop(0, BLOCKS, left, 0)


    for k in range(1, 4):
        for m in range(6):
            spread(k, m).wait_send()
        for i in range(1, 4):
            for way in range(2):
                near(k, i, way).wait_send()
    for kind in kinds:
        far(*kind).wait_send()
        onward(*kind).wait_send()
    for copy in [right_a, right_next, right_last, left_b, left_next, left_last, on_right, on_left] + pairs:
        copy.wait_send()

    def left_here(at, _):
        s = lax.div(at, 4)
        j = lax.div(lax.rem(at, 4), 2)
        copy, apart = message(s, j, lax.rem(at, 2))

        @pl.when(apart > 0)
        def _():
            copy.wait_send()

        to_mate(at).wait_send()
        return 0

    lax.fori_loop(0, BLOCKS, left_here, 0)

    def branch_left(at, _):
        copy, apart = to_home(at)

        @pl.when(apart > 0)
        def _():
            copy.wait_send()

        return 0

    lax.fori_loop(0, 8, branch_left, 0)

    @pl.when(place < BLOCKS - 1)
    def _():
        for s in range(SEQS):
            halo(s).wait_send()

    side_out.wait_send()
    for copy in others:
        copy.wait_send()


def layer(tokens, gain, att_gain, conv_gain, offset, taps, mats, out_att, out_conv):
    hbm = pl.BlockSpec(memory_space=pl.ANY)
    vmem = pl.BlockSpec(memory_space=pltpu.VMEM)
    dma = lambda *shape: pltpu.SemaphoreType.DMA(shape)
    return pl.pallas_call(
        layer_kernel,
        in_specs=[hbm] + [vmem] * 5 + [hbm] * 8,
        out_specs=[vmem, vmem],
        out_shape=[
            jax.ShapeDtypeStruct((1, HALF, D), BF16),
            jax.ShapeDtypeStruct((1, 8, ROWS), F32),
        ],
        scratch_shapes=[
            pltpu.VMEM((SEQS, 2, ROWS, 1024), BF16),
            pltpu.VMEM((4, 4, 128, 768), BF16),
            pltpu.VMEM((BLOCKS, MESSAGE, 128), BF16),
            pltpu.VMEM((BLOCKS, MESSAGE, 128), BF16),
            pltpu.VMEM((BLOCKS, HALF, 128), BF16),
            pltpu.VMEM((SEQS, ROWS + 8, 128), F32),
            pltpu.VMEM((SEQS, ROWS, 128), BF16),
            pltpu.VMEM((8, HALF, 128), BF16),
            pltpu.VMEM((8, HALF, 128), BF16),
            pltpu.VMEM((BLOCKS * ROWS, 256), BF16),
            pltpu.VMEM((BLOCKS, HD, ROWS), BF16),
            pltpu.VMEM((BLOCKS // 2, ROWS, 256), BF16),
            [pltpu.VMEM((ROWS, ROWS), F32)] * 4,
            [pltpu.VMEM((ROWS, ROWS), F32)] * 4,
            [pltpu.VMEM((ROWS, ROWS), BF16)] * 4,
            pltpu.VMEM((HD, ROWS), F32),
            pltpu.VMEM((BLOCKS, 96, 128), BF16),
            pltpu.VMEM((BLOCKS, 96, 128), BF16),
            pltpu.VMEM((BLOCKS, 8, 256), F32),
            pltpu.VMEM((BLOCKS, 8, 256), F32),
            pltpu.VMEM((2, 512, D), BF16),
            pltpu.VMEM((2, 512, D), BF16),
            pltpu.VMEM((2, HALF, 1024), BF16),
            pltpu.VMEM((1, 1152), F32),
            pltpu.VMEM((2, 1, 1152), F32),
            dma(31),
            dma(3, 6), dma(3, 6),
            dma(18), dma(18),
            dma(12), dma(12),
            dma(12), dma(12),
            dma(8), dma(8),
            dma(8), dma(8),
            dma(16), dma(16),
            dma(16), dma(16),
            dma(3), dma(3),
            dma(4), dma(4),
            dma(8), dma(8),
            dma(16), dma(16),
            dma(16), dma(16),
        ],
        compiler_params=pltpu.CompilerParams(
            collective_id=0, has_side_effects=True, vmem_limit_bytes=58 << 20
        ),
        name="layer",
    )(tokens, gain, att_gain, conv_gain, offset, taps, *mats, out_att, out_conv)


def per_device(
    tokens,
    in_gain,
    w_query,
    w_key,
    w_value,
    w_outgate,
    w_ingate,
    w_conv_in,
    score_offset,
    conv_taps,
    att_gain,
    conv_gain,
    out_att,
    out_conv,
):
    mixed, mass = layer(
        tokens[0],
        in_gain.reshape(1, D),
        att_gain.reshape(1, 512),
        conv_gain.reshape(1, 512),
        score_offset.reshape(1, 8),
        conv_taps,
        (w_query, w_key, w_value, w_outgate, w_ingate, w_conv_in),
        out_att,
        out_conv,
    )
    return mixed, jnp.swapaxes(mass, 1, 2)


def solution(mesh):
    return jax.shard_map(
        per_device,
        mesh=mesh,
        in_specs=(
            P("fs", "sp", "tp"),
            P(),
            P("fs", "tp"),
            P("fs", "tp"),
            P("fs", "tp"),
            P("fs", "tp"),
            P("fs", "tp"),
            P("fs", "tp"),
            P("tp"),
            P(None, "tp"),
            P("tp"),
            P("tp"),
            P("tp", None),
            P("tp", None),
        ),
        out_specs=(P("fs", ("sp", "tp"), None), P("fs", "sp", "tp")),
        check_vma=False,
    )
```

```python
import functools

import jax
import jax.numpy as jnp
from jax import lax
from jax.experimental import pallas as pl
from jax.experimental.pallas import tpu as pltpu
from jax.sharding import PartitionSpec as P

D = 2048
CONV_CH = 1024
ATT_WIDTH = 1024
SEQS = 4
ROWS = 384
HALF = 192
BLOCKS = 16
HD = 64
MESSAGE = HALF + HALF // 2
epsilon = 1e-06
LOG2E = 1.4426950408889634
F32 = jnp.float32
BF16 = jnp.bfloat16


def dot(a, b):
    return jnp.dot(a, b, preferred_element_type=F32)


def dot_nt(a, b):
    return lax.dot_general(a, b, (((1,), (1,)), ((), ())), preferred_element_type=F32)


def three_parts(x):
    a = x.astype(BF16)
    rest = x - a.astype(F32)
    b = rest.astype(BF16)
    return a, b, (rest - b.astype(F32)).astype(BF16)


MESH = pl.DeviceIdType.MESH
LEFT, RIGHT = slice(0, 384), slice(384, 768)


def mod4(value):
    return lax.rem(value + 8, 4)


def layer_kernel(
    tokens_ref,
    gain_ref,
    att_gain_ref,
    conv_gain_ref,
    offset_ref,
    taps_ref,
    wq_ref,
    wk_ref,
    wv_ref,
    wo_ref,
    wi_ref,
    wc_ref,
    att_ref,
    conv_ref,
    mixed_ref,
    mass_ref,
    tok,
    wts,
    msg,
    recv,
    mate,
    gated,
    outgate,
    branch_out,
    branch_in,
    keys,
    values,
    queries,
    scores,
    decays,
    weights,
    total,
    att_out,
    att_in,
    mass_out,
    mass_in,
    att_weights,
    conv_weights,
    matrix,
    side,
    sides,
    local_sem,
    spread_send,
    spread_recv,
    near_send,
    near_recv,
    far_send,
    far_recv,
    pass_send,
    pass_recv,
    tok_send,
    tok_recv,
    pair_send,
    pair_recv,
    msg_send,
    msg_recv,
    mate_send,
    mate_recv,
    other_send,
    other_recv,
    halo_send,
    halo_recv,
    branch_send,
    branch_recv,
    att_send,
    att_recv,
    mass_send,
    mass_recv,
):
    place, x, core = lax.axis_index("sp"), lax.axis_index("fs"), lax.axis_index("tp")
    y, z = lax.rem(place, 4), lax.div(place, 4)
    sibling = (place, x, 1 - core)
    mats = (wq_ref, wk_ref, wv_ref, wo_ref, wi_ref, wc_ref)

    def remote(src, dst, send, recv_sem, device):
        return pltpu.make_async_remote_copy(
            src_ref=src, dst_ref=dst, send_sem=send, recv_sem=recv_sem, device_id=device, device_id_type=MESH
        )

    own_tokens = pltpu.make_async_copy(tokens_ref, tok.at[x, core], local_sem.at[6])
    own_tokens.start()
    own_weights = []
    for m in range(6):
        for part in range(4):
            own_weights.append(
                pltpu.make_async_copy(
                    mats[m].at[pl.ds(part * 128, 128), pl.ds(pl.multiple_of(x * 128, 128), 128)],
                    wts.at[x, part, :, m * 128 : (m + 1) * 128],
                    local_sem.at[7 + 4 * m + part],
                )
            )
    for copy in own_weights:
        copy.start()

    side[:, 0:512] = att_gain_ref[...]
    side[:, 512:1024] = conv_gain_ref[...]
    side[:, 1024:1152] = jnp.zeros((1, 128), F32)
    side[:, 1024:1032] = offset_ref[...]
    sides[core] = side[...]
    barrier = pltpu.get_barrier_semaphore()
    for k in range(1, 4):
        pl.semaphore_signal(barrier, inc=1, device_id=(place, mod4(x + k), core), device_id_type=MESH)
    pl.semaphore_signal(barrier, inc=1, device_id=sibling, device_id_type=MESH)

    def greet(k, _):
        there = lax.rem(place + k, BLOCKS)
        pl.semaphore_signal(barrier, inc=1, device_id=(there, x, core), device_id_type=MESH)
        pl.semaphore_signal(barrier, inc=1, device_id=(there, x, 1 - core), device_id_type=MESH)
        return 0

    lax.fori_loop(1, BLOCKS, greet, 0)
    number, row = y, z
    seq = mod4(row - number)

    def greet_far(k, _):
        n = lax.rem(k, 4)
        there, column = mod4(x + n) * 4 + n, lax.div(k, 4)
        for other in range(2):

            @pl.when(lax.abs(there - place) + lax.abs(column - x) + lax.abs(other - core) > 0)
            def _():
                pl.semaphore_signal(barrier, inc=1, device_id=(there, column, other), device_id_type=MESH)

        return 0

    lax.fori_loop(0, 16, greet_far, 0)
    pl.semaphore_wait(barrier, 65 + lax.min(lax.abs(seq - x), 1))

    rows_at = pl.multiple_of(place * 32, 32)

    def spread(k, m):
        there = mod4(x + k)
        return remote(
            mats[m].at[pl.ds(rows_at, 32), pl.ds(pl.multiple_of(there * 128, 128), 128)],
            wts.at[x, z, pl.ds(pl.multiple_of(y * 32, 32), 32), m * 128 : (m + 1) * 128],
            spread_send.at[k - 1, m],
            spread_recv.at[k - 1, m],
            (place, there, core),
        )

    for k in range(1, 4):
        for m in range(6):
            spread(k, m).start()

    side_out = remote(side, sides.at[core], other_send.at[2], other_recv.at[2], sibling)
    side_out.start()
    own_tokens.wait()
    top, bottom = pl.ds(0, HALF), pl.ds(HALF, HALF)
    quarters = [pl.ds(96 * i, 96) for i in range(4)]
    odd = lax.rem(y + z, 2)

    def hop(slot, f, rows, by):
        piece = tok.at[f, core, rows]
        return remote(piece, piece, tok_send.at[slot], tok_recv.at[slot], (place, mod4(x + by), core))

    def pair(slot, f, rows):
        piece = tok.at[f, core, rows]
        return remote(piece, piece, pair_send.at[slot], pair_recv.at[slot], sibling)

    right_a, left_b = hop(0, x, top, 1), hop(2, x, bottom, -1)
    right_next, right_last = hop(1, x, quarters[2], 1), hop(6, x, quarters[3], 1)
    left_next, left_last = hop(3, x, quarters[1], -1), hop(7, x, quarters[0], -1)
    before, after, across = mod4(x - 1), mod4(x + 1), mod4(x + 2)
    on_right, on_left = hop(4, before, top, 1), hop(5, after, bottom, -1)
    for copy in (right_a, left_b, right_next, left_next):
        copy.start()

    @pl.when(odd == 0)
    def _():
        right_last.start()
        left_last.start()

    pairs = [
        pair(0, x, top),
        pair(1, x, bottom),
        pair(2, before, top),
        pair(3, after, bottom),
        pair(4, before, bottom),
        pair(5, after, top),
        pair(6, across, top),
        pair(7, across, bottom),
    ]
    pairs[0].start()
    pairs[1].start()

    my_rows = pl.ds(pl.multiple_of(y * 32, 32), 32)

    def near(k, i, way):
        f = mod4(x + i)
        piece = wts.at[f, z, my_rows, (LEFT, RIGHT)[way]]
        there = (z * 4 + mod4(y + k), x, core) if way == 0 else (mod4(z + k) * 4 + y, x, core)
        at = (3 * way + k - 1) * 3 + i - 1
        return remote(piece, piece, near_send.at[at], near_recv.at[at], there)

    pieces = (3, 1, 2)
    for i in pieces:
        for m in range(6):
            spread(4 - i, m).wait_recv()
        for k in range(1, 4):
            for way in range(2):
                near(k, i, way).start()

    def far(by, i, way):
        f = mod4(x + i)
        if way == 0:
            piece, there = wts.at[f, z, :, LEFT], (mod4(z + by) * 4 + y, x, core)
        else:
            piece, there = wts.at[f, :, my_rows, RIGHT], (z * 4 + mod4(y + by), x, core)
        at = (2 * way + (by + 1) // 2) * 3 + i - 1
        return remote(piece, piece, far_send.at[at], far_recv.at[at], there)

    def onward(by, i, way):
        f = mod4(x + i)
        start = 0 if by == 1 else 1
        if way == 0:
            piece = wts.at[f, mod4(z - by), 64 * start : 64 * start + 64, LEFT]
            there = (mod4(z + by) * 4 + y, x, core)
        else:
            rows = pl.ds(pl.multiple_of(mod4(y - by) * 32, 32), 32)
            piece = wts.at[f, 2 * start : 2 * start + 2, rows, RIGHT]
            there = (z * 4 + mod4(y + by), x, core)
        at = (2 * way + (by + 1) // 2) * 3 + i - 1
        return remote(piece, piece, pass_send.at[at], pass_recv.at[at], there)

    kinds = [(by, i, way) for i in pieces for by in (1, -1) for way in range(2)]
    for i in pieces:
        for k in range(1, 4):
            for way in range(2):
                near(k, i, way).wait_recv()
        for by in (1, -1):
            for way in range(2):
                far(by, i, way).start()
    right_a.wait_recv()
    on_right.start()

    @pl.when(odd == 1)
    def _():
        right_last.start()

    pairs[2].start()
    left_b.wait_recv()
    on_left.start()

    @pl.when(odd == 1)
    def _():
        left_last.start()

    pairs[3].start()
    for kind in kinds:
        far(*kind).wait_recv()
        onward(*kind).start()
    others = [
        remote(att_ref, att_weights.at[core], other_send.at[0], other_recv.at[0], sibling),
        remote(conv_ref, conv_weights.at[core], other_send.at[1], other_recv.at[1], sibling),
    ]
    fetches = [
        pltpu.make_async_copy(att_ref, att_weights.at[core], local_sem.at[0]),
        pltpu.make_async_copy(conv_ref, conv_weights.at[core], local_sem.at[1]),
    ]
    for copy in own_weights:
        copy.wait()
    for kind in kinds:
        onward(*kind).wait_recv()

    def message(s, j, half):
        number = 2 * core + j
        there = mod4(s + number) * 4 + number
        at = 4 * s + 2 * j + half
        return remote(
            msg.at[at], recv.at[place], msg_send.at[at], msg_recv.at[place], (there, x, half)
        ), lax.abs(there - place) + lax.abs(half - core)

    def halo(s):
        return remote(
            gated.at[s, ROWS : ROWS + 8],
            gated.at[s, 0:8],
            halo_send.at[s],
            halo_recv.at[s],
            (lax.rem(place + 1, BLOCKS), x, core),
        )

    def to_home(at):
        s, half = lax.div(at, 2), lax.rem(at, 2)
        mine = 2 * x + core
        return remote(
            branch_out.at[at], branch_in.at[mine], branch_send.at[at], branch_recv.at[mine], (place, s, half)
        ), lax.abs(s - x) + lax.abs(half - core)

    def step(i, _):
        usual = i + lax.div(i, 2) - 2 * lax.div(i, 3)
        other = lax.rem(2 * i, 3) + 3 * lax.div(i, 3)
        s = mod4(x + (1 - odd) * usual + odd * other)

        @pl.when(i == 0)
        def _():
            pairs[0].wait_recv()
            pairs[1].wait_recv()

        @pl.when(i == 1 + odd)
        def _():
            right_next.wait_recv()
            right_last.wait_recv()
            pairs[4].start()
            left_next.wait_recv()
            left_last.wait_recv()
            pairs[5].start()

        @pl.when(i == 3 - 2 * odd)
        def _():
            on_right.wait_recv()
            pairs[6].start()
            on_left.wait_recv()
            pairs[7].start()

        @pl.when(i == 1 + odd)
        def _():
            pairs[3].wait_recv()
            pairs[5].wait_recv()

        @pl.when(i == 2 + odd)
        def _():
            pairs[2].wait_recv()
            pairs[4].wait_recv()

        @pl.when(i == 3 - 2 * odd)
        def _():
            pairs[6].wait_recv()
            pairs[7].wait_recv()

        low = tok[s, 0].astype(F32)
        high = tok[s, 1].astype(F32)
        squares = jnp.sum(low * low, axis=1, keepdims=True) + jnp.sum(high * high, axis=1, keepdims=True)
        scale = lax.rsqrt(squares / D + epsilon)
        product = dot((low * gain_ref[0:1, 0:1024]).astype(BF16), wts[0:2].reshape(1024, 768)) + dot(
            (high * gain_ref[0:1, 1024:2048]).astype(BF16), wts[2:4].reshape(1024, 768)
        )
        out = (product[:, 128:] * scale).astype(BF16)
        key, value = out[:, 0:128], out[:, 128:256]
        query = (product[:, 0:128] * (scale * (LOG2E / 8))).astype(BF16)
        for j in range(2):
            mine = slice(j * HD, (j + 1) * HD)
            both = jnp.concatenate((key[:, mine], value[:, mine]), axis=1)
            for half in range(2):
                r = half * HALF
                folded = jnp.concatenate((query[r : r + 96, mine], query[r + 96 : r + HALF, mine]), axis=1)
                msg[4 * s + 2 * j + half, 0:HALF, :] = both[r : r + HALF]
                msg[4 * s + 2 * j + half, HALF : HALF + 96, :] = folded
        outgate[s] = out[:, 256:384]
        gated[s, 8 : ROWS + 8, :] = out[:, 384:512].astype(F32) * out[:, 512:640].astype(F32)

        @pl.when(place < BLOCKS - 1)
        def _():
            halo(s).start()

        @pl.when(place == 0)
        def _():
            gated[s, 0:8, :] = jnp.zeros((8, 128), F32)

        for j in range(2):
            for half in range(2):
                copy, apart = message(s, j, half)

                @pl.when(apart > 0)
                def _():
                    copy.start()

                @pl.when(apart == 0)
                def _():
                    recv[place] = msg[4 * s + 2 * j + half]

        return 0

    lax.fori_loop(0, 4, step, 0)

    columns = pl.ds(pl.multiple_of(x * 128, 128), 128)

    def convolve(s, _):
        @pl.when(place > 0)
        def _():
            halo(s).wait_recv()

        convolved = sum(
            taps_ref[t : t + 1, columns] * gated[s, 6 + t : 6 + t + ROWS, :] for t in range(3)
        )
        branch = (outgate[s].astype(F32) * convolved).astype(BF16)
        branch_out[2 * s] = branch[0:HALF]
        branch_out[2 * s + 1] = branch[HALF:ROWS]
        for half in range(2):
            copy, apart = to_home(2 * s + half)

            @pl.when(apart > 0)
            def _():
                copy.start()

            @pl.when(apart == 0)
            def _():
                branch_in[2 * x + core] = branch[half * HALF : (half + 1) * HALF]

        return 0

    lax.fori_loop(0, SEQS, convolve, 0)

    for k in range(1, 4):
        for m in range(6):
            spread(k, m).wait_send()
        for i in range(1, 4):
            for way in range(2):
                near(k, i, way).wait_send()
    for kind in kinds:
        far(*kind).wait_send()
        onward(*kind).wait_send()
    for copy in [right_a, right_next, right_last, left_b, left_next, left_last, on_right, on_left] + pairs:
        copy.wait_send()

    def to_mate(block):
        return remote(
            recv.at[block, 0:HALF], mate.at[block], mate_send.at[block], mate_recv.at[block], sibling
        )

    source_core = lax.div(y, 2)

    lanes = lambda shape: lax.broadcasted_iota(jnp.int32, shape, 1)
    rows = lambda shape: lax.broadcasted_iota(jnp.int32, shape, 0)
    side_out.wait_recv()
    place_of_head = lanes((1, 128)) == 2 * x + lax.rem(number, 2)
    offset_lane = sides[lax.div(number, 2), 0:1, 1024:1152]
    offset = jnp.sum(jnp.where(place_of_head, offset_lane, 0.0), axis=1, keepdims=True) * LOG2E
    offset = jnp.broadcast_to(offset, (HALF, 128))
    o1, o2, o3 = (part.astype(F32) for part in three_parts(offset))
    lane_q = lanes((HALF, 128))
    offset_row = jnp.where(
        lane_q == 0, -o1, jnp.where(lane_q == 1, -o2, jnp.where(lane_q == 2, -o3, 0.0))
    ).astype(BF16)
    square = (ROWS, HALF)
    source = lax.rem(rows(square), 8) * 48 + rows(square) // 8 - lanes(square)
    permute_own = (source == core * HALF).astype(F32).astype(BF16)
    permute_mate = (source == HALF - core * HALF).astype(F32).astype(BF16)
    take_high = (lanes((HD, 128)) == rows((HD, 128)) + HD).astype(F32).astype(BF16)
    ones = (lanes((ROWS, 128)) < 3).astype(F32).astype(BF16)
    low_lane = lanes((96, 128)) < HD

    def prepare(block):
        pair = dot(permute_own, recv[block, 0:HALF, :]) + dot(permute_mate, mate[block])
        pair = pair.astype(BF16)
        at = pl.ds(pl.multiple_of(block * ROWS, ROWS), ROWS)
        keys[at, 0:128] = pair
        keys[at, 128:256] = ones
        values[block] = dot_nt(take_high, pair).astype(BF16)
        packed = recv[block, HALF:MESSAGE, :].astype(F32)
        tile, first = lax.div(block, 2), lax.rem(block, 2) * HALF
        rows_of = lambda start, size: pl.ds(pl.multiple_of(first + start, 32), size)
        queries[tile, rows_of(0, 96), 0:128] = jnp.where(low_lane, packed, 0.0).astype(BF16)
        queries[tile, rows_of(96, 96), 0:128] = jnp.where(
            low_lane, pltpu.roll(packed, HD, 1), 0.0
        ).astype(BF16)
        queries[tile, rows_of(0, HALF), 128:256] = offset_row

    def arrive(k):
        block = lax.rem(place + k, BLOCKS)

        @pl.when(k + lax.abs(source_core - core) > 0)
        def _():
            remote(
                msg.at[0], recv.at[block], msg_send.at[0], msg_recv.at[block], (block, x, source_core)
            ).wait_recv()

        to_mate(block).start()

    def use(k):
        block = lax.rem(place + k, BLOCKS)
        to_mate(block).wait_recv()
        prepare(block)

    arrive(0)
    arrive(1)

    def arrive_and_use(k, _):
        arrive(k)
        use(k - 2)
        return 0

    lax.fori_loop(2, BLOCKS, arrive_and_use, 0)
    for copy in others + fetches:
        copy.start()
    use(BLOCKS - 2)
    use(BLOCKS - 1)

    def att_home(block):
        at = 4 * x + number
        apart = lax.abs(block - place) + lax.abs(seq - x)
        return remote(
            att_out.at[block], att_in.at[at], att_send.at[block], att_recv.at[at], (block, seq, core)
        ), apart

    def mass_home(block):
        at = 4 * x + 2 * lax.rem(number, 2) + core
        goal = lax.div(number, 2)
        apart = lax.abs(block - place) + lax.abs(seq - x) + lax.abs(goal - core)
        return remote(
            mass_out.at[block], mass_in.at[at], mass_send.at[block], mass_recv.at[at], (block, seq, goal)
        ), apart

    sub = rows((8, ROWS))
    lane = lanes((8, ROWS))
    where_q = lane + core * HALF + jnp.where(lane < HALF, 0, HALF)

    def score(z_ref, tile_index, block):
        begin = pl.multiple_of(block * ROWS, ROWS)
        z_ref[...] = dot_nt(keys[pl.ds(begin, ROWS), :], queries[tile_index])

    def fold(w_ref, block):
        total[...] += dot(values[block], w_ref[...])

    def decay(z_ref, d_ref, ahead, last_block):
        skip = 128 if last_block else 0
        if last_block:
            ahead = ahead[:, skip:]
            d_ref[:, 0:skip] = jnp.zeros((ROWS, skip), F32)
        run = jnp.zeros((8, ROWS - skip), F32)
        for r in reversed(range(48)):
            z = z_ref[8 * r : 8 * r + 8, skip:]
            soft = jnp.maximum(z, lax.log2(1.0 + jnp.exp2(jnp.minimum(z, 126.0))))
            if ahead is not None:
                valid = ahead > r
                soft = jnp.where(valid, soft, 0.0)
            run = run + soft
            value = jnp.exp2(z - run)
            if ahead is not None:
                value = jnp.where(valid, value, 0.0)
            d_ref[8 * r : 8 * r + 8, skip:] = value
        if last_block:
            run = jnp.concatenate((jnp.zeros((8, skip), F32), run), axis=1)
        return run

    def weigh(d_ref, w_ref, run, carry):
        suffix = run
        for step in (1, 2, 4):
            moved = pltpu.roll(suffix, 8 - step, 0)
            suffix = suffix + jnp.where(sub < 8 - step, moved, 0.0)
        after = jnp.where(sub < 7, pltpu.roll(suffix, 7, 0), 0.0)
        kept = jnp.exp2(-(carry + after))
        for i in range(24):
            both = jnp.concatenate(
                (d_ref[16 * i : 16 * i + 8, :] * kept, d_ref[16 * i + 8 : 16 * i + 16, :] * kept), axis=0
            )
            w_ref[16 * i : 16 * i + 16, :] = both.astype(BF16)
        return carry + jnp.broadcast_to(suffix[0:1], (8, ROWS))

    def run_blocks(tile, top, carry, run, aheads, next_tile, next_top):
        count = len(aheads)
        slots = (0, 1, 2, 3) if count == 4 else (0, 3)
        if count == 4:
            score(scores[3], tile, top - 3)
        else:
            score(scores[2], next_tile, lax.max(next_top - 2, 0))
        if run is not None:
            carry = weigh(decays[3], weights[3], run, carry)
        for i in range(count):
            slot = slots[i]
            run = decay(scores[i], decays[slot], aheads[i], i == 0 and aheads[0] is not None)
            if i > 0:
                fold(weights[slots[i - 1]], top - i + 1)
            elif aheads[0] is None:
                fold(weights[3], top + 1)
            if i < 3:
                score(scores[i], next_tile, lax.max(next_top - i, 0))
            if i < count - 1:
                carry = weigh(decays[slot], weights[slot], run, carry)
        return carry, run

    last = BLOCKS // 2 - 1
    for i in range(3):
        score(scores[i], last, BLOCKS - 1 - i)

    def one_tile(m, odd):
        total[...] = jnp.zeros_like(total)
        aheads = (where_q - ROWS - 48 * sub, where_q - 48 * sub)
        aheads = aheads + (None, None) if odd else aheads
        begin = 2 * m - 3 if odd else 2 * m - 1
        rest = lax.div(m, 2)
        more = lax.min(rest, 1)
        below = lax.max(m - 1, 0)

        def following(top, stay):
            return stay * m + (1 - stay) * below, stay * top + (1 - stay) * (2 * m - 1)

        state = run_blocks(m, 2 * m + 1, jnp.zeros((8, ROWS), F32), None, aheads, *following(begin, more))

        def earlier(i, state):
            top = begin - 4 * i
            stay = lax.min(lax.div(top, 4), 1)
            return run_blocks(m, top, *state, (None,) * 4, *following(top - 4, stay))

        carry, run = lax.fori_loop(0, rest, earlier, state)
        carry = weigh(decays[3], weights[3], run, carry)
        fold(weights[3], 0)
        attended = total[...]
        attended = jnp.concatenate((attended, attended), axis=0).T
        for part in range(2):
            block = 2 * m + part
            r = part * HALF
            folded = jnp.where(lanes((96, 128)) < HD, attended[r : r + 96], attended[r + 96 : r + HALF])
            folded = folded.astype(BF16)
            mass = carry[:, r : r + HALF]
            att_out[block] = folded
            mass_out[block, :, 0:HALF] = mass
            copy, apart = att_home(block)

            @pl.when(apart > 0)
            def _():
                copy.start()

            @pl.when(apart == 0)
            def _():
                att_in[4 * x + number] = folded

            mass_copy, mass_apart = mass_home(block)

            @pl.when(mass_apart > 0)
            def _():
                mass_copy.start()

            @pl.when(mass_apart == 0)
            def _():
                mass_in[4 * x + 2 * lax.rem(number, 2) + core, :, 0:HALF] = mass

    def two_tiles(step, _):
        one_tile(last - 2 * step, True)
        one_tile(last - 1 - 2 * step, False)
        return 0

    lax.fori_loop(0, BLOCKS // 4, two_tiles, 0)

    for copy in fetches:
        copy.wait()
    for copy in others:
        copy.wait_recv()
    def branch_arrived(k, _):
        there = lax.rem(2 * x + core + k, 8)
        remote(
            branch_out.at[0],
            branch_in.at[there],
            branch_send.at[0],
            branch_recv.at[there],
            (place, lax.div(there, 2), lax.rem(there, 2)),
        ).wait_recv()
        return 0

    lax.fori_loop(1, 8, branch_arrived, 0)

    def branch_product(store, row_gain, projection, load):
        squares = jnp.zeros((HALF, 128), F32)
        for owner in range(2):
            for part in range(4):
                piece = load(owner, part)
                squares = squares + piece * piece
                gain = sides[owner, 0:1, row_gain + 128 * part : row_gain + 128 * part + 128]
                at = 512 * owner + 128 * part
                store[:, at : at + 128] = (piece * gain).astype(BF16)
        scale = lax.rsqrt(jnp.sum(squares, axis=1, keepdims=True) / ATT_WIDTH + epsilon)
        return scale * dot(store[...], projection[...].reshape(1024, D))

    mixed = branch_product(
        matrix.at[0], 512, conv_weights, lambda owner, part: branch_in[2 * part + owner].astype(F32)
    )

    def landed(at, _):
        column, n = lax.div(at, 4), lax.rem(at, 4)
        there = mod4(x + n) * 4 + n
        apart = lax.abs(there - place) + lax.abs(column - x)

        @pl.when(apart > 0)
        def _():
            remote(
                att_out.at[0], att_in.at[at], att_send.at[0], att_recv.at[at], (there, column, core)
            ).wait_recv()

        n = 2 * core + lax.div(n, 2)
        owner = lax.rem(at, 2)
        there = mod4(x + n) * 4 + n
        apart = lax.abs(there - place) + lax.abs(column - x) + lax.abs(owner - core)

        @pl.when(apart > 0)
        def _():
            remote(
                mass_out.at[0], mass_in.at[at], mass_send.at[0], mass_recv.at[at], (there, column, owner)
            ).wait_recv()

        return 0

    lax.fori_loop(0, 16, landed, 0)

    def heads(owner, part):
        a = att_in[4 * part + 2 * owner].astype(F32)
        b = att_in[4 * part + 2 * owner + 1].astype(F32)
        low = lanes((96, 128)) < HD
        upper = jnp.where(low, a, pltpu.roll(b, HD, 1))
        lower = jnp.where(low, pltpu.roll(a, HD, 1), b)
        return jnp.concatenate((upper, lower), axis=0)

    mixed = mixed + branch_product(matrix.at[1], 0, att_weights, heads)
    mixed_ref[0] = mixed.astype(BF16)
    for part in range(2):
        kept = jnp.concatenate([mass_in[2 * n + part, 0:1, :] for n in range(8)], axis=0)
        mass = jnp.log(2.0 - jnp.exp2(-kept))
        mass_ref[0, :, part * HALF : (part + 1) * HALF] = mass[:, 0:HALF]

    def left(block, _):
        copy, apart = att_home(block)

        @pl.when(apart > 0)
        def _():
            copy.wait_send()

        mass_copy, mass_apart = mass_home(block)

        @pl.when(mass_apart > 0)
        def _():
            mass_copy.wait_send()

        return 0

    lax.fori_loop(0, BLOCKS, left, 0)


    def left_here(at, _):
        s = lax.div(at, 4)
        j = lax.div(lax.rem(at, 4), 2)
        copy, apart = message(s, j, lax.rem(at, 2))

        @pl.when(apart > 0)
        def _():
            copy.wait_send()

        to_mate(at).wait_send()
        return 0

    lax.fori_loop(0, BLOCKS, left_here, 0)

    def branch_left(at, _):
        copy, apart = to_home(at)

        @pl.when(apart > 0)
        def _():
            copy.wait_send()

        return 0

    lax.fori_loop(0, 8, branch_left, 0)

    @pl.when(place < BLOCKS - 1)
    def _():
        for s in range(SEQS):
            halo(s).wait_send()

    side_out.wait_send()
    for copy in others:
        copy.wait_send()


def layer(tokens, gain, att_gain, conv_gain, offset, taps, mats, out_att, out_conv):
    hbm = pl.BlockSpec(memory_space=pl.ANY)
    vmem = pl.BlockSpec(memory_space=pltpu.VMEM)
    dma = lambda *shape: pltpu.SemaphoreType.DMA(shape)
    return pl.pallas_call(
        layer_kernel,
        in_specs=[hbm] + [vmem] * 5 + [hbm] * 8,
        out_specs=[vmem, vmem],
        out_shape=[
            jax.ShapeDtypeStruct((1, HALF, D), BF16),
            jax.ShapeDtypeStruct((1, 8, ROWS), F32),
        ],
        scratch_shapes=[
            pltpu.VMEM((SEQS, 2, ROWS, 1024), BF16),
            pltpu.VMEM((4, 4, 128, 768), BF16),
            pltpu.VMEM((BLOCKS, MESSAGE, 128), BF16),
            pltpu.VMEM((BLOCKS, MESSAGE, 128), BF16),
            pltpu.VMEM((BLOCKS, HALF, 128), BF16),
            pltpu.VMEM((SEQS, ROWS + 8, 128), F32),
            pltpu.VMEM((SEQS, ROWS, 128), BF16),
            pltpu.VMEM((8, HALF, 128), BF16),
            pltpu.VMEM((8, HALF, 128), BF16),
            pltpu.VMEM((BLOCKS * ROWS, 256), BF16),
            pltpu.VMEM((BLOCKS, HD, ROWS), BF16),
            pltpu.VMEM((BLOCKS // 2, ROWS, 256), BF16),
            [pltpu.VMEM((ROWS, ROWS), F32)] * 4,
            [pltpu.VMEM((ROWS, ROWS), F32)] * 4,
            [pltpu.VMEM((ROWS, ROWS), BF16)] * 4,
            pltpu.VMEM((HD, ROWS), F32),
            pltpu.VMEM((BLOCKS, 96, 128), BF16),
            pltpu.VMEM((BLOCKS, 96, 128), BF16),
            pltpu.VMEM((BLOCKS, 8, 256), F32),
            pltpu.VMEM((BLOCKS, 8, 256), F32),
            pltpu.VMEM((2, 512, D), BF16),
            pltpu.VMEM((2, 512, D), BF16),
            pltpu.VMEM((2, HALF, 1024), BF16),
            pltpu.VMEM((1, 1152), F32),
            pltpu.VMEM((2, 1, 1152), F32),
            dma(31),
            dma(3, 6), dma(3, 6),
            dma(18), dma(18),
            dma(12), dma(12),
            dma(12), dma(12),
            dma(8), dma(8),
            dma(8), dma(8),
            dma(16), dma(16),
            dma(16), dma(16),
            dma(3), dma(3),
            dma(4), dma(4),
            dma(8), dma(8),
            dma(16), dma(16),
            dma(16), dma(16),
        ],
        compiler_params=pltpu.CompilerParams(
            collective_id=0, has_side_effects=True, vmem_limit_bytes=58 << 20
        ),
        name="layer",
    )(tokens, gain, att_gain, conv_gain, offset, taps, *mats, out_att, out_conv)


def per_device(
    tokens,
    in_gain,
    w_query,
    w_key,
    w_value,
    w_outgate,
    w_ingate,
    w_conv_in,
    score_offset,
    conv_taps,
    att_gain,
    conv_gain,
    out_att,
    out_conv,
):
    mixed, mass = layer(
        tokens[0],
        in_gain.reshape(1, D),
        att_gain.reshape(1, 512),
        conv_gain.reshape(1, 512),
        score_offset.reshape(1, 8),
        conv_taps,
        (w_query, w_key, w_value, w_outgate, w_ingate, w_conv_in),
        out_att,
        out_conv,
    )
    return mixed, jnp.swapaxes(mass, 1, 2)


def solution(mesh):
    return jax.shard_map(
        per_device,
        mesh=mesh,
        in_specs=(
            P("fs", "sp", "tp"),
            P(),
            P("fs", "tp"),
            P("fs", "tp"),
            P("fs", "tp"),
            P("fs", "tp"),
            P("fs", "tp"),
            P("fs", "tp"),
            P("tp"),
            P(None, "tp"),
            P("tp"),
            P("tp"),
            P("tp", None),
            P("tp", None),
        ),
        out_specs=(P("fs", ("sp", "tp"), None), P("fs", "sp", "tp")),
        check_vma=False,
    )
```
